128 devices in a mesh: sp: 16 (over z, y), tp: 8 (over x, core).
Axes of the slice: x: 4, y: 4, z: 4, core: 2. Of those that a mesh axis runs over, the one named last changes fastest.
Arguments:
- queries: bfloat16 [12288, 2048], P('sp', 'tp'), may hold values from -11 to 11
- key_rows: bfloat16 [12288, 2048], P('sp', 'tp'), may hold values from -4.5 to 4.5
- value_rows: bfloat16 [12288, 2048], P('sp', 'tp'), may hold values from -6 to 6
- log_forget: float32 [12288, 32], P('sp', 'tp'), may hold values from -1477.56 to 0, as said below
- stream_in: bfloat16 [12288, 2048], P('sp'), may hold values from -6 to 6
- out_weight: bfloat16 [2048, 2048], P('tp'), may hold values from -0.52734375 to 0.52734375
- mix_gain: float32 [2048], replicated, may hold values from 0.1 to 1.9
- mix_bias: float32 [2048], replicated, may hold values from -3 to 3
- gate_weight: bfloat16 [2048, 5632], P('sp', 'tp'), may hold values from -0.125 to 0.125
- up_weight: bfloat16 [2048, 5632], P('sp', 'tp'), may hold values from -0.125 to 0.125
- down_weight: bfloat16 [5632, 2048], P('tp', 'sp'), may hold values from -0.15917969 to 0.15917969
- ffn_gain: float32 [2048], replicated, may hold values from 0.1 to 1.9
- ffn_bias: float32 [2048], replicated, may hold values from -3 to 3
Outputs:
- layer_out: bfloat16 [12288, 2048], P(('sp', 'tp'))
The draws below stay inside these ranges and needn't reach their ends.
Inputs may be any that keep to these rules, and one draw needn't show every extreme that they name: `log_forget`: each column never rises along the positions.
All inputs are finite; a program needn't handle non-finite values.
Results may differ from the reference program's by a relative error of at most 0.015.
Values may be sent and summed in bfloat16 or wider, within the bound.
No kernel may reach another device: no remote copies, remote signals or barrier semaphores. Data moves between devices by JAX's collectives and lax.ppermute only.
A program may use at most 128 MiB of HBM per device.

```python
import math
import jax
import jax.numpy as jnp
from jax import lax

D = 2048
HEAD_TOTAL = 32
FF = 5632
TOK_DEV = 768
SEQUENCE_LENGTH = 12288
N_SP = 16


def draw_queries(key, part):
    base_noise = jax.random.normal(jax.random.fold_in(key, 1), (SEQUENCE_LENGTH, D), jnp.float32)
    row_scale = jnp.exp(jax.random.uniform(jax.random.fold_in(key, 31), (SEQUENCE_LENGTH, 1), jnp.float32, -0.7, 1.6))
    base_noise = jnp.clip(base_noise * row_scale, -11.0, 11.0)
    return base_noise.astype(jnp.bfloat16)


def draw_key_rows(key, part):
    base_noise = jax.random.normal(jax.random.fold_in(key, 2), (SEQUENCE_LENGTH, D), jnp.float32)
    row_scale = jnp.exp(jax.random.uniform(jax.random.fold_in(key, 32), (SEQUENCE_LENGTH, 1), jnp.float32, -0.8, 0.8))
    base_noise = jnp.clip(base_noise * row_scale, -4.5, 4.5)
    return base_noise.astype(jnp.bfloat16)


def draw_log_forget(key, part):
    head_order = jax.random.permutation(jax.random.fold_in(key, 21), HEAD_TOTAL)
    sluggish_heads = head_order < HEAD_TOTAL // 2
    fast_rate = jnp.exp(jax.random.uniform(jax.random.fold_in(key, 22), (HEAD_TOTAL,), jnp.float32, math.log(1.0 / 100.0), math.log(1.0 / 30.0)))
    head_rate = jnp.where(sluggish_heads, 0.5 / SEQUENCE_LENGTH, fast_rate)
    block_count = SEQUENCE_LENGTH // TOK_DEV
    block_factor = jnp.exp(jax.random.uniform(jax.random.fold_in(key, 23), (block_count, HEAD_TOTAL), jnp.float32, math.log(0.5), math.log(2.0)))
    position_factor = jax.random.uniform(jax.random.fold_in(key, 24), (SEQUENCE_LENGTH, HEAD_TOTAL), jnp.float32, 0.25, 1.75)
    logarithm_increments = -head_rate[None, :] * jnp.repeat(block_factor, TOK_DEV, axis=0) * position_factor
    spike_locations = jax.random.randint(jax.random.fold_in(key, 25), (3, HEAD_TOTAL), 0, SEQUENCE_LENGTH)
    spike_lengths = jax.random.uniform(jax.random.fold_in(key, 26), (3, HEAD_TOTAL), jnp.float32, 0.22, 0.69)
    token_positions = jnp.arange(SEQUENCE_LENGTH, dtype=jnp.int32)
    for spike_index in range(3):
        spike_matches = (token_positions[:, None] == spike_locations[spike_index][None, :]) & sluggish_heads[None, :]
        logarithm_increments = logarithm_increments - jnp.where(spike_matches, spike_lengths[spike_index][None, :], 0.0)
    return jnp.cumsum(logarithm_increments, axis=0).astype(jnp.float32)


def levels(key, dims, cuts, low, largest):
    level, own = 1.0, jax.random.fold_in(key, 6)
    for axis_at, blocks in cuts:
        heights = jnp.exp(jax.random.uniform(jax.random.fold_in(own, axis_at), (blocks,), jnp.float32, low / len(cuts), largest / len(cuts)))
        level = level * jnp.repeat(heights, dims[axis_at] // blocks).reshape([-1 if axis == axis_at else 1 for axis in range(len(dims))])
    return level


def scatter_about(key, extent, width, most, split=(), kind=jnp.bfloat16):
    values = width * jax.random.normal(key, extent, jnp.float32)
    if split:
        values = values * levels(key, extent, split, -0.22, 0.18)
    return jnp.clip(values, -most, most).astype(kind)


def setup_inputs(seed: int = 0) -> dict:
    seeds = jax.random.split(jax.random.key(seed), 14)
    return {
        "queries": draw_queries(jax.random.fold_in(seeds[13], 71), 0),
        "key_rows": draw_key_rows(jax.random.fold_in(seeds[13], 71), 0),
        "value_rows": scatter_about(seeds[2], (SEQUENCE_LENGTH, D), 1.0, 6.0, ((0, 16), (1, 8))),
        "log_forget": draw_log_forget(jax.random.fold_in(seeds[13], 71), 0),
        "stream_in": scatter_about(seeds[4], (SEQUENCE_LENGTH, D), 1.0, 6.0, ((0, 16),)),
        "out_weight": scatter_about(seeds[5], (D, D), (4.0 * D ** -0.5), 0.52734375, ((0, 8),)),
        "mix_gain": jnp.clip(1.0 + 0.18 * jax.random.normal(seeds[6], (D,), jnp.float32), 0.1, 1.9),
        "mix_bias": scatter_about(seeds[7], (D,), 0.5, 3.0, (), jnp.float32),
        "gate_weight": scatter_about(seeds[8], (D, FF), D ** -0.5, 0.125, ((0, 16), (1, 8))),
        "up_weight": scatter_about(seeds[9], (D, FF), D ** -0.5, 0.125, ((0, 16), (1, 8))),
        "down_weight": scatter_about(seeds[10], (FF, D), (2.0 * FF ** -0.5), 0.15917969, ((0, 8), (1, 16))),
        "ffn_gain": jnp.clip(1.0 + 0.18 * jax.random.normal(seeds[11], (D,), jnp.float32), 0.1, 1.9),
        "ffn_bias": scatter_about(seeds[12], (D,), 0.5, 3.0, (), jnp.float32),
    }


ALPHA = 8.0 ** 0.25
EPSILON = 1e-05

def layer_norm(matrix, norm_gain, norm_shift):
    centred = matrix - lax.optimization_barrier(jnp.mean(matrix, axis=-1, keepdims=True))
    spread = lax.optimization_barrier(jnp.mean(centred * centred, axis=-1, keepdims=True))
    return centred * lax.rsqrt(spread + EPSILON) * norm_gain + norm_shift

def head_attention(query_head, key_head, value_head, gate_head):
    head_dim = query_head.shape[1]
    score_scale = head_dim ** (-0.5)
    key_pos = jnp.arange(SEQUENCE_LENGTH, dtype=jnp.int32)
    query_blocks = query_head.reshape(N_SP, TOK_DEV, head_dim)
    gate_blocks = gate_head.reshape(N_SP, TOK_DEV)

    def one_block(packed):
        query_block, gate_block, block_index = packed
        scores = jnp.dot(query_block, key_head.T, preferred_element_type=jnp.float32) * score_scale
        scores = scores + gate_block[:, None] - gate_head[None, :]
        query_pos = block_index * TOK_DEV + jnp.arange(TOK_DEV, dtype=jnp.int32)
        allowed = key_pos[None, :] <= query_pos[:, None]
        masked = jnp.where(allowed, scores, -1e+30)
        highest = lax.optimization_barrier(jnp.max(masked, axis=1, keepdims=True))
        exponent = jnp.where(allowed, jnp.exp(masked - highest), 0.0)
        totals = lax.optimization_barrier(jnp.sum(exponent, axis=1, keepdims=True))
        weighted = jnp.dot(exponent.astype(jnp.bfloat16), value_head, preferred_element_type=jnp.float32)
        return (weighted / totals).astype(jnp.bfloat16)
    return lax.map(one_block, (query_blocks, gate_blocks, jnp.arange(N_SP, dtype=jnp.int32)))

def reference(queries, key_rows, value_rows, log_forget, stream_in, out_weight, mix_gain, mix_bias, gate_weight, up_weight, down_weight, ffn_gain, ffn_bias):
    head_count = log_forget.shape[1]
    head_dim = queries.shape[1] // head_count

    def split_heads(matrix):
        return matrix.reshape(SEQUENCE_LENGTH, head_count, head_dim).transpose(1, 0, 2)

    def per_head(packed):
        return head_attention(packed[0], packed[1], packed[2], packed[3])
    attended = lax.map(per_head, (split_heads(queries), split_heads(key_rows), split_heads(value_rows), log_forget.T))
    attended = attended.reshape(head_count, SEQUENCE_LENGTH, head_dim).transpose(1, 0, 2).reshape(SEQUENCE_LENGTH, head_count * head_dim)
    mix_out = jnp.dot(attended, out_weight, preferred_element_type=jnp.float32).astype(jnp.bfloat16)
    mix_out = lax.optimization_barrier(mix_out).astype(jnp.float32)
    normed = layer_norm(ALPHA * stream_in.astype(jnp.float32) + mix_out, mix_gain, mix_bias).astype(jnp.bfloat16)
    gate_part = jnp.dot(normed, gate_weight, preferred_element_type=jnp.float32)
    up_part = jnp.dot(normed, up_weight, preferred_element_type=jnp.float32)
    hidden = (jax.nn.silu(gate_part) * up_part).astype(jnp.bfloat16)
    lowered = jnp.dot(hidden, down_weight, preferred_element_type=jnp.float32).astype(jnp.bfloat16)
    lowered = lax.optimization_barrier(lowered).astype(jnp.float32)
    result = layer_norm(ALPHA * normed.astype(jnp.float32) + lowered, ffn_gain, ffn_bias)
    return result.astype(jnp.bfloat16)
```

```python
import functools
import jax
import jax.numpy as jnp
import numpy as np
from jax import lax
from jax.experimental import pallas as pl
from jax.experimental.pallas import tpu as pltpu
from jax.sharding import Mesh, PartitionSpec as P

ALPHA = 8.0**0.25
EPSILON = 1e-05
F32 = jnp.float32
BF16 = jnp.bfloat16

ROWS = 768
SUB = 192
HALF = 96
HD = 64
NSH = 16
PACK = 800
TILE = 256
TILES = SUB * NSH // TILE


def vmem():
    return pl.BlockSpec(memory_space=pltpu.VMEM)


def smem():
    return pl.BlockSpec(memory_space=pltpu.SMEM)


def params(mb=60):
    return pltpu.CompilerParams(vmem_limit_bytes=mb * 1024 * 1024)


def pack_kernel(q_ref, k_ref, v_ref, g_ref, qo_ref, kvo_ref):
    for h in range(4):
        cols = slice(h * HD, (h + 1) * HD)
        kvo_ref[h, 0:ROWS, 0:HD] = k_ref[:, cols]
        kvo_ref[h, 0:ROWS, HD : 2 * HD] = v_ref[:, cols]
        for z in range(4):
            at = z * SUB
            qo_ref[z * 4 + h, :, 0:HD] = q_ref[at : at + HALF, cols]
            qo_ref[z * 4 + h, :, HD : 2 * HD] = q_ref[at + HALF : at + SUB, cols]
        chunks = [-g_ref[h : h + 1, c * 128 : (c + 1) * 128] for c in range(6)]
        value = jnp.concatenate(chunks, axis=0)
        first = value.astype(BF16).astype(F32)
        second = (value - first).astype(BF16).astype(F32)
        third = value - first - second
        rest = jnp.zeros((PACK - ROWS - 18, 128), F32)
        kvo_ref[h, ROWS:PACK, :] = jnp.concatenate(
            [first, second, third, rest], axis=0
        ).astype(BF16)


def pack(q, k, v, g):
    return pl.pallas_call(
        pack_kernel,
        out_shape=(
            jax.ShapeDtypeStruct((NSH, HALF, 128), BF16),
            jax.ShapeDtypeStruct((4, PACK, 128), BF16),
        ),
        in_specs=[vmem()] * 4,
        out_specs=(vmem(), vmem()),
        compiler_params=params(),
        cost_estimate=pl.CostEstimate(flops=10**6, bytes_accessed=2500000, transcendentals=0),
    )(q, k, v, g)


def unit_table():
    units = []
    for t in range(TILES):
        low = (TILE * t) // SUB
        for j in range(low + 2):
            units.append((t, j, int(j >= low), int(j == low + 1)))
    assert len(units) % 2 == 0
    count = len(units)
    units = [(0, 0, 0, 0)] + units + [units[-1]]
    return count, np.array(units, np.int32).T.copy()


UNITS, TABLE = unit_table()


def attend_kernel(
    tab, z_ref, q_ref, kv_ref, o_ref,
    kaug, vt, qrow, qt, qpos, oscr, s_a, s_b, p_a, p_b, al_a, al_b, top, acc,
):
    lane = lax.broadcasted_iota(jnp.int32, (128, 128), 1)

    def per_shard(s, carry):
        gates = kv_ref[s, ROWS:PACK, :].astype(F32)
        square = jnp.concatenate(
            [jnp.zeros((HD, 128), F32), gates, jnp.zeros((32, 128), F32)], axis=0
        )
        turned = square.T
        for c in range(6):
            part = kv_ref[s, c * 128 : (c + 1) * 128, :].astype(F32)
            mine = (lane == HD + c) | (lane == HD + 6 + c) | (lane == HD + 12 + c)
            kaug[s, c * 128 : (c + 1) * 128, :] = jnp.where(
                lane < HD, part, jnp.where(mine, turned, 0.0)
            ).astype(BF16)
            vt[s, :, c * 128 : (c + 1) * 128] = part.T.astype(BF16)
        vt[s, 48:64, :] = jnp.ones((16, ROWS), BF16)
        return carry

    lax.fori_loop(0, NSH, per_shard, 0)

    lane_h = lax.broadcasted_iota(jnp.int32, (HALF, 128), 1)

    def per_query(s, carry):
        both = q_ref[s].astype(F32) * (HD**-0.5)
        ones = jnp.where(lane_h < HD + 18, 1.0, 0.0)
        qrow[s, 0:HALF, :] = jnp.where(lane_h < HD, both, ones)
        qrow[s, HALF:SUB, :] = jnp.where(lane_h < HD, pltpu.roll(both, HD, 1), ones)
        return carry

    lax.fori_loop(0, NSH, per_query, 0)
    z = z_ref[0]
    lane_t = lax.broadcasted_iota(jnp.int32, (8, TILE), 1)
    for t in range(TILES):
        low = (TILE * t) // SUB
        edge = (low + 1) * SUB - TILE * t
        rows = jnp.concatenate(
            [
                qrow[low, SUB - edge : SUB, :],
                qrow[low + 1, 0 : TILE - edge, :],
            ],
            axis=0,
        )
        qt[t] = rows.T.astype(BF16)
        qpos[t] = z * SUB + jnp.where(
            lane_t < edge,
            low * ROWS + (SUB - edge) + lane_t,
            (low + 1) * ROWS + lane_t - edge,
        )
    acc[...] = jnp.zeros(acc.shape, F32)
    top[...] = jnp.full(top.shape, -1e30, F32)
    al_a[...] = jnp.zeros(al_a.shape, F32)
    al_b[...] = jnp.zeros(al_b.shape, F32)
    p_b[...] = jnp.zeros(p_b.shape, BF16)

    def scores(at, out):
        out[...] = jnp.dot(kaug[tab[1, at]], qt[tab[0, at]], preferred_element_type=F32)

    scores(1, s_a)

    def unit(at, s_now, s_next, p_before, p_now, al_before, al_now):
        def work(masked):
            scores(at + 1, s_next)
            j = tab[1, at]
            pv = jnp.dot(vt[tab[1, at - 1], 48:128, :], p_before[...], preferred_element_type=F32)
            acc[...] = acc[...] * al_before[0:1, :] + pv
            before = jnp.where(j == 0, -1e30, top[0:1, :])
            s = s_now[...]
            if masked:
                pos = j * ROWS + lax.broadcasted_iota(jnp.int32, (ROWS, TILE), 0)
                s = jnp.where(pos <= qpos[tab[0, at], 0:1, :], s, -1e30)
            high = jnp.maximum(before, jnp.max(s, axis=0, keepdims=True))
            p_now[...] = jnp.exp(s - high).astype(BF16)
            top[0:1, :] = high
            al_now[0:1, :] = jnp.exp(before - high)

        lax.cond(tab[2, at] == 1, lambda: work(True), lambda: work(False))
        finish(at - 1)

    def finish(at):
        @pl.when(tab[3, at] == 1)
        def _():
            good = acc[16:80, :] / acc[0:1, :]
            row = pl.multiple_of(tab[0, at] * TILE, TILE)
            full = jnp.concatenate([good, jnp.zeros((HD, TILE), F32)], axis=0)
            oscr[pl.ds(row, TILE), :] = full.T

    def pair(i, carry):
        unit(2 * i + 1, s_a, s_b, p_b, p_a, al_b, al_a)
        unit(2 * i + 2, s_b, s_a, p_a, p_b, al_a, al_b)
        return carry

    lax.fori_loop(0, UNITS // 2, pair, 0)
    pv = jnp.dot(vt[tab[1, UNITS], 48:128, :], p_b[...], preferred_element_type=F32)
    acc[...] = acc[...] * al_b[0:1, :] + pv
    finish(UNITS)

    def out(s, carry):
        row = pl.multiple_of(s * SUB, SUB)
        one = oscr[pl.ds(row, HALF), :]
        two = oscr[pl.ds(row + HALF, HALF), :]
        o_ref[s] = jnp.where(lane_h < HD, one, pltpu.roll(two, HD, 1)).astype(BF16)
        return carry

    lax.fori_loop(0, NSH, out, 0)


def attend(q, kv, z):
    return pl.pallas_call(
        attend_kernel,
        out_shape=jax.ShapeDtypeStruct((NSH, HALF, 128), BF16),
        in_specs=[smem(), smem(), vmem(), vmem()],
        out_specs=vmem(),
        scratch_shapes=[
            pltpu.VMEM((NSH, ROWS, 128), BF16),
            pltpu.VMEM((NSH, 128, ROWS), BF16),
            pltpu.VMEM((NSH, SUB, 128), F32),
            pltpu.VMEM((TILES, 128, TILE), BF16),
            pltpu.VMEM((TILES, 8, TILE), jnp.int32),
            pltpu.VMEM((SUB * NSH, 128), F32),
            pltpu.VMEM((ROWS, TILE), F32),
            pltpu.VMEM((ROWS, TILE), F32),
            pltpu.VMEM((ROWS, TILE), BF16),
            pltpu.VMEM((ROWS, TILE), BF16),
            pltpu.VMEM((8, TILE), F32),
            pltpu.VMEM((8, TILE), F32),
            pltpu.VMEM((8, TILE), F32),
            pltpu.VMEM((80, TILE), F32),
        ],
        compiler_params=params(),
        cost_estimate=pl.CostEstimate(
            flops=35 * 10**9, bytes_accessed=4 * 10**6, transcendentals=2 * 10**7
        ),
    )(jnp.asarray(TABLE), z, q, kv)


def spread_kernel(o_ref, a_ref):
    for z in range(4):
        for y in range(4):
            for half in range(2):
                a_ref[2 * z + half, :, y * HD : (y + 1) * HD] = o_ref[
                    4 * z + y, :, half * HD : (half + 1) * HD
                ]


def spread(o):
    return pl.pallas_call(
        spread_kernel,
        out_shape=jax.ShapeDtypeStruct((8, HALF, 256), BF16),
        in_specs=[vmem()],
        out_specs=vmem(),
        compiler_params=params(),
        cost_estimate=pl.CostEstimate(flops=10**5, bytes_accessed=800000, transcendentals=0),
    )(o)


def norm_rows(matrix, gain, shift):
    centred = matrix - jnp.mean(matrix, axis=-1, keepdims=True)
    spread_ = jnp.mean(centred * centred, axis=-1, keepdims=True)
    return centred * lax.rsqrt(spread_ + EPSILON) * gain + shift


def mix_kernel(place, a_ref, stream_ref, gain_ref, bias_ref, *rest):
    w_refs, n_ref = rest[:8], rest[8]
    total = None
    for i in range(8):
        term = jnp.dot(a_ref[place[i]], w_refs[i][...], preferred_element_type=F32)
        total = term if total is None else total + term
    mixed = total.astype(BF16).astype(F32)
    matrix = ALPHA * stream_ref[...].astype(F32) + mixed
    n_ref[...] = norm_rows(matrix, gain_ref[...], bias_ref[...]).astype(BF16)


def mix(place, own, att, stream, gain, bias, weights):
    def whole(shape):
        return pl.BlockSpec(shape, lambda i, place: (0,) * len(shape))

    return pl.pallas_call(
        mix_kernel,
        out_shape=jax.ShapeDtypeStruct((HALF, 2048), BF16),
        grid_spec=pltpu.PrefetchScalarGridSpec(
            num_scalar_prefetch=1,
            grid=(1,),
            in_specs=[
                whole((8, HALF, 256)),
                pl.BlockSpec((HALF, 2048), lambda i, place: (place[8], 0)),
                whole((1, 2048)),
                whole((1, 2048)),
            ]
            + [whole((256, 2048))] * 8,
            out_specs=whole((HALF, 2048)),
        ),
        compiler_params=params(),
        cost_estimate=pl.CostEstimate(
            flops=2 * HALF * 2048 * 2048, bytes_accessed=9 * 10**6, transcendentals=0
        ),
    )(place, att, stream, gain, bias, *weights)


def ffn_kernel(x_ref, w_ref, out_ref, w_in, w_out, h_scr):
    @pl.when(pl.program_id(0) == 0)
    def _():
        for s in range(NSH):
            w_in[:, s * 128 : (s + 1) * 128] = w_ref[s, 0:1408, :]
            w_out[:, s * 128 : (s + 1) * 128] = w_ref[s, 1408:2112, :]

    both = lax.dot_general(
        x_ref[...], w_in[...], (((1,), (1,)), ((), ())), preferred_element_type=F32
    )
    gate, up = both[:, 0:704], both[:, 704:1408]
    h_scr[...] = (gate / (1.0 + jnp.exp(-gate)) * up).astype(BF16)
    out_ref[...] = jnp.dot(h_scr[...], w_out[...], preferred_element_type=F32).astype(BF16)


def ffn(x, w, tile=192):
    return pl.pallas_call(
        ffn_kernel,
        out_shape=jax.ShapeDtypeStruct((ROWS, 2048), BF16),
        grid=(ROWS // tile,),
        in_specs=[
            pl.BlockSpec((tile, 2048), lambda i: (i, 0)),
            pl.BlockSpec((NSH, 2112, 128), lambda i: (0, 0, 0)),
        ],
        out_specs=pl.BlockSpec((tile, 2048), lambda i: (i, 0)),
        scratch_shapes=[
            pltpu.VMEM((1408, 2048), BF16),
            pltpu.VMEM((704, 2048), BF16),
            pltpu.VMEM((tile, 704), BF16),
        ],
        compiler_params=params(),
        cost_estimate=pl.CostEstimate(
            flops=6 * ROWS * 2048 * 704, bytes_accessed=15 * 10**6, transcendentals=10**6
        ),
    )(x, w)


def last_kernel(p_ref, n_ref, gain_ref, bias_ref, o_ref):
    total = p_ref[0].astype(F32)
    for i in range(1, 8):
        total = total + p_ref[i].astype(F32)
    lowered = total.astype(BF16).astype(F32)
    matrix = ALPHA * n_ref[...].astype(F32) + lowered
    o_ref[...] = norm_rows(matrix, gain_ref[...], bias_ref[...]).astype(BF16)


def last(parts, normed, gain, bias):
    return pl.pallas_call(
        last_kernel,
        out_shape=jax.ShapeDtypeStruct((HALF, 2048), BF16),
        in_specs=[vmem()] * 4,
        out_specs=vmem(),
        compiler_params=params(),
        cost_estimate=pl.CostEstimate(
            flops=4 * 10**6, bytes_accessed=4 * 10**6, transcendentals=0
        ),
    )(parts, normed, gain, bias)


def body(
    queries, key_rows, value_rows, log_forget, stream_in, out_weight, mix_gain, mix_bias,
    gate_weight, up_weight, down_weight, ffn_gain, ffn_bias,
):
    zi = lax.axis_index("z")
    xi = lax.axis_index("x")
    ci = lax.axis_index("c")
    q_pack, kv_pack = pack(queries, key_rows, value_rows, log_forget.T)
    kv_mine = lax.all_to_all(kv_pack, "y", split_axis=0, concat_axis=0, tiled=True)
    q_mine = lax.all_to_all(q_pack, ("z", "y"), split_axis=0, concat_axis=0, tiled=True)
    kv_all = lax.all_gather(kv_mine, "z", axis=0, tiled=True)

    shards = jnp.concatenate([gate_weight.T, up_weight.T, down_weight], axis=0)
    ffn_all = lax.all_gather(shards, ("z", "y"), axis=0, tiled=False)

    weights, places = [out_weight], [2 * xi + ci]
    for d in (1, 3, 2):
        ring = [(i, (i + d) % 4) for i in range(4)]
        weights.append(lax.ppermute(out_weight, "x", ring))
        places.append(2 * ((xi + 4 - d) % 4) + ci)
    for i in range(4):
        weights.append(lax.ppermute(weights[i], "c", [(0, 1), (1, 0)]))
        places.append(places[i] + 1 - 2 * ci)
    own = 2 * xi + ci
    place = jnp.stack(places + [own]).astype(jnp.int32)

    attended = attend(q_mine, kv_all, zi.astype(jnp.int32)[None])
    by_shard = lax.all_to_all(attended, ("z", "y"), split_axis=0, concat_axis=0, tiled=True)
    by_rows = lax.all_to_all(
        spread(by_shard), ("x", "c"), split_axis=0, concat_axis=0, tiled=True
    )
    normed = mix(
        place, own, by_rows, stream_in, mix_gain[None], mix_bias[None], weights
    )
    gathered = lax.all_gather(normed, ("x", "c"), axis=0, tiled=True)
    partial = ffn(gathered, ffn_all)
    parts = lax.all_to_all(
        partial.reshape(8, HALF, 2048), ("x", "c"), split_axis=0, concat_axis=0, tiled=True
    )
    return last(parts, normed, ffn_gain[None], ffn_bias[None])


def solution(mesh):
    fine = Mesh(mesh.devices.reshape(4, 4, 4, 2), ("z", "y", "x", "c"))
    sp, tp = ("z", "y"), ("x", "c")
    placed = (
        P(sp, tp), P(sp, tp), P(sp, tp), P(sp, tp), P(sp, None), P(tp, None), P(), P(),
        P(sp, tp), P(sp, tp), P(tp, sp), P(), P(),
    )
    return jax.shard_map(
        body, mesh=fine, in_specs=placed, out_specs=P(("z", "y", "x", "c"), None), check_vma=False
    )
```

```python
import functools
import jax
import jax.numpy as jnp
import numpy as np
from jax import lax
from jax.experimental import pallas as pl
from jax.experimental.pallas import tpu as pltpu
from jax.sharding import Mesh, PartitionSpec as P


ALPHA = 8.0**0.25
EPSILON = 1e-05
F32 = jnp.float32
BF16 = jnp.bfloat16

ROWS = 768
SUB = 192
HALF = 96
HD = 64
NSH = 16
PACK = 800
TILE = 256
TILES = SUB * NSH // TILE


def vmem():
    return pl.BlockSpec(memory_space=pltpu.VMEM)


def smem():
    return pl.BlockSpec(memory_space=pltpu.SMEM)


def params(mb=60):
    return pltpu.CompilerParams(vmem_limit_bytes=mb * 1024 * 1024)


def pack_kernel(q_ref, k_ref, v_ref, g_ref, qo_ref, kvo_ref):
    for h in range(4):
        cols = slice(h * HD, (h + 1) * HD)
        kvo_ref[h, 0:ROWS, 0:HD] = k_ref[:, cols]
        kvo_ref[h, 0:ROWS, HD : 2 * HD] = v_ref[:, cols]
        for y in range(4):
            at = y * SUB
            qo_ref[h * 4 + y, :, 0:HD] = q_ref[at : at + HALF, cols]
            qo_ref[h * 4 + y, :, HD : 2 * HD] = q_ref[at + HALF : at + SUB, cols]
        chunks = [-g_ref[h : h + 1, c * 128 : (c + 1) * 128] for c in range(6)]
        value = jnp.concatenate(chunks, axis=0)
        first = value.astype(BF16).astype(F32)
        second = (value - first).astype(BF16).astype(F32)
        third = value - first - second
        rest = jnp.zeros((PACK - ROWS - 18, 128), F32)
        kvo_ref[h, ROWS:PACK, :] = jnp.concatenate(
            [first, second, third, rest], axis=0
        ).astype(BF16)


def pack(q, k, v, g):
    return pl.pallas_call(
        pack_kernel,
        out_shape=(
            jax.ShapeDtypeStruct((NSH, HALF, 128), BF16),
            jax.ShapeDtypeStruct((4, PACK, 128), BF16),
        ),
        in_specs=[vmem()] * 4,
        out_specs=(vmem(), vmem()),
        compiler_params=params(),
        cost_estimate=pl.CostEstimate(flops=10**6, bytes_accessed=2500000, transcendentals=0),
    )(q, k, v, g)


def unit_table(steps):
    tables, counts = [], []
    for y in range(4):
        units = []
        for t in range(TILES):
            low = (TILE * t) // SUB
            for i, d in enumerate(steps):
                for z in range(4):
                    s = z * 4 + (y + d) % 4
                    if s <= low + 1:
                        units.append((t, i * 4 + z, s, int(s >= low)))
        if len(units) % 2:
            units.append((0, 0, NSH - 1, 1))
        counts.append(len(units))
        tables.append([(0, 0, 0, 0)] + units + [units[-1]])
    width = max(len(u) for u in tables) + 1
    out = np.zeros((4, 4, width), np.int32)
    for y in range(4):
        out[y, :, : len(tables[y])] = np.array(tables[y], np.int32).T
        out[y, :, -1] = counts[y]
    return out


def attend_kernel(chunks, first, final, *refs):
    refs = list(refs)
    tab, y_ref = refs[:2]
    kv_refs = refs[2 : 2 + chunks]
    at = 2 + chunks
    if first:
        q_ref, qt, top, acc = refs[at : at + 4]
        at += 4
    else:
        qt, top_in, acc_in = refs[at : at + 3]
        at += 3
        if final:
            o_ref = refs[at]
            at += 1
        else:
            top, acc = refs[at : at + 2]
            at += 2
    kaug, vt, qpos, s_a, s_b, p_a, p_b, al_a, al_b = refs[at : at + 9]
    at += 9
    if first:
        qrow = refs[at]
    if final:
        top, acc, oscr = refs[at : at + 3]
    y = y_ref[0]
    lane = lax.broadcasted_iota(jnp.int32, (128, 128), 1)
    for i in range(chunks):
        kv_ref = kv_refs[i]

        def per_shard(s, carry):
            gates = kv_ref[s, ROWS:PACK, :].astype(F32)
            square = jnp.concatenate(
                [jnp.zeros((HD, 128), F32), gates, jnp.zeros((32, 128), F32)], axis=0
            )
            turned = square.T
            to = i * 4 + s
            for c in range(6):
                part = kv_ref[s, c * 128 : (c + 1) * 128, :].astype(F32)
                mine = (lane == HD + c) | (lane == HD + 6 + c) | (lane == HD + 12 + c)
                kaug[to, c * 128 : (c + 1) * 128, :] = jnp.where(
                    lane < HD, part, jnp.where(mine, turned, 0.0)
                ).astype(BF16)
                vt[to, :, c * 128 : (c + 1) * 128] = part.T.astype(BF16)
            vt[to, 48:64, :] = jnp.ones((16, ROWS), BF16)
            return carry

        lax.fori_loop(0, 4, per_shard, 0)

    lane_h = lax.broadcasted_iota(jnp.int32, (HALF, 128), 1)
    lane_t = lax.broadcasted_iota(jnp.int32, (8, TILE), 1)
    if first:

        def per_query(s, carry):
            both = q_ref[s].astype(F32) * (HD**-0.5)
            ones = jnp.where(lane_h < HD + 18, 1.0, 0.0)
            qrow[s, 0:HALF, :] = jnp.where(lane_h < HD, both, ones)
            qrow[s, HALF:SUB, :] = jnp.where(lane_h < HD, pltpu.roll(both, HD, 1), ones)
            return carry

        lax.fori_loop(0, NSH, per_query, 0)
    for t in range(TILES):
        low = (TILE * t) // SUB
        edge = (low + 1) * SUB - TILE * t
        qpos[t] = y * SUB + jnp.where(
            lane_t < edge,
            low * ROWS + (SUB - edge) + lane_t,
            (low + 1) * ROWS + lane_t - edge,
        )
        if first:
            rows = jnp.concatenate(
                [qrow[low, SUB - edge : SUB, :], qrow[low + 1, 0 : TILE - edge, :]], axis=0
            )
            qt[t] = rows.T.astype(BF16)
    if first:
        acc[...] = jnp.zeros(acc.shape, F32)
        top[...] = jnp.full(top.shape, -1e30, F32)
    else:
        acc[...] = acc_in[...]
        top[...] = top_in[...]
    al_b[...] = jnp.ones(al_b.shape, F32)
    p_b[...] = jnp.zeros(p_b.shape, BF16)

    def scores(u, out):
        out[...] = jnp.dot(kaug[tab[y, 1, u]], qt[tab[y, 0, u]], preferred_element_type=F32)

    def gather(u, p_before, al_before):
        t = tab[y, 0, u]
        pv = jnp.dot(vt[tab[y, 1, u], 48:128, :], p_before[...], preferred_element_type=F32)
        acc[t] = acc[t] * al_before[0:1, :] + pv

    scores(1, s_a)

    def unit(u, s_now, s_next, p_before, p_now, al_before, al_now):
        def work(masked):
            scores(u + 1, s_next)
            gather(u - 1, p_before, al_before)
            t = tab[y, 0, u]
            before = top[t, 0:1, :]
            s = s_now[...]
            if masked:
                pos = tab[y, 2, u] * ROWS + lax.broadcasted_iota(jnp.int32, (ROWS, TILE), 0)
                s = jnp.where(pos <= qpos[t, 0:1, :], s, -1e30)
            high = jnp.maximum(before, jnp.max(s, axis=0, keepdims=True))
            p_now[...] = jnp.exp(s - high).astype(BF16)
            top[t, 0:1, :] = high
            al_now[0:1, :] = jnp.exp(before - high)

        lax.cond(tab[y, 3, u] == 1, lambda: work(True), lambda: work(False))

    def pair(i, carry):
        unit(2 * i + 1, s_a, s_b, p_b, p_a, al_b, al_a)
        unit(2 * i + 2, s_b, s_a, p_a, p_b, al_a, al_b)
        return carry

    count = tab[y, 0, tab.shape[2] - 1]
    lax.fori_loop(0, count // 2, pair, 0)
    gather(count, p_b, al_b)

    if final:

        def finish(t, carry):
            good = acc[t, 16:80, :] / acc[t, 0:1, :]
            full = jnp.concatenate([good, jnp.zeros((HD, TILE), F32)], axis=0)
            oscr[pl.ds(pl.multiple_of(t * TILE, TILE), TILE), :] = full.T
            return carry

        lax.fori_loop(0, TILES, finish, 0)

        def out(s, carry):
            row = pl.multiple_of(s * SUB, SUB)
            one = oscr[pl.ds(row, HALF), :]
            two = oscr[pl.ds(row + HALF, HALF), :]
            o_ref[s] = jnp.where(lane_h < HD, one, pltpu.roll(two, HD, 1)).astype(BF16)
            return carry

        lax.fori_loop(0, NSH, out, 0)


def attend(y, steps, kvs, q=None, state=None, final=False):
    chunks, first = len(kvs), q is not None
    state_shapes = (
        jax.ShapeDtypeStruct((TILES, 8, TILE), F32),
        jax.ShapeDtypeStruct((TILES, 80, TILE), F32),
    )
    scratch = [
        pltpu.VMEM((4 * chunks, ROWS, 128), BF16),
        pltpu.VMEM((4 * chunks, 128, ROWS), BF16),
        pltpu.VMEM((TILES, 8, TILE), jnp.int32),
        pltpu.VMEM((ROWS, TILE), F32),
        pltpu.VMEM((ROWS, TILE), F32),
        pltpu.VMEM((ROWS, TILE), BF16),
        pltpu.VMEM((ROWS, TILE), BF16),
        pltpu.VMEM((8, TILE), F32),
        pltpu.VMEM((8, TILE), F32),
    ]
    if first:
        outs = (jax.ShapeDtypeStruct((TILES, 128, TILE), BF16),) + state_shapes
        scratch += [pltpu.VMEM((NSH, SUB, 128), F32)]
        rest = [q]
    elif final:
        outs = jax.ShapeDtypeStruct((NSH, HALF, 128), BF16)
        scratch += [pltpu.VMEM(s.shape, F32) for s in state_shapes]
        scratch += [pltpu.VMEM((SUB * NSH, 128), F32)]
        rest = list(state)
    else:
        outs = state_shapes
        rest = list(state)
    table = unit_table(steps)
    share = int(table[:, 0, -1].mean())
    return pl.pallas_call(
        functools.partial(attend_kernel, chunks, first, final),
        out_shape=outs,
        in_specs=[smem(), smem()] + [vmem()] * (chunks + len(rest)),
        out_specs=jax.tree.map(lambda _: vmem(), outs),
        scratch_shapes=scratch,
        compiler_params=params(),
        cost_estimate=pl.CostEstimate(
            flops=share * 4 * 10**8, bytes_accessed=3 * 10**6, transcendentals=share * 200000
        ),
    )(jnp.asarray(table), y, *kvs, *rest)


def spread_kernel(o_ref, a_ref):
    for z in range(4):
        for y in range(4):
            for half in range(2):
                a_ref[2 * y + half, :, z * HD : (z + 1) * HD] = o_ref[
                    4 * z + y, :, half * HD : (half + 1) * HD
                ]


def spread(o):
    return pl.pallas_call(
        spread_kernel,
        out_shape=jax.ShapeDtypeStruct((8, HALF, 256), BF16),
        in_specs=[vmem()],
        out_specs=vmem(),
        compiler_params=params(),
        cost_estimate=pl.CostEstimate(flops=10**5, bytes_accessed=800000, transcendentals=0),
    )(o)


def norm_rows(matrix, gain, shift):
    centred = matrix - jnp.mean(matrix, axis=-1, keepdims=True)
    spread_ = jnp.mean(centred * centred, axis=-1, keepdims=True)
    return centred * lax.rsqrt(spread_ + EPSILON) * gain + shift


def mix_kernel(place, a_ref, stream_ref, gain_ref, bias_ref, *rest):
    w_refs, n_ref = rest[:8], rest[8]
    total = None
    for i in range(8):
        term = jnp.dot(a_ref[place[i]], w_refs[i][...], preferred_element_type=F32)
        total = term if total is None else total + term
    mixed = total.astype(BF16).astype(F32)
    matrix = ALPHA * stream_ref[...].astype(F32) + mixed
    n_ref[...] = norm_rows(matrix, gain_ref[...], bias_ref[...]).astype(BF16)


def mix(place, att, stream, gain, bias, weights):
    def whole(shape):
        return pl.BlockSpec(shape, lambda i, place: (0,) * len(shape))

    return pl.pallas_call(
        mix_kernel,
        out_shape=jax.ShapeDtypeStruct((HALF, 2048), BF16),
        grid_spec=pltpu.PrefetchScalarGridSpec(
            num_scalar_prefetch=1,
            grid=(1,),
            in_specs=[
                whole((8, HALF, 256)),
                pl.BlockSpec((HALF, 2048), lambda i, place: (place[8], 0)),
                whole((1, 2048)),
                whole((1, 2048)),
            ]
            + [whole((256, 2048))] * 8,
            out_specs=whole((HALF, 2048)),
        ),
        compiler_params=params(),
        cost_estimate=pl.CostEstimate(
            flops=2 * HALF * 2048 * 2048, bytes_accessed=9 * 10**6, transcendentals=0
        ),
    )(place, att, stream, gain, bias, *weights)


def ffn_kernel(x_ref, w_ref, out_ref, w_in, w_out, h_scr):
    @pl.when(pl.program_id(0) == 0)
    def _():
        for s in range(NSH):
            w_in[:, s * 128 : (s + 1) * 128] = w_ref[s, 0:1408, :]
            w_out[:, s * 128 : (s + 1) * 128] = w_ref[s, 1408:2112, :]

    both = lax.dot_general(
        x_ref[...], w_in[...], (((1,), (1,)), ((), ())), preferred_element_type=F32
    )
    gate, up = both[:, 0:704], both[:, 704:1408]
    h_scr[...] = (gate / (1.0 + jnp.exp(-gate)) * up).astype(BF16)
    out_ref[...] = jnp.dot(h_scr[...], w_out[...], preferred_element_type=F32).astype(BF16)


def ffn(x, w, tile=192):
    return pl.pallas_call(
        ffn_kernel,
        out_shape=jax.ShapeDtypeStruct((ROWS, 2048), BF16),
        grid=(ROWS // tile,),
        in_specs=[
            pl.BlockSpec((tile, 2048), lambda i: (i, 0)),
            pl.BlockSpec((NSH, 2112, 128), lambda i: (0, 0, 0)),
        ],
        out_specs=pl.BlockSpec((tile, 2048), lambda i: (i, 0)),
        scratch_shapes=[
            pltpu.VMEM((1408, 2048), BF16),
            pltpu.VMEM((704, 2048), BF16),
            pltpu.VMEM((tile, 704), BF16),
        ],
        compiler_params=params(),
        cost_estimate=pl.CostEstimate(
            flops=6 * ROWS * 2048 * 704, bytes_accessed=15 * 10**6, transcendentals=10**6
        ),
    )(x, w)


def last_kernel(p_ref, n_ref, gain_ref, bias_ref, o_ref):
    total = p_ref[0].astype(F32)
    for i in range(1, 8):
        total = total + p_ref[i].astype(F32)
    lowered = total.astype(BF16).astype(F32)
    matrix = ALPHA * n_ref[...].astype(F32) + lowered
    o_ref[...] = norm_rows(matrix, gain_ref[...], bias_ref[...]).astype(BF16)


def last(parts, normed, gain, bias):
    return pl.pallas_call(
        last_kernel,
        out_shape=jax.ShapeDtypeStruct((HALF, 2048), BF16),
        in_specs=[vmem()] * 4,
        out_specs=vmem(),
        compiler_params=params(),
        cost_estimate=pl.CostEstimate(
            flops=4 * 10**6, bytes_accessed=4 * 10**6, transcendentals=0
        ),
    )(parts, normed, gain, bias)


def body(
    queries, key_rows, value_rows, log_forget, stream_in, out_weight, mix_gain, mix_bias,
    gate_weight, up_weight, down_weight, ffn_gain, ffn_bias,
):
    yi = lax.axis_index("y").astype(jnp.int32)[None]
    xi = lax.axis_index("x")
    ci = lax.axis_index("c")

    def turn(value, axis, d):
        return lax.ppermute(value, axis, [(i, (i + d) % 4) for i in range(4)])

    q_pack, kv_pack = pack(queries, key_rows, value_rows, log_forget.T)
    kv_own = lax.all_to_all(kv_pack, "z", split_axis=0, concat_axis=0, tiled=True)
    q_mine = lax.all_to_all(q_pack, ("z", "y"), split_axis=0, concat_axis=0, tiled=True)
    kv_back, kv_ahead = turn(kv_own, "y", 1), turn(kv_own, "y", 3)
    kv_far = turn(kv_own, "y", 2)

    shards = jnp.concatenate([gate_weight.T, up_weight.T, down_weight], axis=0)
    ffn_all = lax.all_gather(shards, ("z", "y"), axis=0, tiled=False)

    weights, places = [out_weight], [2 * xi + ci]
    for d in (1, 3, 2):
        weights.append(turn(out_weight, "x", d))
        places.append(2 * ((xi + 4 - d) % 4) + ci)
    for i in range(4):
        weights.append(lax.ppermute(weights[i], "c", [(0, 1), (1, 0)]))
        places.append(places[i] + 1 - 2 * ci)
    own = 2 * xi + ci
    place = jnp.stack(places + [own]).astype(jnp.int32)

    qt, *state = attend(yi, (0,), [kv_own], q=q_mine)
    state = attend(yi, (3, 1), [kv_back, kv_ahead], state=(qt, *state))
    attended = attend(yi, (2,), [kv_far], state=(qt, *state), final=True)
    by_shard = lax.all_to_all(attended, ("z", "y"), split_axis=0, concat_axis=0, tiled=True)
    by_rows = lax.all_to_all(
        spread(by_shard), ("x", "c"), split_axis=0, concat_axis=0, tiled=True
    )
    normed = mix(place, by_rows, stream_in, mix_gain[None], mix_bias[None], weights)
    gathered = lax.all_gather(normed, ("x", "c"), axis=0, tiled=True)
    partial = ffn(gathered, ffn_all)
    parts = lax.all_to_all(
        partial.reshape(8, HALF, 2048), ("x", "c"), split_axis=0, concat_axis=0, tiled=True
    )
    return last(parts, normed, ffn_gain[None], ffn_bias[None])


def solution(mesh):
    fine = Mesh(mesh.devices.reshape(4, 4, 4, 2), ("z", "y", "x", "c"))
    sp, tp = ("z", "y"), ("x", "c")
    placed = (
        P(sp, tp), P(sp, tp), P(sp, tp), P(sp, tp), P(sp, None), P(tp, None), P(), P(),
        P(sp, tp), P(sp, tp), P(tp, sp), P(), P(),
    )

    return jax.shard_map(
        body, mesh=fine, in_specs=placed, out_specs=P(("z", "y", "x", "c"), None), check_vma=False
    )
```

```python
import functools
import jax
import jax.numpy as jnp
import numpy as np
from jax import lax
from jax.experimental import pallas as pl
from jax.experimental.pallas import tpu as pltpu
from jax.sharding import Mesh, PartitionSpec as P


ALPHA = 8.0**0.25
EPSILON = 1e-05
F32 = jnp.float32
BF16 = jnp.bfloat16

ROWS = 768
SUB = 192
HALF = 96
HD = 64
NSH = 16
PACK = 800
TILE = 256
TILES = SUB * NSH // TILE


def vmem():
    return pl.BlockSpec(memory_space=pltpu.VMEM)


def smem():
    return pl.BlockSpec(memory_space=pltpu.SMEM)


def params(mb=60):
    return pltpu.CompilerParams(vmem_limit_bytes=mb * 1024 * 1024)


def pack_kernel(q_ref, k_ref, v_ref, g_ref, qo_ref, kvo_ref):
    for h in range(4):
        cols = slice(h * HD, (h + 1) * HD)
        kvo_ref[h, 0:ROWS, 0:HD] = k_ref[:, cols]
        kvo_ref[h, 0:ROWS, HD : 2 * HD] = v_ref[:, cols]
        for y in range(4):
            at = y * SUB
            qo_ref[h * 4 + y, :, 0:HD] = q_ref[at : at + HALF, cols]
            qo_ref[h * 4 + y, :, HD : 2 * HD] = q_ref[at + HALF : at + SUB, cols]
        chunks = [-g_ref[h : h + 1, c * 128 : (c + 1) * 128] for c in range(6)]
        value = jnp.concatenate(chunks, axis=0)
        first = value.astype(BF16).astype(F32)
        second = (value - first).astype(BF16).astype(F32)
        third = value - first - second
        rest = jnp.zeros((PACK - ROWS - 18, 128), F32)
        kvo_ref[h, ROWS:PACK, :] = jnp.concatenate(
            [first, second, third, rest], axis=0
        ).astype(BF16)


def pack(q, k, v, g):
    return pl.pallas_call(
        pack_kernel,
        out_shape=(
            jax.ShapeDtypeStruct((NSH, HALF, 128), BF16),
            jax.ShapeDtypeStruct((4, PACK, 128), BF16),
        ),
        in_specs=[vmem()] * 4,
        out_specs=(vmem(), vmem()),
        compiler_params=params(),
        cost_estimate=pl.CostEstimate(flops=10**6, bytes_accessed=2500000, transcendentals=0),
    )(q, k, v, g)


def unit_table(steps):
    tables, counts = [], []
    for y in range(4):
        units = []
        for t in range(TILES):
            low = (TILE * t) // SUB
            for i, d in enumerate(steps):
                for z in range(4):
                    s = z * 4 + (y + d) % 4
                    if s <= low + 1:
                        units.append((t, i * 4 + z, s, int(s >= low)))
        if len(units) % 2:
            units.append((0, 0, NSH - 1, 1))
        counts.append(len(units))
        tables.append([(0, 0, 0, 0)] + units + [units[-1]])
    width = max(len(u) for u in tables) + 1
    out = np.zeros((4, 4, width), np.int32)
    for y in range(4):
        out[y, :, : len(tables[y])] = np.array(tables[y], np.int32).T
        out[y, :, -1] = counts[y]
    return out


def attend_kernel(chunks, first, final, *refs):
    refs = list(refs)
    tab, y_ref = refs[:2]
    kv_refs = refs[2 : 2 + chunks]
    at = 2 + chunks
    if first:
        q_ref, qt, top, acc = refs[at : at + 4]
        at += 4
    else:
        qt, top_in, acc_in = refs[at : at + 3]
        at += 3
        if final:
            o_ref = refs[at]
            at += 1
        else:
            top, acc = refs[at : at + 2]
            at += 2
    kaug, vt, qpos, s_a, s_b, p_a, p_b, al_a, al_b = refs[at : at + 9]
    at += 9
    if first:
        qrow = refs[at]
    if final:
        top, acc, oscr = refs[at : at + 3]
    y = y_ref[0]
    lane = lax.broadcasted_iota(jnp.int32, (128, 128), 1)
    for i in range(chunks):
        kv_ref = kv_refs[i]

        def per_shard(s, carry):
            gates = kv_ref[s, ROWS:PACK, :].astype(F32)
            square = jnp.concatenate(
                [jnp.zeros((HD, 128), F32), gates, jnp.zeros((32, 128), F32)], axis=0
            )
            turned = square.T
            to = i * 4 + s
            for c in range(6):
                part = kv_ref[s, c * 128 : (c + 1) * 128, :].astype(F32)
                mine = (lane == HD + c) | (lane == HD + 6 + c) | (lane == HD + 12 + c)
                kaug[to, c * 128 : (c + 1) * 128, :] = jnp.where(
                    lane < HD, part, jnp.where(mine, turned, 0.0)
                ).astype(BF16)
                vt[to, :, c * 128 : (c + 1) * 128] = part.T.astype(BF16)
            vt[to, 48:64, :] = jnp.ones((16, ROWS), BF16)
            return carry

        lax.fori_loop(0, 4, per_shard, 0)

    lane_h = lax.broadcasted_iota(jnp.int32, (HALF, 128), 1)
    lane_t = lax.broadcasted_iota(jnp.int32, (8, TILE), 1)
    if first:

        def per_query(s, carry):
            both = q_ref[s].astype(F32) * (HD**-0.5)
            ones = jnp.where(lane_h < HD + 18, 1.0, 0.0)
            qrow[s, 0:HALF, :] = jnp.where(lane_h < HD, both, ones)
            qrow[s, HALF:SUB, :] = jnp.where(lane_h < HD, pltpu.roll(both, HD, 1), ones)
            return carry

        lax.fori_loop(0, NSH, per_query, 0)
    for t in range(TILES):
        low = (TILE * t) // SUB
        edge = (low + 1) * SUB - TILE * t
        qpos[t] = y * SUB + jnp.where(
            lane_t < edge,
            low * ROWS + (SUB - edge) + lane_t,
            (low + 1) * ROWS + lane_t - edge,
        )
        if first:
            rows = jnp.concatenate(
                [qrow[low, SUB - edge : SUB, :], qrow[low + 1, 0 : TILE - edge, :]], axis=0
            )
            qt[t] = rows.T.astype(BF16)
    if first:
        acc[...] = jnp.zeros(acc.shape, F32)
        top[...] = jnp.full(top.shape, -1e30, F32)
    else:
        acc[...] = acc_in[...]
        top[...] = top_in[...]
    al_b[...] = jnp.ones(al_b.shape, F32)
    p_b[...] = jnp.zeros(p_b.shape, BF16)

    def scores(u, out):
        out[...] = jnp.dot(kaug[tab[y, 1, u]], qt[tab[y, 0, u]], preferred_element_type=F32)

    def gather(u, p_before, al_before):
        t = tab[y, 0, u]
        pv = jnp.dot(vt[tab[y, 1, u], 48:128, :], p_before[...], preferred_element_type=F32)
        acc[t] = acc[t] * al_before[0:1, :] + pv

    scores(1, s_a)

    def unit(u, s_now, s_next, p_before, p_now, al_before, al_now):
        def work(masked):
            scores(u + 1, s_next)
            gather(u - 1, p_before, al_before)
            t = tab[y, 0, u]
            before = top[t, 0:1, :]
            s = s_now[...]
            if masked:
                pos = tab[y, 2, u] * ROWS + lax.broadcasted_iota(jnp.int32, (ROWS, TILE), 0)
                s = jnp.where(pos <= qpos[t, 0:1, :], s, -1e30)
            high = jnp.maximum(before, jnp.max(s, axis=0, keepdims=True))
            p_now[...] = jnp.exp(s - high).astype(BF16)
            top[t, 0:1, :] = high
            al_now[0:1, :] = jnp.exp(before - high)

        lax.cond(tab[y, 3, u] == 1, lambda: work(True), lambda: work(False))

    def pair(i, carry):
        unit(2 * i + 1, s_a, s_b, p_b, p_a, al_b, al_a)
        unit(2 * i + 2, s_b, s_a, p_a, p_b, al_a, al_b)
        return carry

    count = tab[y, 0, tab.shape[2] - 1]
    lax.fori_loop(0, count // 2, pair, 0)
    gather(count, p_b, al_b)

    if final:

        def finish(t, carry):
            good = acc[t, 16:80, :] / acc[t, 0:1, :]
            full = jnp.concatenate([good, jnp.zeros((HD, TILE), F32)], axis=0)
            oscr[pl.ds(pl.multiple_of(t * TILE, TILE), TILE), :] = full.T
            return carry

        lax.fori_loop(0, TILES, finish, 0)

        def out(s, carry):
            row = pl.multiple_of(s * SUB, SUB)
            one = oscr[pl.ds(row, HALF), :]
            two = oscr[pl.ds(row + HALF, HALF), :]
            o_ref[s] = jnp.where(lane_h < HD, one, pltpu.roll(two, HD, 1)).astype(BF16)
            return carry

        lax.fori_loop(0, NSH, out, 0)


def attend(y, steps, kvs, q=None, state=None, final=False):
    chunks, first = len(kvs), q is not None
    state_shapes = (
        jax.ShapeDtypeStruct((TILES, 8, TILE), F32),
        jax.ShapeDtypeStruct((TILES, 80, TILE), F32),
    )
    scratch = [
        pltpu.VMEM((4 * chunks, ROWS, 128), BF16),
        pltpu.VMEM((4 * chunks, 128, ROWS), BF16),
        pltpu.VMEM((TILES, 8, TILE), jnp.int32),
        pltpu.VMEM((ROWS, TILE), F32),
        pltpu.VMEM((ROWS, TILE), F32),
        pltpu.VMEM((ROWS, TILE), BF16),
        pltpu.VMEM((ROWS, TILE), BF16),
        pltpu.VMEM((8, TILE), F32),
        pltpu.VMEM((8, TILE), F32),
    ]
    if first:
        outs = (jax.ShapeDtypeStruct((TILES, 128, TILE), BF16),) + state_shapes
        scratch += [pltpu.VMEM((NSH, SUB, 128), F32)]
        rest = [q]
    elif final:
        outs = jax.ShapeDtypeStruct((NSH, HALF, 128), BF16)
        scratch += [pltpu.VMEM(s.shape, F32) for s in state_shapes]
        scratch += [pltpu.VMEM((SUB * NSH, 128), F32)]
        rest = list(state)
    else:
        outs = state_shapes
        rest = list(state)
    table = unit_table(steps)
    share = int(table[:, 0, -1].mean())
    return pl.pallas_call(
        functools.partial(attend_kernel, chunks, first, final),
        out_shape=outs,
        in_specs=[smem(), smem()] + [vmem()] * (chunks + len(rest)),
        out_specs=jax.tree.map(lambda _: vmem(), outs),
        scratch_shapes=scratch,
        compiler_params=params(),
        cost_estimate=pl.CostEstimate(
            flops=share * 4 * 10**8, bytes_accessed=3 * 10**6, transcendentals=share * 200000
        ),
    )(jnp.asarray(table), y, *kvs, *rest)


def spread_kernel(o_ref, a_ref):
    for z in range(4):
        for y in range(4):
            for half in range(2):
                a_ref[2 * y + half, :, z * HD : (z + 1) * HD] = o_ref[
                    4 * z + y, :, half * HD : (half + 1) * HD
                ]


def spread(o):
    return pl.pallas_call(
        spread_kernel,
        out_shape=jax.ShapeDtypeStruct((8, HALF, 256), BF16),
        in_specs=[vmem()],
        out_specs=vmem(),
        compiler_params=params(),
        cost_estimate=pl.CostEstimate(flops=10**5, bytes_accessed=800000, transcendentals=0),
    )(o)


def norm_rows(matrix, gain, shift):
    centred = matrix - jnp.mean(matrix, axis=-1, keepdims=True)
    spread_ = jnp.mean(centred * centred, axis=-1, keepdims=True)
    return centred * lax.rsqrt(spread_ + EPSILON) * gain + shift


def mix_kernel(place, a_ref, stream_ref, gain_ref, bias_ref, same_ref, other_ref, n_ref, total):
    c, x = place[0], pl.program_id(0)
    term = jnp.dot(a_ref[2 * x + c], same_ref[0], preferred_element_type=F32)
    term = term + jnp.dot(a_ref[2 * x + 1 - c], other_ref[0], preferred_element_type=F32)

    @pl.when(x == 0)
    def _():
        total[...] = term

    @pl.when(x > 0)
    def _():
        total[...] += term

    @pl.when(x == 3)
    def _():
        mixed = total[...].astype(BF16).astype(F32)
        matrix = ALPHA * stream_ref[...].astype(F32) + mixed
        n_ref[...] = norm_rows(matrix, gain_ref[...], bias_ref[...]).astype(BF16)


def whole(shape):
    return pl.BlockSpec(shape, lambda i, place: (0,) * len(shape))


def along(shape):
    return pl.BlockSpec((1, *shape), lambda i, place: (i,) + (0,) * len(shape))


def mix(place, att, stream, gain, bias, same, other):
    return pl.pallas_call(
        mix_kernel,
        out_shape=jax.ShapeDtypeStruct((HALF, 2048), BF16),
        grid_spec=pltpu.PrefetchScalarGridSpec(
            num_scalar_prefetch=1,
            grid=(4,),
            in_specs=[
                whole((8, HALF, 256)),
                pl.BlockSpec((HALF, 2048), lambda i, place: (place[1], 0)),
                whole((1, 2048)),
                whole((1, 2048)),
                along((256, 2048)),
                along((256, 2048)),
            ],
            out_specs=whole((HALF, 2048)),
            scratch_shapes=[pltpu.VMEM((HALF, 2048), F32)],
        ),
        compiler_params=params(),
        cost_estimate=pl.CostEstimate(
            flops=2 * HALF * 2048 * 2048, bytes_accessed=9 * 10**6, transcendentals=0
        ),
    )(place, att, stream, gain, bias, same, other)


BLOCKS = 3


def prepare_kernel(w_ref, in_ref, out_ref):
    for j in range(BLOCKS):
        live = min(256, 704 - 256 * j)
        for part in range(2):
            at = 704 * part + 256 * j
            in_ref[j, :, 256 * part : 256 * part + live] = w_ref[0, at : at + live, :].T
            if live < 256:
                in_ref[j, :, 256 * part + live : 256 * part + 256] = jnp.zeros(
                    (128, 256 - live), BF16
                )
        at = 1408 + 256 * j
        out_ref[j, 0:live, :] = w_ref[0, at : at + live, :]
        if live < 256:
            out_ref[j, live:256, :] = jnp.zeros((256 - live, 128), BF16)


def prepare(w):
    return pl.pallas_call(
        prepare_kernel,
        out_shape=(
            jax.ShapeDtypeStruct((BLOCKS, 2048, 512), BF16),
            jax.ShapeDtypeStruct((BLOCKS, 256, 2048), BF16),
        ),
        grid=(NSH,),
        in_specs=[pl.BlockSpec((1, 2112, 128), lambda s: (s, 0, 0))],
        out_specs=(
            pl.BlockSpec((BLOCKS, 128, 512), lambda s: (0, s, 0)),
            pl.BlockSpec((BLOCKS, 256, 128), lambda s: (0, 0, s)),
        ),
        compiler_params=params(),
        cost_estimate=pl.CostEstimate(
            flops=10**9, bytes_accessed=17 * 10**6, transcendentals=0
        ),
    )(w)


def ffn_kernel(count, place, *refs):
    x_refs = refs[: 2 * count]
    in_ref, out_ref, same_ref, other_ref, total = refs[2 * count :]
    j = pl.program_id(0)
    x = jnp.concatenate([r[0] for r in x_refs], axis=0)
    both = jnp.dot(x, in_ref[0], preferred_element_type=F32)
    gate, up = both[:, 0:256], both[:, 256:512]
    hidden = (gate / (1.0 + jnp.exp(-gate)) * up).astype(BF16)
    term = jnp.dot(hidden, out_ref[0], preferred_element_type=F32)

    @pl.when(j == 0)
    def _():
        total[...] = term

    @pl.when(j == 1)
    def _():
        total[...] += term

    @pl.when(j == BLOCKS - 1)
    def _():
        out = (total[...] + term).astype(BF16)
        for i in range(count):
            same_ref[i] = out[i * HALF : (i + 1) * HALF]
            other_ref[i] = out[(count + i) * HALF : (count + i + 1) * HALF]


def ffn(count, place, gathered, w_in, w_out):
    def block(i):
        return pl.BlockSpec((1, HALF, 2048), lambda g, place: (place[i], 0, 0))

    shape = jax.ShapeDtypeStruct((count, HALF, 2048), BF16)
    rows = 2 * count * HALF
    return pl.pallas_call(
        functools.partial(ffn_kernel, count),
        out_shape=(shape, shape),
        grid_spec=pltpu.PrefetchScalarGridSpec(
            num_scalar_prefetch=1,
            grid=(BLOCKS,),
            in_specs=[block(i) for i in range(2 * count)]
            + [along((2048, 512)), along((256, 2048))],
            out_specs=(whole((count, HALF, 2048)),) * 2,
            scratch_shapes=[pltpu.VMEM((rows, 2048), F32)],
        ),
        compiler_params=params(),
        cost_estimate=pl.CostEstimate(
            flops=6 * rows * 2048 * 704, bytes_accessed=10**7, transcendentals=rows * 704
        ),
    )(place, *([gathered] * (2 * count)), w_in, w_out)


def last_kernel(n_ref, gain_ref, bias_ref, *refs):
    o_ref = refs[-1]
    total = refs[0][...].astype(F32)
    for r in refs[1:-1]:
        total = total + r[...].astype(F32)
    lowered = total.astype(BF16).astype(F32)
    matrix = ALPHA * n_ref[...].astype(F32) + lowered
    o_ref[...] = norm_rows(matrix, gain_ref[...], bias_ref[...]).astype(BF16)


def last(parts, normed, gain, bias):
    return pl.pallas_call(
        last_kernel,
        out_shape=jax.ShapeDtypeStruct((HALF, 2048), BF16),
        in_specs=[vmem()] * (3 + len(parts)),
        out_specs=vmem(),
        compiler_params=params(),
        cost_estimate=pl.CostEstimate(
            flops=4 * 10**6, bytes_accessed=4 * 10**6, transcendentals=0
        ),
    )(normed, gain, bias, *parts)


def body(
    queries, key_rows, value_rows, log_forget, stream_in, out_weight, mix_gain, mix_bias,
    gate_weight, up_weight, down_weight, ffn_gain, ffn_bias,
):
    yi = lax.axis_index("y").astype(jnp.int32)[None]
    xi = lax.axis_index("x")
    ci = lax.axis_index("c")

    def turn(value, axis, d):
        return lax.ppermute(value, axis, [(i, (i + d) % 4) for i in range(4)])

    def swap(value):
        return lax.ppermute(value, "c", [(0, 1), (1, 0)])

    q_pack, kv_pack = pack(queries, key_rows, value_rows, log_forget.T)
    kv_own = lax.all_to_all(kv_pack, "z", split_axis=0, concat_axis=0, tiled=True)
    q_mine = lax.all_to_all(q_pack, ("z", "y"), split_axis=0, concat_axis=0, tiled=True)
    kv_back, kv_ahead = turn(kv_own, "y", 1), turn(kv_own, "y", 3)
    kv_far = turn(kv_own, "y", 2)
    w_same = lax.all_gather(out_weight, "x", axis=0, tiled=False)
    w_other = swap(w_same)
    shards = jnp.concatenate([gate_weight.T, up_weight.T, down_weight], axis=0)
    ffn_all = lax.all_gather(shards, ("z", "y"), axis=0, tiled=False)

    qt, *state = attend(yi, (0,), [kv_own], q=q_mine)
    state = attend(yi, (3, 1), [kv_back, kv_ahead], state=(qt, *state))
    attended = attend(yi, (2,), [kv_far], state=(qt, *state), final=True)
    by_shard = lax.all_to_all(attended, ("z", "y"), split_axis=0, concat_axis=0, tiled=True)
    by_rows = lax.all_to_all(
        spread(by_shard), ("x", "c"), split_axis=0, concat_axis=0, tiled=True
    )
    place = jnp.stack([ci, 2 * xi + ci]).astype(jnp.int32)
    normed = mix(place, by_rows, stream_in, mix_gain[None], mix_bias[None], w_same, w_other)
    gathered = lax.all_gather(normed, ("x", "c"), axis=0, tiled=False)
    w_in, w_out = prepare(ffn_all)

    def chips(steps):
        at = [2 * ((xi + d) % 4) for d in steps]
        both = [i + ci for i in at] + [i + 1 - ci for i in at]
        return jnp.stack(both).astype(jnp.int32)

    def joined(one, two):
        return (one.astype(F32) + two.astype(F32)).astype(BF16)

    far_same, far_other = ffn(1, chips((2,)), gathered, w_in, w_out)
    far_swapped = swap(far_other)
    near_same, near_other = ffn(2, chips((1, 3)), gathered, w_in, w_out)
    near_swapped = swap(near_other)
    own_same, own_other = ffn(1, chips((0,)), gathered, w_in, w_out)
    own_swapped = swap(own_other)
    from_far = turn(joined(far_same[0], far_swapped[0]), "x", 2)
    from_back = turn(joined(near_same[0], near_swapped[0]), "x", 1)
    from_ahead = turn(joined(near_same[1], near_swapped[1]), "x", 3)
    parts = [own_same[0], own_swapped[0], from_back, from_ahead, from_far]
    return last(parts, normed, ffn_gain[None], ffn_bias[None])


def solution(mesh):
    fine = Mesh(mesh.devices.reshape(4, 4, 4, 2), ("z", "y", "x", "c"))
    sp, tp = ("z", "y"), ("x", "c")
    placed = (
        P(sp, tp), P(sp, tp), P(sp, tp), P(sp, tp), P(sp, None), P(tp, None), P(), P(),
        P(sp, tp), P(sp, tp), P(tp, sp), P(), P(),
    )

    return jax.shard_map(
        body, mesh=fine, in_specs=placed, out_specs=P(("z", "y", "x", "c"), None), check_vma=False
    )
```

```python
import functools
import jax
import jax.numpy as jnp
import numpy as np
from jax import lax
from jax.experimental import pallas as pl
from jax.experimental.pallas import tpu as pltpu
from jax.sharding import Mesh, PartitionSpec as P


ALPHA = 8.0**0.25
EPSILON = 1e-05
F32 = jnp.float32
BF16 = jnp.bfloat16

ROWS = 768
SUB = 192
HALF = 96
HD = 64
NSH = 16
PACK = 800
TILE = 256
TILES = SUB * NSH // TILE


def vmem():
    return pl.BlockSpec(memory_space=pltpu.VMEM)


def smem():
    return pl.BlockSpec(memory_space=pltpu.SMEM)


def params(mb):
    return pltpu.CompilerParams(vmem_limit_bytes=mb * 1024 * 1024)


def pack_kernel(q_ref, k_ref, v_ref, g_ref, qo_ref, kvo_ref):
    for h in range(4):
        cols = slice(h * HD, (h + 1) * HD)
        kvo_ref[h, 0:ROWS, 0:HD] = k_ref[:, cols]
        kvo_ref[h, 0:ROWS, HD : 2 * HD] = v_ref[:, cols]
        for y in range(4):
            at = y * SUB
            qo_ref[h * 4 + y, :, 0:HD] = q_ref[at : at + HALF, cols]
            qo_ref[h * 4 + y, :, HD : 2 * HD] = q_ref[at + HALF : at + SUB, cols]
        chunks = [-g_ref[h : h + 1, c * 128 : (c + 1) * 128] for c in range(6)]
        value = jnp.concatenate(chunks, axis=0)
        first = value.astype(BF16).astype(F32)
        second = (value - first).astype(BF16).astype(F32)
        third = value - first - second
        rest = jnp.zeros((PACK - ROWS - 18, 128), F32)
        kvo_ref[h, ROWS:PACK, :] = jnp.concatenate(
            [first, second, third, rest], axis=0
        ).astype(BF16)


def pack(q, k, v, g):
    return pl.pallas_call(
        pack_kernel,
        out_shape=(
            jax.ShapeDtypeStruct((NSH, HALF, 128), BF16),
            jax.ShapeDtypeStruct((4, PACK, 128), BF16),
        ),
        in_specs=[vmem()] * 4,
        out_specs=(vmem(), vmem()),
        compiler_params=params(60),
        cost_estimate=pl.CostEstimate(flops=10**6, bytes_accessed=2500000, transcendentals=0),
    )(q, k, v, g)


def unit_table(steps):
    tables, counts = [], []
    for y in range(4):
        units = []
        for t in range(TILES):
            low = (TILE * t) // SUB
            for i, d in enumerate(steps):
                for z in range(4):
                    s = z * 4 + (y + d) % 4
                    if s <= low + 1:
                        units.append((t, i * 4 + z, s, int(s >= low)))
        if len(units) % 2:
            units.append((0, 0, NSH - 1, 1))
        counts.append(len(units))
        tables.append([(0, 0, 0, 0)] + units + [units[-1]])
    width = max(len(u) for u in tables) + 1
    out = np.zeros((4, 4, width), np.int32)
    for y in range(4):
        out[y, :, : len(tables[y])] = np.array(tables[y], np.int32).T
        out[y, :, -1] = counts[y]
    return out


def attend_kernel(chunks, first, final, *refs):
    refs = list(refs)
    tab, y_ref = refs[:2]
    kv_refs = refs[2 : 2 + chunks]
    at = 2 + chunks
    if first:
        q_ref, qt, top, acc = refs[at : at + 4]
        at += 4
    else:
        qt, top_in, acc_in = refs[at : at + 3]
        at += 3
        if final:
            o_ref = refs[at]
            at += 1
        else:
            top, acc = refs[at : at + 2]
            at += 2
    kaug, vt, qpos, s_a, s_b, p_a, p_b, al_a, al_b = refs[at : at + 9]
    at += 9
    if first:
        qrow = refs[at]
    if final:
        top, acc, oscr = refs[at : at + 3]
    y = y_ref[0]
    lane = lax.broadcasted_iota(jnp.int32, (128, 128), 1)
    for i in range(chunks):
        kv_ref = kv_refs[i]

        def per_shard(s, carry):
            gates = kv_ref[s, ROWS:PACK, :].astype(F32)
            square = jnp.concatenate(
                [jnp.zeros((HD, 128), F32), gates, jnp.zeros((32, 128), F32)], axis=0
            )
            turned = square.T
            to = i * 4 + s
            for c in range(6):
                part = kv_ref[s, c * 128 : (c + 1) * 128, :].astype(F32)
                mine = (lane == HD + c) | (lane == HD + 6 + c) | (lane == HD + 12 + c)
                kaug[to, c * 128 : (c + 1) * 128, :] = jnp.where(
                    lane < HD, part, jnp.where(mine, turned, 0.0)
                ).astype(BF16)
                vt[to, :, c * 128 : (c + 1) * 128] = part.T.astype(BF16)
            vt[to, 48:64, :] = jnp.ones((16, ROWS), BF16)
            return carry

        lax.fori_loop(0, 4, per_shard, 0)

    lane_h = lax.broadcasted_iota(jnp.int32, (HALF, 128), 1)
    lane_t = lax.broadcasted_iota(jnp.int32, (8, TILE), 1)
    if first:

        def per_query(s, carry):
            both = q_ref[s].astype(F32) * (HD**-0.5)
            ones = jnp.where(lane_h < HD + 18, 1.0, 0.0)
            qrow[s, 0:HALF, :] = jnp.where(lane_h < HD, both, ones)
            qrow[s, HALF:SUB, :] = jnp.where(lane_h < HD, pltpu.roll(both, HD, 1), ones)
            return carry

        lax.fori_loop(0, NSH, per_query, 0)
    for t in range(TILES):
        low = (TILE * t) // SUB
        edge = (low + 1) * SUB - TILE * t
        qpos[t] = y * SUB + jnp.where(
            lane_t < edge,
            low * ROWS + (SUB - edge) + lane_t,
            (low + 1) * ROWS + lane_t - edge,
        )
        if first:
            rows = jnp.concatenate(
                [qrow[low, SUB - edge : SUB, :], qrow[low + 1, 0 : TILE - edge, :]], axis=0
            )
            qt[t] = rows.T.astype(BF16)
    if first:
        acc[...] = jnp.zeros(acc.shape, F32)
        top[...] = jnp.full(top.shape, -1e30, F32)
    else:
        acc[...] = acc_in[...]
        top[...] = top_in[...]
    al_b[...] = jnp.ones(al_b.shape, F32)
    p_b[...] = jnp.zeros(p_b.shape, BF16)

    def scores(u, out):
        out[...] = jnp.dot(kaug[tab[y, 1, u]], qt[tab[y, 0, u]], preferred_element_type=F32)

    def gather(u, p_before, al_before):
        t = tab[y, 0, u]
        pv = jnp.dot(vt[tab[y, 1, u], 48:128, :], p_before[...], preferred_element_type=F32)
        acc[t] = acc[t] * al_before[0:1, :] + pv

    scores(1, s_a)

    def unit(u, s_now, s_next, p_before, p_now, al_before, al_now):
        def work(masked):
            scores(u + 1, s_next)
            gather(u - 1, p_before, al_before)
            t = tab[y, 0, u]
            before = top[t, 0:1, :]
            s = s_now[...]
            if masked:
                pos = tab[y, 2, u] * ROWS + lax.broadcasted_iota(jnp.int32, (ROWS, TILE), 0)
                s = jnp.where(pos <= qpos[t, 0:1, :], s, -1e30)
            high = jnp.maximum(before, jnp.max(s, axis=0, keepdims=True))
            p_now[...] = jnp.exp(s - high).astype(BF16)
            top[t, 0:1, :] = high
            al_now[0:1, :] = jnp.exp(before - high)

        lax.cond(tab[y, 3, u] == 1, lambda: work(True), lambda: work(False))

    def pair(i, carry):
        unit(2 * i + 1, s_a, s_b, p_b, p_a, al_b, al_a)
        unit(2 * i + 2, s_b, s_a, p_a, p_b, al_a, al_b)
        return carry

    count = tab[y, 0, tab.shape[2] - 1]
    lax.fori_loop(0, count // 2, pair, 0)
    gather(count, p_b, al_b)

    if final:

        def finish(t, carry):
            good = acc[t, 16:80, :] / acc[t, 0:1, :]
            full = jnp.concatenate([good, jnp.zeros((HD, TILE), F32)], axis=0)
            oscr[pl.ds(pl.multiple_of(t * TILE, TILE), TILE), :] = full.T
            return carry

        lax.fori_loop(0, TILES, finish, 0)

        def out(s, carry):
            row = pl.multiple_of(s * SUB, SUB)
            one = oscr[pl.ds(row, HALF), :]
            two = oscr[pl.ds(row + HALF, HALF), :]
            o_ref[s] = jnp.where(lane_h < HD, one, pltpu.roll(two, HD, 1)).astype(BF16)
            return carry

        lax.fori_loop(0, NSH, out, 0)


def attend(y, steps, kvs, q=None, state=None, final=False):
    chunks, first = len(kvs), q is not None
    state_shapes = (
        jax.ShapeDtypeStruct((TILES, 8, TILE), F32),
        jax.ShapeDtypeStruct((TILES, 80, TILE), F32),
    )
    scratch = [
        pltpu.VMEM((4 * chunks, ROWS, 128), BF16),
        pltpu.VMEM((4 * chunks, 128, ROWS), BF16),
        pltpu.VMEM((TILES, 8, TILE), jnp.int32),
        pltpu.VMEM((ROWS, TILE), F32),
        pltpu.VMEM((ROWS, TILE), F32),
        pltpu.VMEM((ROWS, TILE), BF16),
        pltpu.VMEM((ROWS, TILE), BF16),
        pltpu.VMEM((8, TILE), F32),
        pltpu.VMEM((8, TILE), F32),
    ]
    if first:
        outs = (jax.ShapeDtypeStruct((TILES, 128, TILE), BF16),) + state_shapes
        scratch += [pltpu.VMEM((NSH, SUB, 128), F32)]
        rest = [q]
    elif final:
        outs = jax.ShapeDtypeStruct((NSH, HALF, 128), BF16)
        scratch += [pltpu.VMEM(s.shape, F32) for s in state_shapes]
        scratch += [pltpu.VMEM((SUB * NSH, 128), F32)]
        rest = list(state)
    else:
        outs = state_shapes
        rest = list(state)
    table = unit_table(steps)
    share = int(table[:, 0, -1].mean())
    return pl.pallas_call(
        functools.partial(attend_kernel, chunks, first, final),
        out_shape=outs,
        in_specs=[smem(), smem()] + [vmem()] * (chunks + len(rest)),
        out_specs=jax.tree.map(lambda _: vmem(), outs),
        scratch_shapes=scratch,
        compiler_params=params(60),
        cost_estimate=pl.CostEstimate(
            flops=share * 4 * 10**8, bytes_accessed=3 * 10**6, transcendentals=share * 200000
        ),
    )(jnp.asarray(table), y, *kvs, *rest)


def spread_kernel(o_ref, a_ref):
    for z in range(4):
        for y in range(4):
            for half in range(2):
                a_ref[2 * y + half, :, z * HD : (z + 1) * HD] = o_ref[
                    4 * z + y, :, half * HD : (half + 1) * HD
                ]


def spread(o):
    return pl.pallas_call(
        spread_kernel,
        out_shape=jax.ShapeDtypeStruct((8, HALF, 256), BF16),
        in_specs=[vmem()],
        out_specs=vmem(),
        compiler_params=params(60),
        cost_estimate=pl.CostEstimate(flops=10**5, bytes_accessed=800000, transcendentals=0),
    )(o)


def norm_rows(matrix, gain, shift):
    centred = matrix - jnp.mean(matrix, axis=-1, keepdims=True)
    spread_ = jnp.mean(centred * centred, axis=-1, keepdims=True)
    return centred * lax.rsqrt(spread_ + EPSILON) * gain + shift


def mix_kernel(place, a_ref, stream_ref, gain_ref, bias_ref, same_ref, other_ref, n_ref, total):
    c, x = place[0], pl.program_id(0)
    term = jnp.dot(a_ref[2 * x + c], same_ref[0], preferred_element_type=F32)
    term = term + jnp.dot(a_ref[2 * x + 1 - c], other_ref[0], preferred_element_type=F32)

    @pl.when(x == 0)
    def _():
        total[...] = term

    @pl.when(x > 0)
    def _():
        total[...] += term

    @pl.when(x == 3)
    def _():
        mixed = total[...].astype(BF16).astype(F32)
        matrix = ALPHA * stream_ref[...].astype(F32) + mixed
        n_ref[...] = norm_rows(matrix, gain_ref[...], bias_ref[...]).astype(BF16)


def whole(shape):
    return pl.BlockSpec(shape, lambda i, place: (0,) * len(shape))


def along(shape):
    return pl.BlockSpec((1, *shape), lambda i, place: (i,) + (0,) * len(shape))


def mix(place, att, stream, gain, bias, same, other):
    return pl.pallas_call(
        mix_kernel,
        out_shape=jax.ShapeDtypeStruct((HALF, 2048), BF16),
        grid_spec=pltpu.PrefetchScalarGridSpec(
            num_scalar_prefetch=1,
            grid=(4,),
            in_specs=[
                whole((8, HALF, 256)),
                pl.BlockSpec((HALF, 2048), lambda i, place: (place[1], 0)),
                whole((1, 2048)),
                whole((1, 2048)),
                along((256, 2048)),
                along((256, 2048)),
            ],
            out_specs=whole((HALF, 2048)),
            scratch_shapes=[pltpu.VMEM((HALF, 2048), F32)],
        ),
        compiler_params=params(60),
        cost_estimate=pl.CostEstimate(
            flops=2 * HALF * 2048 * 2048, bytes_accessed=9 * 10**6, transcendentals=0
        ),
    )(place, att, stream, gain, bias, same, other)


BLOCKS = 3


def prepare_kernel(w_ref, in_ref):
    for j in range(BLOCKS):
        live = min(256, 704 - 256 * j)
        for part in range(2):
            at = 704 * part + 256 * j
            in_ref[j, :, 256 * part : 256 * part + live] = w_ref[0, at : at + live, :].T
            if live < 256:
                in_ref[j, :, 256 * part + live : 256 * part + 256] = jnp.zeros(
                    (128, 256 - live), BF16
                )


def prepare(w):
    return pl.pallas_call(
        prepare_kernel,
        out_shape=jax.ShapeDtypeStruct((BLOCKS, 2048, 512), BF16),
        grid=(NSH,),
        in_specs=[pl.BlockSpec((1, 1408, 128), lambda s: (s, 0, 0))],
        out_specs=pl.BlockSpec((BLOCKS, 128, 512), lambda s: (0, s, 0)),
        compiler_params=params(60),
        cost_estimate=pl.CostEstimate(
            flops=10**9, bytes_accessed=11 * 10**6, transcendentals=0
        ),
    )(w)


def ffn_kernel(count, place, *refs):
    x_refs = refs[: 2 * count]
    in_ref, out_refs = refs[2 * count], refs[2 * count + 1 : 2 * count + 5]
    same_ref, other_ref, total = refs[2 * count + 5 :]
    j = pl.program_id(0)
    x = jnp.concatenate([r[0] for r in x_refs], axis=0)
    both = jnp.dot(x, in_ref[0], preferred_element_type=F32)
    gate, up = both[:, 0:256], both[:, 256:512]
    hidden = (gate / (1.0 + jnp.exp(-gate)) * up).astype(BF16)
    rows = [jnp.concatenate([r[s] for s in range(NSH)], axis=1) for r in out_refs]
    term = jnp.dot(hidden, jnp.concatenate(rows, axis=0), preferred_element_type=F32)

    @pl.when(j == 0)
    def _():
        total[...] = term

    @pl.when(j == 1)
    def _():
        total[...] += term

    @pl.when(j == BLOCKS - 1)
    def _():
        out = (total[...] + term).astype(BF16)
        for i in range(count):
            same_ref[i] = out[i * HALF : (i + 1) * HALF]
            other_ref[i] = out[(count + i) * HALF : (count + i + 1) * HALF]


def ffn(steps, place, gathered, w_in, w_down):
    count = len(steps)

    def block(d, swapped):
        def at(g, place):
            x, c = place[2], place[0]
            return (2 * lax.rem(x + d, 4) + (1 - c if swapped else c), 0, 0)

        return pl.BlockSpec((1, HALF, 2048), at)

    def down(i):
        return pl.BlockSpec((NSH, 64, 128), lambda g, place: (0, jnp.minimum(4 * g + i, 10), 0))

    shape = jax.ShapeDtypeStruct((count, HALF, 2048), BF16)
    rows = 2 * count * HALF
    return pl.pallas_call(
        functools.partial(ffn_kernel, count),
        out_shape=(shape, shape),
        grid_spec=pltpu.PrefetchScalarGridSpec(
            num_scalar_prefetch=1,
            grid=(BLOCKS,),
            in_specs=[block(d, swapped) for swapped in (False, True) for d in steps]
            + [along((2048, 512))]
            + [down(i) for i in range(4)],
            out_specs=(whole((count, HALF, 2048)),) * 2,
            scratch_shapes=[pltpu.VMEM((rows, 2048), F32)],
        ),
        compiler_params=params(60),
        cost_estimate=pl.CostEstimate(
            flops=6 * rows * 2048 * 704, bytes_accessed=10**7, transcendentals=rows * 704
        ),
    )(place, *([gathered] * (2 * count)), w_in, *([w_down] * 4))


def join_kernel(count, *refs):
    same_ref, other_ref = refs[:2]
    for i in range(count):
        refs[2 + i][...] = (same_ref[i].astype(F32) + other_ref[i].astype(F32)).astype(BF16)


def join(same, other):
    count = same.shape[0]
    shape = jax.ShapeDtypeStruct((HALF, 2048), BF16)
    return pl.pallas_call(
        functools.partial(join_kernel, count),
        out_shape=(shape,) * count,
        in_specs=[vmem()] * 2,
        out_specs=(vmem(),) * count,
        compiler_params=params(60),
        cost_estimate=pl.CostEstimate(flops=10**6, bytes_accessed=10**6, transcendentals=0),
    )(same, other)


def last_kernel(n_ref, gain_ref, bias_ref, *refs):
    o_ref = refs[-1]
    total = refs[0][...].astype(F32)
    for r in refs[1:-1]:
        total = total + r[...].astype(F32)
    lowered = total.astype(BF16).astype(F32)
    matrix = ALPHA * n_ref[...].astype(F32) + lowered
    o_ref[...] = norm_rows(matrix, gain_ref[...], bias_ref[...]).astype(BF16)


def last(parts, normed, gain, bias):
    return pl.pallas_call(
        last_kernel,
        out_shape=jax.ShapeDtypeStruct((HALF, 2048), BF16),
        in_specs=[vmem()] * (3 + len(parts)),
        out_specs=vmem(),
        compiler_params=params(60),
        cost_estimate=pl.CostEstimate(
            flops=4 * 10**6, bytes_accessed=4 * 10**6, transcendentals=0
        ),
    )(normed, gain, bias, *parts)


def body(
    queries, key_rows, value_rows, log_forget, stream_in, out_weight, mix_gain, mix_bias,
    gate_weight, up_weight, down_weight, ffn_gain, ffn_bias,
):
    yi = lax.axis_index("y").astype(jnp.int32)[None]
    xi = lax.axis_index("x")
    ci = lax.axis_index("c")

    def turn(value, axis, d):
        return lax.ppermute(value, axis, [(i, (i + d) % 4) for i in range(4)])

    def swap(value):
        return lax.ppermute(value, "c", [(0, 1), (1, 0)])

    place = jnp.stack([ci, 2 * xi + ci, xi]).astype(jnp.int32)
    w_same = lax.all_gather(out_weight, "x", axis=0, tiled=False)
    q_pack, kv_pack = pack(queries, key_rows, value_rows, log_forget.T)
    q_mine = lax.all_to_all(q_pack, ("z", "y"), split_axis=0, concat_axis=0, tiled=True)
    kv_own = lax.all_to_all(kv_pack, "z", split_axis=0, concat_axis=0, tiled=True)
    kv_back, kv_ahead = turn(kv_own, "y", 1), turn(kv_own, "y", 3)
    kv_far = turn(kv_own, "y", 2)
    w_other = swap(w_same)
    shards = jnp.concatenate([gate_weight.T, up_weight.T], axis=0)
    gu_all = lax.all_gather(shards, ("z", "y"), axis=0, tiled=False)
    w_down = lax.all_gather(down_weight, ("z", "y"), axis=0, tiled=False)

    qt, *state = attend(yi, (0,), [kv_own], q=q_mine)
    state = attend(yi, (3, 1), [kv_back, kv_ahead], state=(qt, *state))
    attended = attend(yi, (2,), [kv_far], state=(qt, *state), final=True)
    by_shard = lax.all_to_all(attended, ("z", "y"), split_axis=0, concat_axis=0, tiled=True)
    by_rows = lax.all_to_all(
        spread(by_shard), ("x", "c"), split_axis=0, concat_axis=0, tiled=True
    )
    normed = mix(place, by_rows, stream_in, mix_gain[None], mix_bias[None], w_same, w_other)
    gathered = lax.all_gather(normed, ("x", "c"), axis=0, tiled=False)
    w_in = prepare(gu_all)

    far_same, far_other = ffn((2,), place, gathered, w_in, w_down)
    far_swapped = swap(far_other)
    near_same, near_other = ffn((1, 3), place, gathered, w_in, w_down)
    near_swapped = swap(near_other)
    own_same, own_other = ffn((0,), place, gathered, w_in, w_down)
    own_swapped = swap(own_other)
    from_far = turn(join(far_same, far_swapped)[0], "x", 2)
    near_back, near_ahead = join(near_same, near_swapped)
    from_back, from_ahead = turn(near_back, "x", 1), turn(near_ahead, "x", 3)
    parts = [own_same[0], own_swapped[0], from_back, from_ahead, from_far]
    return last(parts, normed, ffn_gain[None], ffn_bias[None])


def solution(mesh):
    fine = Mesh(mesh.devices.reshape(4, 4, 4, 2), ("z", "y", "x", "c"))
    sp, tp = ("z", "y"), ("x", "c")
    placed = (
        P(sp, tp), P(sp, tp), P(sp, tp), P(sp, tp), P(sp, None), P(tp, None), P(), P(),
        P(sp, tp), P(sp, tp), P(tp, sp), P(), P(),
    )

    return jax.shard_map(
        body, mesh=fine, in_specs=placed, out_specs=P(("z", "y", "x", "c"), None), check_vma=False
    )
```

```python
import functools
import jax
import jax.numpy as jnp
import numpy as np
from jax import lax
from jax.experimental import pallas as pl
from jax.experimental.pallas import tpu as pltpu
from jax.sharding import Mesh, PartitionSpec as P


ALPHA = 8.0**0.25
EPSILON = 1e-05
F32 = jnp.float32
BF16 = jnp.bfloat16

ROWS = 768
SUB = 192
HALF = 96
HD = 64
NSH = 16
PACK = 800
TILE = 256
TILES = SUB * NSH // TILE


def vmem():
    return pl.BlockSpec(memory_space=pltpu.VMEM)


def smem():
    return pl.BlockSpec(memory_space=pltpu.SMEM)


def params(mb):
    return pltpu.CompilerParams(vmem_limit_bytes=mb * 1024 * 1024)


def pack_kernel(q_ref, k_ref, v_ref, g_ref, qo_ref, kvo_ref):
    for h in range(4):
        cols = slice(h * HD, (h + 1) * HD)
        kvo_ref[h, 0:ROWS, 0:HD] = k_ref[:, cols]
        kvo_ref[h, 0:ROWS, HD : 2 * HD] = v_ref[:, cols]
        for y in range(4):
            at = y * SUB
            qo_ref[h * 4 + y, :, 0:HD] = q_ref[at : at + HALF, cols]
            qo_ref[h * 4 + y, :, HD : 2 * HD] = q_ref[at + HALF : at + SUB, cols]
        chunks = [-g_ref[h : h + 1, c * 128 : (c + 1) * 128] for c in range(6)]
        value = jnp.concatenate(chunks, axis=0)
        first = value.astype(BF16).astype(F32)
        second = (value - first).astype(BF16).astype(F32)
        third = value - first - second
        rest = jnp.zeros((PACK - ROWS - 18, 128), F32)
        kvo_ref[h, ROWS:PACK, :] = jnp.concatenate(
            [first, second, third, rest], axis=0
        ).astype(BF16)


def pack(q, k, v, g):
    return pl.pallas_call(
        pack_kernel,
        out_shape=(
            jax.ShapeDtypeStruct((NSH, HALF, 128), BF16),
            jax.ShapeDtypeStruct((4, PACK, 128), BF16),
        ),
        in_specs=[vmem()] * 4,
        out_specs=(vmem(), vmem()),
        compiler_params=params(60),
        cost_estimate=pl.CostEstimate(flops=10**6, bytes_accessed=2500000, transcendentals=0),
    )(q, k, v, g)


def unit_table(steps):
    tables, counts = [], []
    for y in range(4):
        units = []
        for t in range(TILES):
            low = (TILE * t) // SUB
            for i, d in enumerate(steps):
                for z in range(4):
                    s = z * 4 + (y + d) % 4
                    if s <= low + 1:
                        units.append((t, i * 4 + z, s, int(s >= low)))
        if len(units) % 2:
            units.append((0, 0, NSH - 1, 1))
        counts.append(len(units))
        tables.append([(0, 0, 0, 0)] + units + [units[-1]])
    width = max(len(u) for u in tables) + 1
    out = np.zeros((4, 4, width), np.int32)
    for y in range(4):
        out[y, :, : len(tables[y])] = np.array(tables[y], np.int32).T
        out[y, :, -1] = counts[y]
    return out


def attend_kernel(chunks, first, final, *refs):
    refs = list(refs)
    tab, y_ref = refs[:2]
    kv_refs = refs[2 : 2 + chunks]
    at = 2 + chunks
    if first:
        q_ref, qt, top, acc = refs[at : at + 4]
        at += 4
    else:
        qt, top_in, acc_in = refs[at : at + 3]
        at += 3
        if final:
            o_ref = refs[at]
            at += 1
        else:
            top, acc = refs[at : at + 2]
            at += 2
    kaug, vt, qpos, s_a, s_b, p_a, p_b, al_a, al_b = refs[at : at + 9]
    at += 9
    if first:
        qrow = refs[at]
    if final:
        top, acc, oscr = refs[at : at + 3]
    y = y_ref[0]
    lane = lax.broadcasted_iota(jnp.int32, (128, 128), 1)
    for i in range(chunks):
        kv_ref = kv_refs[i]

        def per_shard(s, carry):
            gates = kv_ref[s, ROWS:PACK, :].astype(F32)
            square = jnp.concatenate(
                [jnp.zeros((HD, 128), F32), gates, jnp.zeros((32, 128), F32)], axis=0
            )
            turned = square.T
            to = i * 4 + s
            for c in range(6):
                part = kv_ref[s, c * 128 : (c + 1) * 128, :].astype(F32)
                mine = (lane == HD + c) | (lane == HD + 6 + c) | (lane == HD + 12 + c)
                kaug[to, c * 128 : (c + 1) * 128, :] = jnp.where(
                    lane < HD, part, jnp.where(mine, turned, 0.0)
                ).astype(BF16)
                vt[to, :, c * 128 : (c + 1) * 128] = part.T.astype(BF16)
            vt[to, 48:64, :] = jnp.ones((16, ROWS), BF16)
            return carry

        lax.fori_loop(0, 4, per_shard, 0)

    lane_h = lax.broadcasted_iota(jnp.int32, (HALF, 128), 1)
    lane_t = lax.broadcasted_iota(jnp.int32, (8, TILE), 1)
    if first:

        def per_query(s, carry):
            both = q_ref[s].astype(F32) * (HD**-0.5)
            ones = jnp.where(lane_h < HD + 18, 1.0, 0.0)
            qrow[s, 0:HALF, :] = jnp.where(lane_h < HD, both, ones)
            qrow[s, HALF:SUB, :] = jnp.where(lane_h < HD, pltpu.roll(both, HD, 1), ones)
            return carry

        lax.fori_loop(0, NSH, per_query, 0)
    for t in range(TILES):
        low = (TILE * t) // SUB
        edge = (low + 1) * SUB - TILE * t
        qpos[t] = y * SUB + jnp.where(
            lane_t < edge,
            low * ROWS + (SUB - edge) + lane_t,
            (low + 1) * ROWS + lane_t - edge,
        )
        if first:
            rows = jnp.concatenate(
                [qrow[low, SUB - edge : SUB, :], qrow[low + 1, 0 : TILE - edge, :]], axis=0
            )
            qt[t] = rows.T.astype(BF16)
    if first:
        acc[...] = jnp.zeros(acc.shape, F32)
        top[...] = jnp.full(top.shape, -1e30, F32)
    else:
        acc[...] = acc_in[...]
        top[...] = top_in[...]
    al_b[...] = jnp.ones(al_b.shape, F32)
    p_b[...] = jnp.zeros(p_b.shape, BF16)

    def scores(u, out):
        out[...] = jnp.dot(kaug[tab[y, 1, u]], qt[tab[y, 0, u]], preferred_element_type=F32)

    def gather(u, p_before, al_before):
        t = tab[y, 0, u]
        pv = jnp.dot(vt[tab[y, 1, u], 48:128, :], p_before[...], preferred_element_type=F32)
        acc[t] = acc[t] * al_before[0:1, :] + pv

    scores(1, s_a)

    def unit(u, s_now, s_next, p_before, p_now, al_before, al_now):
        def work(masked):
            scores(u + 1, s_next)
            gather(u - 1, p_before, al_before)
            t = tab[y, 0, u]
            before = top[t, 0:1, :]
            s = s_now[...]
            if masked:
                pos = tab[y, 2, u] * ROWS + lax.broadcasted_iota(jnp.int32, (ROWS, TILE), 0)
                s = jnp.where(pos <= qpos[t, 0:1, :], s, -1e30)
            high = jnp.maximum(before, jnp.max(s, axis=0, keepdims=True))
            p_now[...] = jnp.exp(s - high).astype(BF16)
            top[t, 0:1, :] = high
            al_now[0:1, :] = jnp.exp(before - high)

        lax.cond(tab[y, 3, u] == 1, lambda: work(True), lambda: work(False))

    def pair(i, carry):
        unit(2 * i + 1, s_a, s_b, p_b, p_a, al_b, al_a)
        unit(2 * i + 2, s_b, s_a, p_a, p_b, al_a, al_b)
        return carry

    count = tab[y, 0, tab.shape[2] - 1]
    lax.fori_loop(0, count // 2, pair, 0)
    gather(count, p_b, al_b)

    if final:

        def finish(t, carry):
            good = acc[t, 16:80, :] / acc[t, 0:1, :]
            full = jnp.concatenate([good, jnp.zeros((HD, TILE), F32)], axis=0)
            oscr[pl.ds(pl.multiple_of(t * TILE, TILE), TILE), :] = full.T
            return carry

        lax.fori_loop(0, TILES, finish, 0)

        def out(s, carry):
            row = pl.multiple_of(s * SUB, SUB)
            one = oscr[pl.ds(row, HALF), :]
            two = oscr[pl.ds(row + HALF, HALF), :]
            o_ref[s] = jnp.where(lane_h < HD, one, pltpu.roll(two, HD, 1)).astype(BF16)
            return carry

        lax.fori_loop(0, NSH, out, 0)


def attend(y, steps, kvs, q=None, state=None, final=False):
    chunks, first = len(kvs), q is not None
    state_shapes = (
        jax.ShapeDtypeStruct((TILES, 8, TILE), F32),
        jax.ShapeDtypeStruct((TILES, 80, TILE), F32),
    )
    scratch = [
        pltpu.VMEM((4 * chunks, ROWS, 128), BF16),
        pltpu.VMEM((4 * chunks, 128, ROWS), BF16),
        pltpu.VMEM((TILES, 8, TILE), jnp.int32),
        pltpu.VMEM((ROWS, TILE), F32),
        pltpu.VMEM((ROWS, TILE), F32),
        pltpu.VMEM((ROWS, TILE), BF16),
        pltpu.VMEM((ROWS, TILE), BF16),
        pltpu.VMEM((8, TILE), F32),
        pltpu.VMEM((8, TILE), F32),
    ]
    if first:
        outs = (jax.ShapeDtypeStruct((TILES, 128, TILE), BF16),) + state_shapes
        scratch += [pltpu.VMEM((NSH, SUB, 128), F32)]
        rest = [q]
    elif final:
        outs = jax.ShapeDtypeStruct((NSH, HALF, 128), BF16)
        scratch += [pltpu.VMEM(s.shape, F32) for s in state_shapes]
        scratch += [pltpu.VMEM((SUB * NSH, 128), F32)]
        rest = list(state)
    else:
        outs = state_shapes
        rest = list(state)
    table = unit_table(steps)
    share = int(table[:, 0, -1].mean())
    return pl.pallas_call(
        functools.partial(attend_kernel, chunks, first, final),
        out_shape=outs,
        in_specs=[smem(), smem()] + [vmem()] * (chunks + len(rest)),
        out_specs=jax.tree.map(lambda _: vmem(), outs),
        scratch_shapes=scratch,
        compiler_params=params(60),
        cost_estimate=pl.CostEstimate(
            flops=share * 4 * 10**8, bytes_accessed=3 * 10**6, transcendentals=share * 200000
        ),
    )(jnp.asarray(table), y, *kvs, *rest)


def spread_kernel(o_ref, a_ref):
    for z in range(4):
        for y in range(4):
            for half in range(2):
                a_ref[2 * y + half, :, z * HD : (z + 1) * HD] = o_ref[
                    4 * z + y, :, half * HD : (half + 1) * HD
                ]


def spread(o):
    return pl.pallas_call(
        spread_kernel,
        out_shape=jax.ShapeDtypeStruct((8, HALF, 256), BF16),
        in_specs=[vmem()],
        out_specs=vmem(),
        compiler_params=params(60),
        cost_estimate=pl.CostEstimate(flops=10**5, bytes_accessed=800000, transcendentals=0),
    )(o)


def norm_rows(matrix, gain, shift):
    centred = matrix - jnp.mean(matrix, axis=-1, keepdims=True)
    spread_ = jnp.mean(centred * centred, axis=-1, keepdims=True)
    return centred * lax.rsqrt(spread_ + EPSILON) * gain + shift


def mix_kernel(place, a_ref, stream_ref, gain_ref, bias_ref, same_ref, other_ref, n_ref, total):
    c, x = place[0], pl.program_id(0)
    term = jnp.dot(a_ref[2 * x + c], same_ref[0], preferred_element_type=F32)
    term = term + jnp.dot(a_ref[2 * x + 1 - c], other_ref[0], preferred_element_type=F32)

    @pl.when(x == 0)
    def _():
        total[...] = term

    @pl.when(x > 0)
    def _():
        total[...] += term

    @pl.when(x == 3)
    def _():
        mixed = total[...].astype(BF16).astype(F32)
        matrix = ALPHA * stream_ref[...].astype(F32) + mixed
        n_ref[...] = norm_rows(matrix, gain_ref[...], bias_ref[...]).astype(BF16)


def whole(shape):
    return pl.BlockSpec(shape, lambda i, place: (0,) * len(shape))


def along(shape):
    return pl.BlockSpec((1, *shape), lambda i, place: (i,) + (0,) * len(shape))


def mix(place, att, stream, gain, bias, same, other):
    return pl.pallas_call(
        mix_kernel,
        out_shape=jax.ShapeDtypeStruct((HALF, 2048), BF16),
        grid_spec=pltpu.PrefetchScalarGridSpec(
            num_scalar_prefetch=1,
            grid=(4,),
            in_specs=[
                whole((8, HALF, 256)),
                pl.BlockSpec((HALF, 2048), lambda i, place: (place[1], 0)),
                whole((1, 2048)),
                whole((1, 2048)),
                along((256, 2048)),
                along((256, 2048)),
            ],
            out_specs=whole((HALF, 2048)),
            scratch_shapes=[pltpu.VMEM((HALF, 2048), F32)],
        ),
        compiler_params=params(60),
        cost_estimate=pl.CostEstimate(
            flops=2 * HALF * 2048 * 2048, bytes_accessed=9 * 10**6, transcendentals=0
        ),
    )(place, att, stream, gain, bias, same, other)


BLOCKS = 3


def prepare_kernel(w_ref, in_ref, down_ref):
    down_ref[...] = w_ref[:, 1408:2112, :]
    for j in range(BLOCKS):
        live = min(256, 704 - 256 * j)
        for part in range(2):
            at = 704 * part + 256 * j
            in_ref[j, :, 256 * part : 256 * part + live] = w_ref[0, at : at + live, :].T
            if live < 256:
                in_ref[j, :, 256 * part + live : 256 * part + 256] = jnp.zeros(
                    (128, 256 - live), BF16
                )


def prepare(w):
    return pl.pallas_call(
        prepare_kernel,
        out_shape=(
            jax.ShapeDtypeStruct((BLOCKS, 2048, 512), BF16),
            jax.ShapeDtypeStruct((NSH, 704, 128), BF16),
        ),
        grid=(NSH,),
        in_specs=[pl.BlockSpec((1, 2112, 128), lambda s: (s, 0, 0))],
        out_specs=(
            pl.BlockSpec((BLOCKS, 128, 512), lambda s: (0, s, 0)),
            pl.BlockSpec((1, 704, 128), lambda s: (s, 0, 0)),
        ),
        compiler_params=params(60),
        cost_estimate=pl.CostEstimate(
            flops=10**9, bytes_accessed=11 * 10**6, transcendentals=0
        ),
    )(w)


def ffn_kernel(count, place, *refs):
    x_refs = refs[: 2 * count]
    in_ref, out_refs = refs[2 * count], refs[2 * count + 1 : 2 * count + 5]
    same_ref, other_ref, total = refs[2 * count + 5 :]
    j = pl.program_id(0)
    x = jnp.concatenate([r[0] for r in x_refs], axis=0)
    both = jnp.dot(x, in_ref[0], preferred_element_type=F32)
    gate, up = both[:, 0:256], both[:, 256:512]
    hidden = (gate / (1.0 + jnp.exp(-gate)) * up).astype(BF16)
    rows = [jnp.concatenate([r[s] for s in range(NSH)], axis=1) for r in out_refs]
    term = jnp.dot(hidden, jnp.concatenate(rows, axis=0), preferred_element_type=F32)

    @pl.when(j == 0)
    def _():
        total[...] = term

    @pl.when(j == 1)
    def _():
        total[...] += term

    @pl.when(j == BLOCKS - 1)
    def _():
        out = (total[...] + term).astype(BF16)
        for i in range(count):
            same_ref[i] = out[i * HALF : (i + 1) * HALF]
            other_ref[i] = out[(count + i) * HALF : (count + i + 1) * HALF]


def ffn(steps, place, gathered, w_in, w_down):
    count = len(steps)

    def block(d, swapped):
        def at(g, place):
            x, c = place[2], place[0]
            return (2 * lax.rem(x + d, 4) + (1 - c if swapped else c), 0, 0)

        return pl.BlockSpec((1, HALF, 2048), at)

    def down(i):
        return pl.BlockSpec((NSH, 64, 128), lambda g, place: (0, jnp.minimum(4 * g + i, 10), 0))

    shape = jax.ShapeDtypeStruct((count, HALF, 2048), BF16)
    rows = 2 * count * HALF
    return pl.pallas_call(
        functools.partial(ffn_kernel, count),
        out_shape=(shape, shape),
        grid_spec=pltpu.PrefetchScalarGridSpec(
            num_scalar_prefetch=1,
            grid=(BLOCKS,),
            in_specs=[block(d, swapped) for swapped in (False, True) for d in steps]
            + [along((2048, 512))]
            + [down(i) for i in range(4)],
            out_specs=(whole((count, HALF, 2048)),) * 2,
            scratch_shapes=[pltpu.VMEM((rows, 2048), F32)],
        ),
        compiler_params=params(60),
        cost_estimate=pl.CostEstimate(
            flops=6 * rows * 2048 * 704, bytes_accessed=10**7, transcendentals=rows * 704
        ),
    )(place, *([gathered] * (2 * count)), w_in, *([w_down] * 4))


def join(one, two):
    return (one.astype(F32) + two.astype(F32)).astype(BF16)


def last_kernel(n_ref, gain_ref, bias_ref, *refs):
    o_ref = refs[-1]
    total = refs[0][...].astype(F32)
    for r in refs[1:-1]:
        total = total + r[...].astype(F32)
    lowered = total.astype(BF16).astype(F32)
    matrix = ALPHA * n_ref[...].astype(F32) + lowered
    o_ref[...] = norm_rows(matrix, gain_ref[...], bias_ref[...]).astype(BF16)


def last(parts, normed, gain, bias):
    return pl.pallas_call(
        last_kernel,
        out_shape=jax.ShapeDtypeStruct((HALF, 2048), BF16),
        in_specs=[vmem()] * (3 + len(parts)),
        out_specs=vmem(),
        compiler_params=params(60),
        cost_estimate=pl.CostEstimate(
            flops=4 * 10**6, bytes_accessed=4 * 10**6, transcendentals=0
        ),
    )(normed, gain, bias, *parts)


def body(
    queries, key_rows, value_rows, log_forget, stream_in, out_weight, mix_gain, mix_bias,
    gate_weight, up_weight, down_weight, ffn_gain, ffn_bias,
):
    yi = lax.axis_index("y").astype(jnp.int32)[None]
    xi = lax.axis_index("x")
    ci = lax.axis_index("c")

    def turn(value, axis, d):
        return lax.ppermute(value, axis, [(i, (i + d) % 4) for i in range(4)])

    def swap(value):
        return lax.ppermute(value, "c", [(0, 1), (1, 0)])

    place = jnp.stack([ci, 2 * xi + ci, xi]).astype(jnp.int32)
    w_same = lax.all_gather(out_weight, "x", axis=0, tiled=False)
    q_pack, kv_pack = pack(queries, key_rows, value_rows, log_forget.T)
    q_mine = lax.all_to_all(q_pack, ("z", "y"), split_axis=0, concat_axis=0, tiled=True)
    kv_own = lax.all_to_all(kv_pack, "z", split_axis=0, concat_axis=0, tiled=True)
    kv_back, kv_ahead = turn(kv_own, "y", 1), turn(kv_own, "y", 3)
    kv_far = turn(kv_own, "y", 2)
    w_other = swap(w_same)
    shards = jnp.concatenate([gate_weight.T, up_weight.T, down_weight], axis=0)
    ffn_all = lax.all_gather(shards, ("z", "y"), axis=0, tiled=False)

    qt, *state = attend(yi, (0,), [kv_own], q=q_mine)
    state = attend(yi, (3, 1), [kv_back, kv_ahead], state=(qt, *state))
    attended = attend(yi, (2,), [kv_far], state=(qt, *state), final=True)
    by_shard = lax.all_to_all(attended, ("z", "y"), split_axis=0, concat_axis=0, tiled=True)
    by_rows = lax.all_to_all(
        spread(by_shard), ("x", "c"), split_axis=0, concat_axis=0, tiled=True
    )
    normed = mix(place, by_rows, stream_in, mix_gain[None], mix_bias[None], w_same, w_other)
    gathered = lax.all_gather(normed, ("x", "c"), axis=0, tiled=False)
    w_in, w_down = prepare(ffn_all)

    far_same, far_other = ffn((2,), place, gathered, w_in, w_down)
    far_swapped = swap(far_other)
    near_same, near_other = ffn((1, 3), place, gathered, w_in, w_down)
    near_swapped = swap(near_other)
    own_same, own_other = ffn((0,), place, gathered, w_in, w_down)
    own_swapped = swap(own_other)
    from_far = turn(join(far_same[0], far_swapped[0]), "x", 2)
    near = [join(near_same[i], near_swapped[i]) for i in range(2)]
    from_back, from_ahead = turn(near[0], "x", 1), turn(near[1], "x", 3)
    parts = [own_same[0], own_swapped[0], from_back, from_ahead, from_far]
    return last(parts, normed, ffn_gain[None], ffn_bias[None])


def solution(mesh):
    fine = Mesh(mesh.devices.reshape(4, 4, 4, 2), ("z", "y", "x", "c"))
    sp, tp = ("z", "y"), ("x", "c")
    placed = (
        P(sp, tp), P(sp, tp), P(sp, tp), P(sp, tp), P(sp, None), P(tp, None), P(), P(),
        P(sp, tp), P(sp, tp), P(tp, sp), P(), P(),
    )

    return jax.shard_map(
        body, mesh=fine, in_specs=placed, out_specs=P(("z", "y", "x", "c"), None), check_vma=False
    )
```

```python
import functools
import jax
import jax.numpy as jnp
import numpy as np
from jax import lax
from jax.experimental import pallas as pl
from jax.experimental.pallas import tpu as pltpu
from jax.sharding import Mesh, PartitionSpec as P


ALPHA = 8.0**0.25
EPSILON = 1e-05
F32 = jnp.float32
BF16 = jnp.bfloat16

ROWS = 768
SUB = 192
HALF = 96
HD = 64
NSH = 16
PACK = 800
TILE = 256
SPLIT = 1
TILES = SUB * NSH // TILE


def vmem():
    return pl.BlockSpec(memory_space=pltpu.VMEM)


def smem():
    return pl.BlockSpec(memory_space=pltpu.SMEM)


def params(mb):
    return pltpu.CompilerParams(vmem_limit_bytes=mb * 1024 * 1024)


def pack_kernel(q_ref, k_ref, v_ref, g_ref, qo_ref, kvo_ref):
    for h in range(4):
        cols = slice(h * HD, (h + 1) * HD)
        kvo_ref[h, 0:ROWS, 0:HD] = k_ref[:, cols]
        kvo_ref[h, 0:ROWS, HD : 2 * HD] = v_ref[:, cols]
        for y in range(4):
            at = y * SUB
            qo_ref[h * 4 + y, :, 0:HD] = q_ref[at : at + HALF, cols]
            qo_ref[h * 4 + y, :, HD : 2 * HD] = q_ref[at + HALF : at + SUB, cols]
        chunks = [-g_ref[h : h + 1, c * 128 : (c + 1) * 128] for c in range(6)]
        value = jnp.concatenate(chunks, axis=0)
        first = value.astype(BF16).astype(F32)
        second = (value - first).astype(BF16).astype(F32)
        third = value - first - second
        rest = jnp.zeros((PACK - ROWS - 18, 128), F32)
        kvo_ref[h, ROWS:PACK, :] = jnp.concatenate(
            [first, second, third, rest], axis=0
        ).astype(BF16)


def pack(q, k, v, g):
    return pl.pallas_call(
        pack_kernel,
        out_shape=(
            jax.ShapeDtypeStruct((NSH, HALF, 128), BF16),
            jax.ShapeDtypeStruct((4, PACK, 128), BF16),
        ),
        in_specs=[vmem()] * 4,
        out_specs=(vmem(), vmem()),
        compiler_params=params(60),
        cost_estimate=pl.CostEstimate(flops=10**6, bytes_accessed=2500000, transcendentals=0),
    )(q, k, v, g)


def unit_table(steps):
    tables, counts = [], []
    for y in range(4):
        units = []
        for t in range(TILES):
            low = (TILE * t) // SUB
            for i, d in enumerate(steps):
                for z in range(4):
                    s = z * 4 + (y + d) % 4
                    if s <= low + 1:
                        units.append((t, i * 4 + z, s, int(s >= low)))
        plain = [u for u in units if not u[3]]
        held = [u for u in units if u[3]]
        if len(plain) % 2:
            held.insert(0, plain.pop())
        if len(held) % 2:
            held.append((0, 0, NSH - 1, 1))
        units = plain + held
        counts.append((len(plain) // 2, len(units) // 2))
        tables.append([(0, 0, 0, 0)] + units + [units[-1]])
    width = max(len(u) for u in tables) + 1
    out = np.zeros((4, 4, width), np.int32)
    for y in range(4):
        out[y, :, : len(tables[y])] = np.array(tables[y], np.int32).T
        out[y, 0:2, -1] = counts[y]
    return out


def attend_kernel(chunks, first, final, *refs):
    refs = list(refs)
    tab, y_ref = refs[:2]
    kv_refs = refs[2 : 2 + chunks]
    at = 2 + chunks
    if first:
        q_ref, qt, top, acc = refs[at : at + 4]
        at += 4
    else:
        qt, top_in, acc_in = refs[at : at + 3]
        at += 3
        if final:
            o_ref = refs[at]
            at += 1
        else:
            top, acc = refs[at : at + 2]
            at += 2
    kaug, vt, qpos, s_a, s_b, p_a, p_b, al_a, al_b, mx_a, mx_b = refs[at : at + 11]
    at += 11
    if first:
        qrow = refs[at]
    if final:
        top, acc, oscr = refs[at : at + 3]
    y = y_ref[0]
    lane = lax.broadcasted_iota(jnp.int32, (128, 128), 1)
    for i in range(chunks):
        kv_ref = kv_refs[i]

        def per_shard(s, carry):
            gates = kv_ref[s, ROWS:PACK, :].astype(F32)
            square = jnp.concatenate(
                [jnp.zeros((HD, 128), F32), gates, jnp.zeros((32, 128), F32)], axis=0
            )
            turned = square.T
            to = i * 4 + s
            for c in range(6):
                part = kv_ref[s, c * 128 : (c + 1) * 128, :].astype(F32)
                mine = (lane == HD + c) | (lane == HD + 6 + c) | (lane == HD + 12 + c)
                kaug[to, c * 128 : (c + 1) * 128, :] = jnp.where(
                    lane < HD, part, jnp.where(mine, turned, 0.0)
                ).astype(BF16)
                vt[to, :, c * 128 : (c + 1) * 128] = part.T.astype(BF16)
            vt[to, 48:64, :] = jnp.ones((16, ROWS), BF16)
            return carry

        lax.fori_loop(0, 4, per_shard, 0)

    lane_h = lax.broadcasted_iota(jnp.int32, (HALF, 128), 1)
    lane_t = lax.broadcasted_iota(jnp.int32, (8, TILE), 1)
    if first:

        def per_query(s, carry):
            both = q_ref[s].astype(F32) * (HD**-0.5)
            ones = jnp.where(lane_h < HD + 18, 1.0, 0.0)
            qrow[s, 0:HALF, :] = jnp.where(lane_h < HD, both, ones)
            qrow[s, HALF:SUB, :] = jnp.where(lane_h < HD, pltpu.roll(both, HD, 1), ones)
            return carry

        lax.fori_loop(0, NSH, per_query, 0)
    for t in range(TILES):
        low = (TILE * t) // SUB
        edge = (low + 1) * SUB - TILE * t
        qpos[t] = y * SUB + jnp.where(
            lane_t < edge,
            low * ROWS + (SUB - edge) + lane_t,
            (low + 1) * ROWS + lane_t - edge,
        )
        if first:
            rows = jnp.concatenate(
                [qrow[low, SUB - edge : SUB, :], qrow[low + 1, 0 : TILE - edge, :]], axis=0
            )
            qt[t] = rows.T.astype(BF16)
    if first:
        acc[...] = jnp.zeros(acc.shape, F32)
        top[...] = jnp.full(top.shape, -1e30, F32)
    else:
        acc[...] = acc_in[...]
        top[...] = top_in[...]
    al_b[...] = jnp.ones(al_b.shape, F32)
    p_b[...] = jnp.zeros(p_b.shape, BF16)

    def scores(u, out, most, masked):
        rows = ROWS // SPLIT
        high = None
        for i in range(SPLIT):
            part = slice(i * rows, (i + 1) * rows)
            s = jnp.dot(
                kaug[tab[y, 1, u], part, :], qt[tab[y, 0, u]], preferred_element_type=F32
            )
            if masked:
                pos = tab[y, 2, u] * ROWS + i * rows
                pos = pos + lax.broadcasted_iota(jnp.int32, (rows, TILE), 0)
                s = jnp.where(pos <= qpos[tab[y, 0, u], 0:1, :], s, -1e30)
            out[part, :] = s
            here = jnp.max(s.reshape(rows // 8, 8, TILE), axis=0)
            high = here if high is None else jnp.maximum(high, here)
        most[...] = high

    def gather(u, p_before, al_before):
        t = tab[y, 0, u]
        pv = jnp.dot(vt[tab[y, 1, u], 48:128, :], p_before[...], preferred_element_type=F32)
        acc[t] = acc[t] * al_before[0:1, :] + pv

    def unit(u, now, later, before, masked):
        s_now, p_now, al_now, mx_now = now
        s_next, _, _, mx_next = later
        _, p_before, al_before, _ = before
        t = tab[y, 0, u]
        old = top[t, 0:1, :]
        high = jnp.maximum(old, jnp.max(mx_now[...], axis=0, keepdims=True))
        top[t, 0:1, :] = high
        al_now[0:1, :] = jnp.exp(old - high)
        scores(u + 1, s_next, mx_next, masked)
        p_now[...] = jnp.exp(s_now[...] - high).astype(BF16)
        gather(u - 1, p_before, al_before)

    one, two = (s_a, p_a, al_a, mx_a), (s_b, p_b, al_b, mx_b)
    last_at = tab.shape[2] - 1
    plain, pairs = tab[y, 0, last_at], tab[y, 1, last_at]
    for masked, low, high in ((False, 0, plain), (True, plain, pairs)):

        def pair(i, carry):
            unit(2 * i + 1, one, two, two, masked)
            unit(2 * i + 2, two, one, one, masked)
            return carry

        scores(2 * low + 1, s_a, mx_a, masked)
        lax.fori_loop(low, high, pair, 0)
    gather(2 * pairs, p_b, al_b)

    if final:

        def finish(t, carry):
            good = acc[t, 16:80, :] / acc[t, 0:1, :]
            full = jnp.concatenate([good, jnp.zeros((HD, TILE), F32)], axis=0)
            oscr[pl.ds(pl.multiple_of(t * TILE, TILE), TILE), :] = full.T
            return carry

        lax.fori_loop(0, TILES, finish, 0)

        def out(s, carry):
            row = pl.multiple_of(s * SUB, SUB)
            one = oscr[pl.ds(row, HALF), :]
            two = oscr[pl.ds(row + HALF, HALF), :]
            o_ref[s] = jnp.where(lane_h < HD, one, pltpu.roll(two, HD, 1)).astype(BF16)
            return carry

        lax.fori_loop(0, NSH, out, 0)


def attend(y, steps, kvs, q=None, state=None, final=False):
    chunks, first = len(kvs), q is not None
    state_shapes = (
        jax.ShapeDtypeStruct((TILES, 8, TILE), F32),
        jax.ShapeDtypeStruct((TILES, 80, TILE), F32),
    )
    scratch = [
        pltpu.VMEM((4 * chunks, ROWS, 128), BF16),
        pltpu.VMEM((4 * chunks, 128, ROWS), BF16),
        pltpu.VMEM((TILES, 8, TILE), jnp.int32),
        pltpu.VMEM((ROWS, TILE), F32),
        pltpu.VMEM((ROWS, TILE), F32),
        pltpu.VMEM((ROWS, TILE), BF16),
        pltpu.VMEM((ROWS, TILE), BF16),
    ] + [pltpu.VMEM((8, TILE), F32)] * 4
    if first:
        outs = (jax.ShapeDtypeStruct((TILES, 128, TILE), BF16),) + state_shapes
        scratch += [pltpu.VMEM((NSH, SUB, 128), F32)]
        rest = [q]
    elif final:
        outs = jax.ShapeDtypeStruct((NSH, HALF, 128), BF16)
        scratch += [pltpu.VMEM(s.shape, F32) for s in state_shapes]
        scratch += [pltpu.VMEM((SUB * NSH, 128), F32)]
        rest = list(state)
    else:
        outs = state_shapes
        rest = list(state)
    table = unit_table(steps)
    share = 2 * int(table[:, 1, -1].mean())
    return pl.pallas_call(
        functools.partial(attend_kernel, chunks, first, final),
        out_shape=outs,
        in_specs=[smem(), smem()] + [vmem()] * (chunks + len(rest)),
        out_specs=jax.tree.map(lambda _: vmem(), outs),
        scratch_shapes=scratch,
        compiler_params=params(60),
        cost_estimate=pl.CostEstimate(
            flops=share * 4 * 10**8, bytes_accessed=3 * 10**6, transcendentals=share * 200000
        ),
    )(jnp.asarray(table), y, *kvs, *rest)


def spread_kernel(o_ref, a_ref):
    for z in range(4):
        for y in range(4):
            for half in range(2):
                a_ref[2 * y + half, :, z * HD : (z + 1) * HD] = o_ref[
                    4 * z + y, :, half * HD : (half + 1) * HD
                ]


def spread(o):
    return pl.pallas_call(
        spread_kernel,
        out_shape=jax.ShapeDtypeStruct((8, HALF, 256), BF16),
        in_specs=[vmem()],
        out_specs=vmem(),
        compiler_params=params(60),
        cost_estimate=pl.CostEstimate(flops=10**5, bytes_accessed=800000, transcendentals=0),
    )(o)


def norm_rows(matrix, gain, shift):
    centred = matrix - jnp.mean(matrix, axis=-1, keepdims=True)
    spread_ = jnp.mean(centred * centred, axis=-1, keepdims=True)
    return centred * lax.rsqrt(spread_ + EPSILON) * gain + shift


def mix_kernel(place, a_ref, stream_ref, gain_ref, bias_ref, same_ref, other_ref, n_ref, total):
    c, x = place[0], pl.program_id(0)
    term = jnp.dot(a_ref[2 * x + c], same_ref[0], preferred_element_type=F32)
    term = term + jnp.dot(a_ref[2 * x + 1 - c], other_ref[0], preferred_element_type=F32)

    @pl.when(x == 0)
    def _():
        total[...] = term

    @pl.when(x > 0)
    def _():
        total[...] += term

    @pl.when(x == 3)
    def _():
        mixed = total[...].astype(BF16).astype(F32)
        matrix = ALPHA * stream_ref[...].astype(F32) + mixed
        n_ref[...] = norm_rows(matrix, gain_ref[...], bias_ref[...]).astype(BF16)


def whole(shape):
    return pl.BlockSpec(shape, lambda i, place: (0,) * len(shape))


def along(shape):
    return pl.BlockSpec((1, *shape), lambda i, place: (i,) + (0,) * len(shape))


def mix(place, att, stream, gain, bias, same, other):
    return pl.pallas_call(
        mix_kernel,
        out_shape=jax.ShapeDtypeStruct((HALF, 2048), BF16),
        grid_spec=pltpu.PrefetchScalarGridSpec(
            num_scalar_prefetch=1,
            grid=(4,),
            in_specs=[
                whole((8, HALF, 256)),
                pl.BlockSpec((HALF, 2048), lambda i, place: (place[1], 0)),
                whole((1, 2048)),
                whole((1, 2048)),
                along((256, 2048)),
                along((256, 2048)),
            ],
            out_specs=whole((HALF, 2048)),
            scratch_shapes=[pltpu.VMEM((HALF, 2048), F32)],
        ),
        compiler_params=params(60),
        cost_estimate=pl.CostEstimate(
            flops=2 * HALF * 2048 * 2048, bytes_accessed=9 * 10**6, transcendentals=0
        ),
    )(place, att, stream, gain, bias, same, other)


BLOCKS = 3


def prepare_kernel(w_ref, in_ref, down_ref):
    down_ref[...] = w_ref[:, 1408:2112, :]
    for j in range(BLOCKS):
        live = min(256, 704 - 256 * j)
        for part in range(2):
            at = 704 * part + 256 * j
            in_ref[j, :, 256 * part : 256 * part + live] = w_ref[0, at : at + live, :].T
            if live < 256:
                in_ref[j, :, 256 * part + live : 256 * part + 256] = jnp.zeros(
                    (128, 256 - live), BF16
                )


def prepare(w):
    return pl.pallas_call(
        prepare_kernel,
        out_shape=(
            jax.ShapeDtypeStruct((BLOCKS, 2048, 512), BF16),
            jax.ShapeDtypeStruct((NSH, 704, 128), BF16),
        ),
        grid=(NSH,),
        in_specs=[pl.BlockSpec((1, 2112, 128), lambda s: (s, 0, 0))],
        out_specs=(
            pl.BlockSpec((BLOCKS, 128, 512), lambda s: (0, s, 0)),
            pl.BlockSpec((1, 704, 128), lambda s: (s, 0, 0)),
        ),
        compiler_params=params(60),
        cost_estimate=pl.CostEstimate(
            flops=10**9, bytes_accessed=11 * 10**6, transcendentals=0
        ),
    )(w)


def ffn_kernel(count, place, *refs):
    x_refs = refs[: 2 * count]
    in_ref, out_refs = refs[2 * count], refs[2 * count + 1 : 2 * count + 5]
    same_ref, other_ref, total = refs[2 * count + 5 :]
    j = pl.program_id(0)
    x = jnp.concatenate([r[0] for r in x_refs], axis=0)
    both = jnp.dot(x, in_ref[0], preferred_element_type=F32)
    gate, up = both[:, 0:256], both[:, 256:512]
    hidden = (gate / (1.0 + jnp.exp(-gate)) * up).astype(BF16)
    rows = [jnp.concatenate([r[s] for s in range(NSH)], axis=1) for r in out_refs]
    term = jnp.dot(hidden, jnp.concatenate(rows, axis=0), preferred_element_type=F32)

    @pl.when(j == 0)
    def _():
        total[...] = term

    @pl.when(j == 1)
    def _():
        total[...] += term

    @pl.when(j == BLOCKS - 1)
    def _():
        out = (total[...] + term).astype(BF16)
        for i in range(count):
            same_ref[i] = out[i * HALF : (i + 1) * HALF]
            other_ref[i] = out[(count + i) * HALF : (count + i + 1) * HALF]


def ffn(steps, place, gathered, w_in, w_down):
    count = len(steps)

    def block(d, swapped):
        def at(g, place):
            x, c = place[2], place[0]
            return (2 * lax.rem(x + d, 4) + (1 - c if swapped else c), 0, 0)

        return pl.BlockSpec((1, HALF, 2048), at)

    def down(i):
        return pl.BlockSpec((NSH, 64, 128), lambda g, place: (0, jnp.minimum(4 * g + i, 10), 0))

    shape = jax.ShapeDtypeStruct((count, HALF, 2048), BF16)
    rows = 2 * count * HALF
    return pl.pallas_call(
        functools.partial(ffn_kernel, count),
        out_shape=(shape, shape),
        grid_spec=pltpu.PrefetchScalarGridSpec(
            num_scalar_prefetch=1,
            grid=(BLOCKS,),
            in_specs=[block(d, swapped) for swapped in (False, True) for d in steps]
            + [along((2048, 512))]
            + [down(i) for i in range(4)],
            out_specs=(whole((count, HALF, 2048)),) * 2,
            scratch_shapes=[pltpu.VMEM((rows, 2048), F32)],
        ),
        compiler_params=params(60),
        cost_estimate=pl.CostEstimate(
            flops=6 * rows * 2048 * 704, bytes_accessed=10**7, transcendentals=rows * 704
        ),
    )(place, *([gathered] * (2 * count)), w_in, *([w_down] * 4))


def join(one, two):
    return (one.astype(F32) + two.astype(F32)).astype(BF16)


def last_kernel(n_ref, gain_ref, bias_ref, *refs):
    o_ref = refs[-1]
    total = refs[0][...].astype(F32)
    for r in refs[1:-1]:
        total = total + r[...].astype(F32)
    lowered = total.astype(BF16).astype(F32)
    matrix = ALPHA * n_ref[...].astype(F32) + lowered
    o_ref[...] = norm_rows(matrix, gain_ref[...], bias_ref[...]).astype(BF16)


def last(parts, normed, gain, bias):
    return pl.pallas_call(
        last_kernel,
        out_shape=jax.ShapeDtypeStruct((HALF, 2048), BF16),
        in_specs=[vmem()] * (3 + len(parts)),
        out_specs=vmem(),
        compiler_params=params(60),
        cost_estimate=pl.CostEstimate(
            flops=4 * 10**6, bytes_accessed=4 * 10**6, transcendentals=0
        ),
    )(normed, gain, bias, *parts)


def body(
    queries, key_rows, value_rows, log_forget, stream_in, out_weight, mix_gain, mix_bias,
    gate_weight, up_weight, down_weight, ffn_gain, ffn_bias,
):
    yi = lax.axis_index("y").astype(jnp.int32)[None]
    xi = lax.axis_index("x")
    ci = lax.axis_index("c")

    def turn(value, axis, d):
        return lax.ppermute(value, axis, [(i, (i + d) % 4) for i in range(4)])

    def swap(value):
        return lax.ppermute(value, "c", [(0, 1), (1, 0)])

    place = jnp.stack([ci, 2 * xi + ci, xi]).astype(jnp.int32)
    w_same = lax.all_gather(out_weight, "x", axis=0, tiled=False)
    q_pack, kv_pack = pack(queries, key_rows, value_rows, log_forget.T)
    q_mine = lax.all_to_all(q_pack, ("z", "y"), split_axis=0, concat_axis=0, tiled=True)
    kv_own = lax.all_to_all(kv_pack, "z", split_axis=0, concat_axis=0, tiled=True)
    kv_back, kv_ahead = turn(kv_own, "y", 1), turn(kv_own, "y", 3)
    kv_far = turn(kv_own, "y", 2)
    w_other = swap(w_same)
    shards = jnp.concatenate([gate_weight.T, up_weight.T, down_weight], axis=0)
    ffn_all = lax.all_gather(shards, ("z", "y"), axis=0, tiled=False)

    qt, *state = attend(yi, (0,), [kv_own], q=q_mine)
    state = attend(yi, (3, 1), [kv_back, kv_ahead], state=(qt, *state))
    attended = attend(yi, (2,), [kv_far], state=(qt, *state), final=True)
    by_shard = lax.all_to_all(attended, ("z", "y"), split_axis=0, concat_axis=0, tiled=True)
    by_rows = lax.all_to_all(
        spread(by_shard), ("x", "c"), split_axis=0, concat_axis=0, tiled=True
    )
    normed = mix(place, by_rows, stream_in, mix_gain[None], mix_bias[None], w_same, w_other)
    gathered = lax.all_gather(normed, ("x", "c"), axis=0, tiled=False)
    w_in, w_down = prepare(ffn_all)

    far_same, far_other = ffn((2,), place, gathered, w_in, w_down)
    far_swapped = swap(far_other)
    near_same, near_other = ffn((1, 3), place, gathered, w_in, w_down)
    near_swapped = swap(near_other)
    own_same, own_other = ffn((0,), place, gathered, w_in, w_down)
    own_swapped = swap(own_other)
    from_far = turn(join(far_same[0], far_swapped[0]), "x", 2)
    near = [join(near_same[i], near_swapped[i]) for i in range(2)]
    from_back, from_ahead = turn(near[0], "x", 1), turn(near[1], "x", 3)
    parts = [own_same[0], own_swapped[0], from_back, from_ahead, from_far]
    return last(parts, normed, ffn_gain[None], ffn_bias[None])


def solution(mesh):
    fine = Mesh(mesh.devices.reshape(4, 4, 4, 2), ("z", "y", "x", "c"))
    sp, tp = ("z", "y"), ("x", "c")
    placed = (
        P(sp, tp), P(sp, tp), P(sp, tp), P(sp, tp), P(sp, None), P(tp, None), P(), P(),
        P(sp, tp), P(sp, tp), P(tp, sp), P(), P(),
    )

    return jax.shard_map(
        body, mesh=fine, in_specs=placed, out_specs=P(("z", "y", "x", "c"), None), check_vma=False
    )
```

```python
import functools
import jax
import jax.numpy as jnp
import numpy as np
from jax import lax
from jax.experimental import pallas as pl
from jax.experimental.pallas import tpu as pltpu
from jax.sharding import Mesh, PartitionSpec as P


ALPHA = 8.0**0.25
EPSILON = 1e-05
F32 = jnp.float32
BF16 = jnp.bfloat16

ROWS = 768
SUB = 192
HALF = 96
HD = 64
NSH = 16
PACK = 800
TILE = 256
SPLIT = 1
TILES = SUB * NSH // TILE


def vmem():
    return pl.BlockSpec(memory_space=pltpu.VMEM)


def smem():
    return pl.BlockSpec(memory_space=pltpu.SMEM)


def params(mb):
    return pltpu.CompilerParams(vmem_limit_bytes=mb * 1024 * 1024)


def pack_kernel(q_ref, k_ref, v_ref, g_ref, qo_ref, kvo_ref):
    for h in range(4):
        cols = slice(h * HD, (h + 1) * HD)
        kvo_ref[h, 0:ROWS, 0:HD] = k_ref[:, cols]
        kvo_ref[h, 0:ROWS, HD : 2 * HD] = v_ref[:, cols]
        for y in range(4):
            at = y * SUB
            qo_ref[h * 4 + y, :, 0:HD] = q_ref[at : at + HALF, cols]
            qo_ref[h * 4 + y, :, HD : 2 * HD] = q_ref[at + HALF : at + SUB, cols]
        chunks = [-g_ref[h : h + 1, c * 128 : (c + 1) * 128] for c in range(6)]
        value = jnp.concatenate(chunks, axis=0)
        first = value.astype(BF16).astype(F32)
        second = (value - first).astype(BF16).astype(F32)
        third = value - first - second
        rest = jnp.zeros((PACK - ROWS - 18, 128), F32)
        kvo_ref[h, ROWS:PACK, :] = jnp.concatenate(
            [first, second, third, rest], axis=0
        ).astype(BF16)


def pack(q, k, v, g):
    return pl.pallas_call(
        pack_kernel,
        out_shape=(
            jax.ShapeDtypeStruct((NSH, HALF, 128), BF16),
            jax.ShapeDtypeStruct((4, PACK, 128), BF16),
        ),
        in_specs=[vmem()] * 4,
        out_specs=(vmem(), vmem()),
        compiler_params=params(60),
        cost_estimate=pl.CostEstimate(flops=10**6, bytes_accessed=2500000, transcendentals=0),
    )(q, k, v, g)


def unit_table(steps):
    tables, counts = [], []
    for y in range(4):
        units = []
        for t in range(TILES):
            low = (TILE * t) // SUB
            for i, d in enumerate(steps):
                for z in range(4):
                    s = z * 4 + (y + d) % 4
                    if s <= low + 1:
                        units.append((t, i * 4 + z, s, int(s >= low)))
        plain = [u for u in units if not u[3]]
        held = [u for u in units if u[3]]
        if len(plain) % 2:
            held.insert(0, plain.pop())
        if len(held) % 2:
            held.append((0, 0, NSH - 1, 1))
        units = plain + held
        counts.append((len(plain) // 2, len(units) // 2))
        tables.append([(0, 0, 0, 0)] + units + [units[-1]])
    width = max(len(u) for u in tables) + 1
    out = np.zeros((4, 4, width), np.int32)
    for y in range(4):
        out[y, :, : len(tables[y])] = np.array(tables[y], np.int32).T
        out[y, 0:2, -1] = counts[y]
    return out


def attend_kernel(chunks, first, final, *refs):
    refs = list(refs)
    tab, y_ref = refs[:2]
    kv_refs = refs[2 : 2 + chunks]
    at = 2 + chunks
    if first:
        q_ref, qt, top, acc = refs[at : at + 4]
        at += 4
    else:
        qt, top_in, acc_in = refs[at : at + 3]
        at += 3
        if final:
            o_ref = refs[at]
            at += 1
        else:
            top, acc = refs[at : at + 2]
            at += 2
    kaug, vt, qpos, s_a, s_b, p_a, p_b, al_a, al_b, mx_a, mx_b = refs[at : at + 11]
    at += 11
    if first:
        qrow = refs[at]
    if final:
        top, acc, oscr = refs[at : at + 3]
    y = y_ref[0]
    lane = lax.broadcasted_iota(jnp.int32, (128, 128), 1)
    for i in range(chunks):
        kv_ref = kv_refs[i]

        def per_shard(s, carry):
            gates = kv_ref[s, ROWS:PACK, :].astype(F32)
            square = jnp.concatenate(
                [jnp.zeros((HD, 128), F32), gates, jnp.zeros((32, 128), F32)], axis=0
            )
            turned = square.T
            to = i * 4 + s
            for c in range(6):
                part = kv_ref[s, c * 128 : (c + 1) * 128, :].astype(F32)
                mine = (lane == HD + c) | (lane == HD + 6 + c) | (lane == HD + 12 + c)
                kaug[to, c * 128 : (c + 1) * 128, :] = jnp.where(
                    lane < HD, part, jnp.where(mine, turned, 0.0)
                ).astype(BF16)
                vt[to, :, c * 128 : (c + 1) * 128] = part.T.astype(BF16)
            vt[to, 48:64, :] = jnp.ones((16, ROWS), BF16)
            return carry

        lax.fori_loop(0, 4, per_shard, 0)

    lane_h = lax.broadcasted_iota(jnp.int32, (HALF, 128), 1)
    lane_t = lax.broadcasted_iota(jnp.int32, (8, TILE), 1)
    if first:

        def per_query(s, carry):
            both = q_ref[s].astype(F32) * (HD**-0.5)
            ones = jnp.where(lane_h < HD + 18, 1.0, 0.0)
            qrow[s, 0:HALF, :] = jnp.where(lane_h < HD, both, ones)
            qrow[s, HALF:SUB, :] = jnp.where(lane_h < HD, pltpu.roll(both, HD, 1), ones)
            return carry

        lax.fori_loop(0, NSH, per_query, 0)
    for t in range(TILES):
        low = (TILE * t) // SUB
        edge = (low + 1) * SUB - TILE * t
        qpos[t] = y * SUB + jnp.where(
            lane_t < edge,
            low * ROWS + (SUB - edge) + lane_t,
            (low + 1) * ROWS + lane_t - edge,
        )
        if first:
            rows = jnp.concatenate(
                [qrow[low, SUB - edge : SUB, :], qrow[low + 1, 0 : TILE - edge, :]], axis=0
            )
            qt[t] = rows.T.astype(BF16)
    if first:
        acc[...] = jnp.zeros(acc.shape, F32)
        top[...] = jnp.full(top.shape, -1e30, F32)
    else:
        acc[...] = acc_in[...]
        top[...] = top_in[...]
    al_b[...] = jnp.ones(al_b.shape, F32)
    p_b[...] = jnp.zeros(p_b.shape, BF16)

    def scores(u, out, most, masked):
        rows = ROWS // SPLIT
        high = None
        for i in range(SPLIT):
            part = slice(i * rows, (i + 1) * rows)
            s = jnp.dot(
                kaug[tab[y, 1, u], part, :], qt[tab[y, 0, u]], preferred_element_type=F32
            )
            if masked:
                pos = tab[y, 2, u] * ROWS + i * rows
                pos = pos + lax.broadcasted_iota(jnp.int32, (rows, TILE), 0)
                s = jnp.where(pos <= qpos[tab[y, 0, u], 0:1, :], s, -1e30)
            out[part, :] = s
            here = jnp.max(s.reshape(rows // 8, 8, TILE), axis=0)
            high = here if high is None else jnp.maximum(high, here)
        most[...] = high

    def gather(u, p_before, al_before):
        t = tab[y, 0, u]
        pv = jnp.dot(vt[tab[y, 1, u], 48:128, :], p_before[...], preferred_element_type=F32)
        acc[t] = acc[t] * al_before[0:1, :] + pv

    def unit(u, now, later, before, masked):
        s_now, p_now, al_now, mx_now = now
        s_next, _, _, mx_next = later
        _, p_before, al_before, _ = before
        t = tab[y, 0, u]
        old = top[t, 0:1, :]
        high = jnp.maximum(old, jnp.max(mx_now[...], axis=0, keepdims=True))
        top[t, 0:1, :] = high
        al_now[0:1, :] = jnp.exp(old - high)
        scores(u + 1, s_next, mx_next, masked)
        p_now[...] = jnp.exp(s_now[...] - high).astype(BF16)
        gather(u - 1, p_before, al_before)

    one, two = (s_a, p_a, al_a, mx_a), (s_b, p_b, al_b, mx_b)
    last_at = tab.shape[2] - 1
    plain, pairs = tab[y, 0, last_at], tab[y, 1, last_at]
    for masked, low, high in ((False, 0, plain), (True, plain, pairs)):

        def pair(i, carry):
            unit(2 * i + 1, one, two, two, masked)
            unit(2 * i + 2, two, one, one, masked)
            return carry

        scores(2 * low + 1, s_a, mx_a, masked)
        lax.fori_loop(low, high, pair, 0)
    gather(2 * pairs, p_b, al_b)

    if final:

        def finish(t, carry):
            good = acc[t, 16:80, :] / acc[t, 0:1, :]
            full = jnp.concatenate([good, jnp.zeros((HD, TILE), F32)], axis=0)
            oscr[pl.ds(pl.multiple_of(t * TILE, TILE), TILE), :] = full.T
            return carry

        lax.fori_loop(0, TILES, finish, 0)

        def out(s, carry):
            row = pl.multiple_of(s * SUB, SUB)
            one = oscr[pl.ds(row, HALF), :]
            two = oscr[pl.ds(row + HALF, HALF), :]
            o_ref[s] = jnp.where(lane_h < HD, one, pltpu.roll(two, HD, 1)).astype(BF16)
            return carry

        lax.fori_loop(0, NSH, out, 0)


def attend(y, steps, kvs, q=None, state=None, final=False):
    chunks, first = len(kvs), q is not None
    state_shapes = (
        jax.ShapeDtypeStruct((TILES, 8, TILE), F32),
        jax.ShapeDtypeStruct((TILES, 80, TILE), F32),
    )
    scratch = [
        pltpu.VMEM((4 * chunks, ROWS, 128), BF16),
        pltpu.VMEM((4 * chunks, 128, ROWS), BF16),
        pltpu.VMEM((TILES, 8, TILE), jnp.int32),
        pltpu.VMEM((ROWS, TILE), F32),
        pltpu.VMEM((ROWS, TILE), F32),
        pltpu.VMEM((ROWS, TILE), BF16),
        pltpu.VMEM((ROWS, TILE), BF16),
    ] + [pltpu.VMEM((8, TILE), F32)] * 4
    if first:
        outs = (jax.ShapeDtypeStruct((TILES, 128, TILE), BF16),) + state_shapes
        scratch += [pltpu.VMEM((NSH, SUB, 128), F32)]
        rest = [q]
    elif final:
        outs = jax.ShapeDtypeStruct((NSH, HALF, 128), BF16)
        scratch += [pltpu.VMEM(s.shape, F32) for s in state_shapes]
        scratch += [pltpu.VMEM((SUB * NSH, 128), F32)]
        rest = list(state)
    else:
        outs = state_shapes
        rest = list(state)
    table = unit_table(steps)
    share = 2 * int(table[:, 1, -1].mean())
    return pl.pallas_call(
        functools.partial(attend_kernel, chunks, first, final),
        out_shape=outs,
        in_specs=[smem(), smem()] + [vmem()] * (chunks + len(rest)),
        out_specs=jax.tree.map(lambda _: vmem(), outs),
        scratch_shapes=scratch,
        compiler_params=params(60),
        cost_estimate=pl.CostEstimate(
            flops=share * 4 * 10**8, bytes_accessed=3 * 10**6, transcendentals=share * 200000
        ),
    )(jnp.asarray(table), y, *kvs, *rest)


def spread_kernel(o_ref, a_ref):
    for z in range(4):
        for y in range(4):
            for half in range(2):
                a_ref[2 * y + half, :, z * HD : (z + 1) * HD] = o_ref[
                    4 * z + y, :, half * HD : (half + 1) * HD
                ]


def spread(o):
    return pl.pallas_call(
        spread_kernel,
        out_shape=jax.ShapeDtypeStruct((8, HALF, 256), BF16),
        in_specs=[vmem()],
        out_specs=vmem(),
        compiler_params=params(60),
        cost_estimate=pl.CostEstimate(flops=10**5, bytes_accessed=800000, transcendentals=0),
    )(o)


def norm_rows(matrix, gain, shift):
    centred = matrix - jnp.mean(matrix, axis=-1, keepdims=True)
    spread_ = jnp.mean(centred * centred, axis=-1, keepdims=True)
    return centred * lax.rsqrt(spread_ + EPSILON) * gain + shift


def mix_kernel(place, a_ref, stream_ref, gain_ref, bias_ref, same_ref, other_ref, n_ref, total):
    c, x = place[0], pl.program_id(0)
    term = jnp.dot(a_ref[2 * x + c], same_ref[0], preferred_element_type=F32)
    term = term + jnp.dot(a_ref[2 * x + 1 - c], other_ref[0], preferred_element_type=F32)

    @pl.when(x == 0)
    def _():
        total[...] = term

    @pl.when(x > 0)
    def _():
        total[...] += term

    @pl.when(x == 3)
    def _():
        mixed = total[...].astype(BF16).astype(F32)
        matrix = ALPHA * stream_ref[...].astype(F32) + mixed
        n_ref[...] = norm_rows(matrix, gain_ref[...], bias_ref[...]).astype(BF16)


def whole(shape):
    return pl.BlockSpec(shape, lambda i, place: (0,) * len(shape))


def along(shape):
    return pl.BlockSpec((1, *shape), lambda i, place: (i,) + (0,) * len(shape))


def mix(place, att, stream, gain, bias, same, other):
    return pl.pallas_call(
        mix_kernel,
        out_shape=jax.ShapeDtypeStruct((HALF, 2048), BF16),
        grid_spec=pltpu.PrefetchScalarGridSpec(
            num_scalar_prefetch=1,
            grid=(4,),
            in_specs=[
                whole((8, HALF, 256)),
                pl.BlockSpec((HALF, 2048), lambda i, place: (place[1], 0)),
                whole((1, 2048)),
                whole((1, 2048)),
                along((256, 2048)),
                along((256, 2048)),
            ],
            out_specs=whole((HALF, 2048)),
            scratch_shapes=[pltpu.VMEM((HALF, 2048), F32)],
        ),
        compiler_params=params(60),
        cost_estimate=pl.CostEstimate(
            flops=2 * HALF * 2048 * 2048, bytes_accessed=9 * 10**6, transcendentals=0
        ),
    )(place, att, stream, gain, bias, same, other)


BLOCKS = 3


def ffn_kernel(count, *refs):
    x_refs = refs[: 2 * count]
    w_ref, same_ref, other_ref = refs[2 * count :]
    x = jnp.concatenate([r[...] for r in x_refs], axis=0)

    def rows(at, width):
        return jnp.concatenate([w_ref[s, at : at + width, :] for s in range(NSH)], axis=1)

    total = None
    for j in range(BLOCKS):
        width = min(256, 704 - 256 * j)
        across = (((1,), (1,)), ((), ()))
        gate = lax.dot_general(x, rows(256 * j, width), across, preferred_element_type=F32)
        up = lax.dot_general(x, rows(704 + 256 * j, width), across, preferred_element_type=F32)
        hidden = (gate / (1.0 + jnp.exp(-gate)) * up).astype(BF16)
        term = jnp.dot(hidden, rows(1408 + 256 * j, width), preferred_element_type=F32)
        total = term if total is None else total + term
    out = total.astype(BF16)
    for i in range(count):
        same_ref[i] = out[i * HALF : (i + 1) * HALF]
        other_ref[i] = out[(count + i) * HALF : (count + i + 1) * HALF]


def ffn(pieces, w):
    count = len(pieces) // 2
    shape = jax.ShapeDtypeStruct((count, HALF, 2048), BF16)
    rows = 2 * count * HALF
    return pl.pallas_call(
        functools.partial(ffn_kernel, count),
        out_shape=(shape, shape),
        in_specs=[vmem()] * (2 * count + 1),
        out_specs=(vmem(), vmem()),
        compiler_params=params(30),
        cost_estimate=pl.CostEstimate(
            flops=6 * rows * 2048 * 704, bytes_accessed=10**7, transcendentals=rows * 704
        ),
    )(*pieces, w)


def join_kernel(count, *refs):
    same_ref, other_ref = refs[:2]
    for i in range(count):
        refs[2 + i][...] = (same_ref[i].astype(F32) + other_ref[i].astype(F32)).astype(BF16)


def join(same, other):
    count = same.shape[0]
    shape = jax.ShapeDtypeStruct((HALF, 2048), BF16)
    return pl.pallas_call(
        functools.partial(join_kernel, count),
        out_shape=(shape,) * count,
        in_specs=[vmem()] * 2,
        out_specs=(vmem(),) * count,
        compiler_params=params(8),
        cost_estimate=pl.CostEstimate(flops=10**6, bytes_accessed=10**6, transcendentals=0),
    )(same, other)


def last_kernel(n_ref, gain_ref, bias_ref, *refs):
    o_ref = refs[-1]
    total = refs[0][...].astype(F32)
    for r in refs[1:-1]:
        total = total + r[...].astype(F32)
    lowered = total.astype(BF16).astype(F32)
    matrix = ALPHA * n_ref[...].astype(F32) + lowered
    o_ref[...] = norm_rows(matrix, gain_ref[...], bias_ref[...]).astype(BF16)


def last(parts, normed, gain, bias):
    return pl.pallas_call(
        last_kernel,
        out_shape=jax.ShapeDtypeStruct((HALF, 2048), BF16),
        in_specs=[vmem()] * (3 + len(parts)),
        out_specs=vmem(),
        compiler_params=params(60),
        cost_estimate=pl.CostEstimate(
            flops=4 * 10**6, bytes_accessed=4 * 10**6, transcendentals=0
        ),
    )(normed, gain, bias, *parts)


def body(
    queries, key_rows, value_rows, log_forget, stream_in, out_weight, mix_gain, mix_bias,
    gate_weight, up_weight, down_weight, ffn_gain, ffn_bias,
):
    yi = lax.axis_index("y").astype(jnp.int32)[None]
    xi = lax.axis_index("x")
    ci = lax.axis_index("c")

    def turn(value, axis, d):
        return lax.ppermute(value, axis, [(i, (i + d) % 4) for i in range(4)])

    def swap(value):
        return lax.ppermute(value, "c", [(0, 1), (1, 0)])

    place = jnp.stack([ci, 2 * xi + ci, xi]).astype(jnp.int32)
    w_same = lax.all_gather(out_weight, "x", axis=0, tiled=False)
    q_pack, kv_pack = pack(queries, key_rows, value_rows, log_forget.T)
    q_mine = lax.all_to_all(q_pack, ("z", "y"), split_axis=0, concat_axis=0, tiled=True)
    kv_own = lax.all_to_all(kv_pack, "z", split_axis=0, concat_axis=0, tiled=True)
    kv_back, kv_ahead = turn(kv_own, "y", 1), turn(kv_own, "y", 3)
    kv_far = turn(kv_own, "y", 2)
    w_other = swap(w_same)
    shards = jnp.concatenate([gate_weight.T, up_weight.T, down_weight], axis=0)
    ffn_all = lax.all_gather(shards, ("z", "y"), axis=0, tiled=False)

    qt, *state = attend(yi, (0,), [kv_own], q=q_mine)
    state = attend(yi, (3, 1), [kv_back, kv_ahead], state=(qt, *state))
    attended = attend(yi, (2,), [kv_far], state=(qt, *state), final=True)
    by_shard = lax.all_to_all(attended, ("z", "y"), split_axis=0, concat_axis=0, tiled=True)
    by_rows = lax.all_to_all(
        spread(by_shard), ("x", "c"), split_axis=0, concat_axis=0, tiled=True
    )
    normed = mix(place, by_rows, stream_in, mix_gain[None], mix_bias[None], w_same, w_other)
    back, ahead = turn(normed, "x", 1), turn(normed, "x", 3)
    n_swapped = swap(normed)
    own_same, own_other = ffn((normed, n_swapped), ffn_all)
    own_swapped = swap(own_other)
    far = turn(back, "x", 1)
    near = (back, ahead, swap(back), swap(ahead))
    near_same, near_other = ffn(near, ffn_all)
    near_swapped = swap(near_other)
    far_other_rows = swap(far)
    to_back, to_ahead = join(near_same, near_swapped)
    from_ahead, from_back = turn(to_back, "x", 3), turn(to_ahead, "x", 1)
    far_same, far_other = ffn((far, far_other_rows), ffn_all)
    far_swapped = swap(far_other)
    (to_far,) = join(far_same, far_swapped)
    from_far = turn(to_far, "x", 2)
    parts = [own_same[0], own_swapped[0], from_back, from_ahead, from_far]
    return last(parts, normed, ffn_gain[None], ffn_bias[None])


def solution(mesh):
    fine = Mesh(mesh.devices.reshape(4, 4, 4, 2), ("z", "y", "x", "c"))
    sp, tp = ("z", "y"), ("x", "c")
    placed = (
        P(sp, tp), P(sp, tp), P(sp, tp), P(sp, tp), P(sp, None), P(tp, None), P(), P(),
        P(sp, tp), P(sp, tp), P(tp, sp), P(), P(),
    )

    return jax.shard_map(
        body, mesh=fine, in_specs=placed, out_specs=P(("z", "y", "x", "c"), None), check_vma=False
    )
```

```python
import functools
import jax
import jax.numpy as jnp
import numpy as np
from jax import lax
from jax.experimental import pallas as pl
from jax.experimental.pallas import tpu as pltpu
from jax.sharding import Mesh, PartitionSpec as P


ALPHA = 8.0**0.25
EPSILON = 1e-05
F32 = jnp.float32
BF16 = jnp.bfloat16

ROWS = 768
SUB = 192
HALF = 96
HD = 64
NSH = 16
PACK = 800
TILE = 256
SPLIT = 1
TILES = SUB * NSH // TILE


def vmem():
    return pl.BlockSpec(memory_space=pltpu.VMEM)


def smem():
    return pl.BlockSpec(memory_space=pltpu.SMEM)


def params(mb):
    return pltpu.CompilerParams(vmem_limit_bytes=mb * 1024 * 1024)


def pack_kernel(q_ref, k_ref, v_ref, g_ref, qo_ref, kvo_ref):
    for h in range(4):
        cols = slice(h * HD, (h + 1) * HD)
        kvo_ref[h, 0:ROWS, 0:HD] = k_ref[:, cols]
        kvo_ref[h, 0:ROWS, HD : 2 * HD] = v_ref[:, cols]
        for y in range(4):
            at = y * SUB
            qo_ref[h * 4 + y, :, 0:HD] = q_ref[at : at + HALF, cols]
            qo_ref[h * 4 + y, :, HD : 2 * HD] = q_ref[at + HALF : at + SUB, cols]
        chunks = [-g_ref[h : h + 1, c * 128 : (c + 1) * 128] for c in range(6)]
        value = jnp.concatenate(chunks, axis=0)
        first = value.astype(BF16).astype(F32)
        second = (value - first).astype(BF16).astype(F32)
        third = value - first - second
        rest = jnp.zeros((PACK - ROWS - 18, 128), F32)
        kvo_ref[h, ROWS:PACK, :] = jnp.concatenate(
            [first, second, third, rest], axis=0
        ).astype(BF16)


def pack(q, k, v, g):
    return pl.pallas_call(
        pack_kernel,
        out_shape=(
            jax.ShapeDtypeStruct((NSH, HALF, 128), BF16),
            jax.ShapeDtypeStruct((4, PACK, 128), BF16),
        ),
        in_specs=[vmem()] * 4,
        out_specs=(vmem(), vmem()),
        compiler_params=params(60),
        cost_estimate=pl.CostEstimate(flops=10**6, bytes_accessed=2500000, transcendentals=0),
    )(q, k, v, g)


def unit_table(steps):
    tables, counts = [], []
    for y in range(4):
        units = []
        for t in range(TILES):
            low = (TILE * t) // SUB
            for i, d in enumerate(steps):
                for z in range(4):
                    s = z * 4 + (y + d) % 4
                    if s <= low + 1:
                        units.append((t, i * 4 + z, s, int(s >= low)))
        plain = [u for u in units if not u[3]]
        held = [u for u in units if u[3]]
        if len(plain) % 2:
            held.insert(0, plain.pop())
        if len(held) % 2:
            held.append((0, 0, NSH - 1, 1))
        units = plain + held
        counts.append((len(plain) // 2, len(units) // 2))
        tables.append([(0, 0, 0, 0)] + units + [units[-1]])
    width = max(len(u) for u in tables) + 1
    out = np.zeros((4, 4, width), np.int32)
    for y in range(4):
        out[y, :, : len(tables[y])] = np.array(tables[y], np.int32).T
        out[y, 0:2, -1] = counts[y]
    return out


def attend_kernel(chunks, first, final, *refs):
    refs = list(refs)
    tab, y_ref = refs[:2]
    kv_refs = refs[2 : 2 + chunks]
    at = 2 + chunks
    if first:
        q_ref, qt, top, acc = refs[at : at + 4]
        at += 4
    else:
        qt, top_in, acc_in = refs[at : at + 3]
        at += 3
        if final:
            o_ref = refs[at]
            at += 1
        else:
            top, acc = refs[at : at + 2]
            at += 2
    kaug, vt, qpos, s_a, s_b, p_a, p_b, al_a, al_b, mx_a, mx_b = refs[at : at + 11]
    at += 11
    if first:
        qrow = refs[at]
    if final:
        top, acc, oscr = refs[at : at + 3]
    y = y_ref[0]
    lane = lax.broadcasted_iota(jnp.int32, (1, 128), 1)
    for i in range(chunks):
        kv_ref = kv_refs[i]

        def per_shard(s, carry):
            gates = kv_ref[s, ROWS:PACK, :].astype(F32)
            square = jnp.concatenate(
                [jnp.zeros((HD, 128), F32), gates, jnp.zeros((32, 128), F32)], axis=0
            )
            turned = square.T
            to = i * 4 + s
            for c in range(6):
                part = kv_ref[s, c * 128 : (c + 1) * 128, :]
                mine = (lane == HD + c) | (lane == HD + 6 + c) | (lane == HD + 12 + c)
                biased = jnp.where(mine, turned, 0.0).astype(BF16)
                kaug[to, c * 128 : (c + 1) * 128, :] = jnp.where(lane < HD, part, biased)
                vt[to, :, c * 128 : (c + 1) * 128] = part.T
            vt[to, 48:64, :] = jnp.ones((16, ROWS), BF16)
            return carry

        lax.fori_loop(0, 4, per_shard, 0)

    lane_h = lax.broadcasted_iota(jnp.int32, (HALF, 128), 1)
    lane_t = lax.broadcasted_iota(jnp.int32, (8, TILE), 1)
    if first:

        def per_query(s, carry):
            both = q_ref[s].astype(F32) * (HD**-0.5)
            ones = jnp.where(lane_h < HD + 18, 1.0, 0.0)
            qrow[s, 0:HALF, :] = jnp.where(lane_h < HD, both, ones)
            qrow[s, HALF:SUB, :] = jnp.where(lane_h < HD, pltpu.roll(both, HD, 1), ones)
            return carry

        lax.fori_loop(0, NSH, per_query, 0)
    for t in range(TILES):
        low = (TILE * t) // SUB
        edge = (low + 1) * SUB - TILE * t
        qpos[t] = y * SUB + jnp.where(
            lane_t < edge,
            low * ROWS + (SUB - edge) + lane_t,
            (low + 1) * ROWS + lane_t - edge,
        )
        if first:
            rows = jnp.concatenate(
                [qrow[low, SUB - edge : SUB, :], qrow[low + 1, 0 : TILE - edge, :]], axis=0
            )
            qt[t] = rows.T.astype(BF16)
    if first:
        acc[...] = jnp.zeros(acc.shape, F32)
        top[...] = jnp.full(top.shape, -1e30, F32)
    else:
        acc[...] = acc_in[...]
        top[...] = top_in[...]
    al_b[...] = jnp.ones(al_b.shape, F32)
    p_b[...] = jnp.zeros(p_b.shape, BF16)

    def scores(u, out, most, masked):
        rows = ROWS // SPLIT
        high = None
        for i in range(SPLIT):
            part = slice(i * rows, (i + 1) * rows)
            s = jnp.dot(
                kaug[tab[y, 1, u], part, :], qt[tab[y, 0, u]], preferred_element_type=F32
            )
            if masked:
                pos = tab[y, 2, u] * ROWS + i * rows
                pos = pos + lax.broadcasted_iota(jnp.int32, (rows, TILE), 0)
                s = jnp.where(pos <= qpos[tab[y, 0, u], 0:1, :], s, -1e30)
            out[part, :] = s
            here = jnp.max(s.reshape(rows // 8, 8, TILE), axis=0)
            high = here if high is None else jnp.maximum(high, here)
        most[...] = high

    def gather(u, p_before, al_before):
        t = tab[y, 0, u]
        pv = jnp.dot(vt[tab[y, 1, u], 48:128, :], p_before[...], preferred_element_type=F32)
        acc[t] = acc[t] * al_before[0:1, :] + pv

    def unit(u, now, later, before, masked):
        s_now, p_now, al_now, mx_now = now
        s_next, _, _, mx_next = later
        _, p_before, al_before, _ = before
        t = tab[y, 0, u]
        old = top[t, 0:1, :]
        high = jnp.maximum(old, jnp.max(mx_now[...], axis=0, keepdims=True))
        top[t, 0:1, :] = high
        al_now[0:1, :] = jnp.exp(old - high)
        scores(u + 1, s_next, mx_next, masked)
        p_now[...] = jnp.exp(s_now[...] - high).astype(BF16)
        gather(u - 1, p_before, al_before)

    one, two = (s_a, p_a, al_a, mx_a), (s_b, p_b, al_b, mx_b)
    last_at = tab.shape[2] - 1
    plain, pairs = tab[y, 0, last_at], tab[y, 1, last_at]
    for masked, low, high in ((False, 0, plain), (True, plain, pairs)):

        def pair(i, carry):
            unit(2 * i + 1, one, two, two, masked)
            unit(2 * i + 2, two, one, one, masked)
            return carry

        scores(2 * low + 1, s_a, mx_a, masked)
        lax.fori_loop(low, high, pair, 0)
    gather(2 * pairs, p_b, al_b)

    if final:

        def finish(t, carry):
            good = acc[t, 16:80, :] / acc[t, 0:1, :]
            full = jnp.concatenate([good, jnp.zeros((HD, TILE), F32)], axis=0)
            oscr[pl.ds(pl.multiple_of(t * TILE, TILE), TILE), :] = full.T
            return carry

        lax.fori_loop(0, TILES, finish, 0)

        def out(s, carry):
            row = pl.multiple_of(s * SUB, SUB)
            one = oscr[pl.ds(row, HALF), :]
            two = oscr[pl.ds(row + HALF, HALF), :]
            o_ref[s] = jnp.where(lane_h < HD, one, pltpu.roll(two, HD, 1)).astype(BF16)
            return carry

        lax.fori_loop(0, NSH, out, 0)


def attend(y, steps, kvs, q=None, state=None, final=False):
    chunks, first = len(kvs), q is not None
    state_shapes = (
        jax.ShapeDtypeStruct((TILES, 8, TILE), F32),
        jax.ShapeDtypeStruct((TILES, 80, TILE), F32),
    )
    scratch = [
        pltpu.VMEM((4 * chunks, ROWS, 128), BF16),
        pltpu.VMEM((4 * chunks, 128, ROWS), BF16),
        pltpu.VMEM((TILES, 8, TILE), jnp.int32),
        pltpu.VMEM((ROWS, TILE), F32),
        pltpu.VMEM((ROWS, TILE), F32),
        pltpu.VMEM((ROWS, TILE), BF16),
        pltpu.VMEM((ROWS, TILE), BF16),
    ] + [pltpu.VMEM((8, TILE), F32)] * 4
    if first:
        outs = (jax.ShapeDtypeStruct((TILES, 128, TILE), BF16),) + state_shapes
        scratch += [pltpu.VMEM((NSH, SUB, 128), F32)]
        rest = [q]
    elif final:
        outs = jax.ShapeDtypeStruct((NSH, HALF, 128), BF16)
        scratch += [pltpu.VMEM(s.shape, F32) for s in state_shapes]
        scratch += [pltpu.VMEM((SUB * NSH, 128), F32)]
        rest = list(state)
    else:
        outs = state_shapes
        rest = list(state)
    table = unit_table(steps)
    share = 2 * int(table[:, 1, -1].mean())
    return pl.pallas_call(
        functools.partial(attend_kernel, chunks, first, final),
        out_shape=outs,
        in_specs=[smem(), smem()] + [vmem()] * (chunks + len(rest)),
        out_specs=jax.tree.map(lambda _: vmem(), outs),
        scratch_shapes=scratch,
        compiler_params=params(60),
        cost_estimate=pl.CostEstimate(
            flops=share * 4 * 10**8, bytes_accessed=3 * 10**6, transcendentals=share * 200000
        ),
    )(jnp.asarray(table), y, *kvs, *rest)


def spread_kernel(o_ref, a_ref):
    for z in range(4):
        for y in range(4):
            for half in range(2):
                a_ref[2 * y + half, :, z * HD : (z + 1) * HD] = o_ref[
                    4 * z + y, :, half * HD : (half + 1) * HD
                ]


def spread(o):
    return pl.pallas_call(
        spread_kernel,
        out_shape=jax.ShapeDtypeStruct((8, HALF, 256), BF16),
        in_specs=[vmem()],
        out_specs=vmem(),
        compiler_params=params(60),
        cost_estimate=pl.CostEstimate(flops=10**5, bytes_accessed=800000, transcendentals=0),
    )(o)


def norm_rows(matrix, gain, shift):
    centred = matrix - jnp.mean(matrix, axis=-1, keepdims=True)
    spread_ = jnp.mean(centred * centred, axis=-1, keepdims=True)
    return centred * lax.rsqrt(spread_ + EPSILON) * gain + shift


def mix_kernel(place, a_ref, stream_ref, gain_ref, bias_ref, same_ref, other_ref, n_ref, total):
    c, x = place[0], pl.program_id(0)
    term = jnp.dot(a_ref[2 * x + c], same_ref[0], preferred_element_type=F32)
    term = term + jnp.dot(a_ref[2 * x + 1 - c], other_ref[0], preferred_element_type=F32)

    @pl.when(x == 0)
    def _():
        total[...] = term

    @pl.when(x > 0)
    def _():
        total[...] += term

    @pl.when(x == 3)
    def _():
        mixed = total[...].astype(BF16).astype(F32)
        matrix = ALPHA * stream_ref[...].astype(F32) + mixed
        n_ref[...] = norm_rows(matrix, gain_ref[...], bias_ref[...]).astype(BF16)


def whole(shape):
    return pl.BlockSpec(shape, lambda i, place: (0,) * len(shape))


def along(shape):
    return pl.BlockSpec((1, *shape), lambda i, place: (i,) + (0,) * len(shape))


def mix(place, att, stream, gain, bias, same, other):
    return pl.pallas_call(
        mix_kernel,
        out_shape=jax.ShapeDtypeStruct((HALF, 2048), BF16),
        grid_spec=pltpu.PrefetchScalarGridSpec(
            num_scalar_prefetch=1,
            grid=(4,),
            in_specs=[
                whole((8, HALF, 256)),
                pl.BlockSpec((HALF, 2048), lambda i, place: (place[1], 0)),
                whole((1, 2048)),
                whole((1, 2048)),
                along((256, 2048)),
                along((256, 2048)),
            ],
            out_specs=whole((HALF, 2048)),
            scratch_shapes=[pltpu.VMEM((HALF, 2048), F32)],
        ),
        compiler_params=params(60),
        cost_estimate=pl.CostEstimate(
            flops=2 * HALF * 2048 * 2048, bytes_accessed=9 * 10**6, transcendentals=0
        ),
    )(place, att, stream, gain, bias, same, other)


BLOCKS = 3


def ffn_kernel(count, *refs):
    x_refs = refs[: 2 * count]
    w_ref, same_ref, other_ref = refs[2 * count :]
    x = jnp.concatenate([r[...] for r in x_refs], axis=0)

    def rows(at, width):
        return jnp.concatenate([w_ref[s, at : at + width, :] for s in range(NSH)], axis=1)

    total = None
    for j in range(BLOCKS):
        width = min(256, 704 - 256 * j)
        across = (((1,), (1,)), ((), ()))
        gate = lax.dot_general(x, rows(256 * j, width), across, preferred_element_type=F32)
        up = lax.dot_general(x, rows(704 + 256 * j, width), across, preferred_element_type=F32)
        hidden = (gate / (1.0 + jnp.exp(-gate)) * up).astype(BF16)
        term = jnp.dot(hidden, rows(1408 + 256 * j, width), preferred_element_type=F32)
        total = term if total is None else total + term
    out = total.astype(BF16)
    for i in range(count):
        same_ref[i] = out[i * HALF : (i + 1) * HALF]
        other_ref[i] = out[(count + i) * HALF : (count + i + 1) * HALF]


def ffn(pieces, w):
    count = len(pieces) // 2
    shape = jax.ShapeDtypeStruct((count, HALF, 2048), BF16)
    rows = 2 * count * HALF
    return pl.pallas_call(
        functools.partial(ffn_kernel, count),
        out_shape=(shape, shape),
        in_specs=[vmem()] * (2 * count + 1),
        out_specs=(vmem(), vmem()),
        compiler_params=params(30),
        cost_estimate=pl.CostEstimate(
            flops=6 * rows * 2048 * 704, bytes_accessed=10**7, transcendentals=rows * 704
        ),
    )(*pieces, w)


def join_kernel(split, *refs):
    same_ref, other_ref = refs[:2]
    outs = refs[2:]
    for i in range(same_ref.shape[0]):
        both = (same_ref[i].astype(F32) + other_ref[i].astype(F32)).astype(BF16)
        for k in range(split):
            rows = HALF // split
            outs[i * split + k][...] = both[k * rows : (k + 1) * rows]


def join(same, other, split=1):
    count = same.shape[0] * split
    shape = jax.ShapeDtypeStruct((HALF // split, 2048), BF16)
    return pl.pallas_call(
        functools.partial(join_kernel, split),
        out_shape=(shape,) * count,
        in_specs=[vmem()] * 2,
        out_specs=(vmem(),) * count,
        compiler_params=params(8),
        cost_estimate=pl.CostEstimate(flops=10**6, bytes_accessed=10**6, transcendentals=0),
    )(same, other)


def last_kernel(n_ref, gain_ref, bias_ref, *refs):
    o_ref = refs[-1]
    total = jnp.concatenate([r[...].astype(F32) for r in refs[-3:-1]], axis=0)
    for r in refs[:-3]:
        total = total + r[...].astype(F32)
    lowered = total.astype(BF16).astype(F32)
    matrix = ALPHA * n_ref[...].astype(F32) + lowered
    o_ref[...] = norm_rows(matrix, gain_ref[...], bias_ref[...]).astype(BF16)


def last(parts, normed, gain, bias):
    return pl.pallas_call(
        last_kernel,
        out_shape=jax.ShapeDtypeStruct((HALF, 2048), BF16),
        in_specs=[vmem()] * (3 + len(parts)),
        out_specs=vmem(),
        compiler_params=params(60),
        cost_estimate=pl.CostEstimate(
            flops=4 * 10**6, bytes_accessed=4 * 10**6, transcendentals=0
        ),
    )(normed, gain, bias, *parts)


def body(
    queries, key_rows, value_rows, log_forget, stream_in, out_weight, mix_gain, mix_bias,
    gate_weight, up_weight, down_weight, ffn_gain, ffn_bias,
):
    yi = lax.axis_index("y").astype(jnp.int32)[None]
    xi = lax.axis_index("x")
    ci = lax.axis_index("c")

    def turn(value, axis, d):
        return lax.ppermute(value, axis, [(i, (i + d) % 4) for i in range(4)])

    def swap(value):
        return lax.ppermute(value, "c", [(0, 1), (1, 0)])

    place = jnp.stack([ci, 2 * xi + ci, xi]).astype(jnp.int32)
    w_same = lax.all_gather(out_weight, "x", axis=0, tiled=False)
    q_pack, kv_pack = pack(queries, key_rows, value_rows, log_forget.T)
    q_mine = lax.all_to_all(q_pack, ("z", "y"), split_axis=0, concat_axis=0, tiled=True)
    kv_own = lax.all_to_all(kv_pack, "z", split_axis=0, concat_axis=0, tiled=True)
    kv_back, kv_ahead = turn(kv_own, "y", 1), turn(kv_own, "y", 3)
    kv_far = turn(kv_own, "y", 2)
    w_other = swap(w_same)
    shards = jnp.concatenate([gate_weight.T, up_weight.T, down_weight], axis=0)
    ffn_all = lax.all_gather(shards, ("z", "y"), axis=0, tiled=False)

    qt, *state = attend(yi, (0,), [kv_own], q=q_mine)
    state = attend(yi, (3, 1), [kv_back, kv_ahead], state=(qt, *state))
    attended = attend(yi, (2,), [kv_far], state=(qt, *state), final=True)
    by_shard = lax.all_to_all(attended, ("z", "y"), split_axis=0, concat_axis=0, tiled=True)
    by_rows = lax.all_to_all(
        spread(by_shard), ("x", "c"), split_axis=0, concat_axis=0, tiled=True
    )
    normed = mix(place, by_rows, stream_in, mix_gain[None], mix_bias[None], w_same, w_other)
    back, ahead = turn(normed, "x", 1), turn(normed, "x", 3)
    n_swapped = swap(normed)
    own_same, own_other = ffn((normed, n_swapped), ffn_all)
    own_swapped = swap(own_other)
    far = turn(back, "x", 1)
    near = (back, ahead, swap(back), swap(ahead))
    near_same, near_other = ffn(near, ffn_all)
    near_swapped = swap(near_other)
    far_other_rows = swap(far)
    to_back, to_ahead = join(near_same, near_swapped)
    from_ahead, from_back = turn(to_back, "x", 3), turn(to_ahead, "x", 1)
    far_same, far_other = ffn((far, far_other_rows), ffn_all)
    far_swapped = swap(far_other)
    to_far, to_far_round = join(far_same, far_swapped, 2)
    from_far = turn(to_far, "x", 2)
    from_round = turn(turn(to_far_round, "x", 3), "x", 3)
    parts = [own_same[0], own_swapped[0], from_back, from_ahead, from_far, from_round]
    return last(parts, normed, ffn_gain[None], ffn_bias[None])


def solution(mesh):
    fine = Mesh(mesh.devices.reshape(4, 4, 4, 2), ("z", "y", "x", "c"))
    sp, tp = ("z", "y"), ("x", "c")
    placed = (
        P(sp, tp), P(sp, tp), P(sp, tp), P(sp, tp), P(sp, None), P(tp, None), P(), P(),
        P(sp, tp), P(sp, tp), P(tp, sp), P(), P(),
    )

    return jax.shard_map(
        body, mesh=fine, in_specs=placed, out_specs=P(("z", "y", "x", "c"), None), check_vma=False
    )
```

```python
import functools
import jax
import jax.numpy as jnp
import numpy as np
from jax import lax
from jax.experimental import pallas as pl
from jax.experimental.pallas import tpu as pltpu
from jax.sharding import Mesh, PartitionSpec as P


ALPHA = 8.0**0.25
EPSILON = 1e-05
F32 = jnp.float32
BF16 = jnp.bfloat16

ROWS = 768
SUB = 192
HALF = 96
HD = 64
NSH = 16
PACK = 800
TILE = 256
SPLIT = 1
TILES = SUB * NSH // TILE


def vmem():
    return pl.BlockSpec(memory_space=pltpu.VMEM)


def smem():
    return pl.BlockSpec(memory_space=pltpu.SMEM)


def params(mb):
    return pltpu.CompilerParams(vmem_limit_bytes=mb * 1024 * 1024)


def pack_kernel(q_ref, k_ref, v_ref, g_ref, qo_ref, kvo_ref):
    for h in range(4):
        cols = slice(h * HD, (h + 1) * HD)
        kvo_ref[h, 0:ROWS, 0:HD] = k_ref[:, cols]
        kvo_ref[h, 0:ROWS, HD : 2 * HD] = v_ref[:, cols]
        for y in range(4):
            at = y * SUB
            qo_ref[h * 4 + y, :, 0:HD] = q_ref[at : at + HALF, cols]
            qo_ref[h * 4 + y, :, HD : 2 * HD] = q_ref[at + HALF : at + SUB, cols]
        chunks = [-g_ref[h : h + 1, c * 128 : (c + 1) * 128] for c in range(6)]
        value = jnp.concatenate(chunks, axis=0)
        first = value.astype(BF16).astype(F32)
        second = (value - first).astype(BF16).astype(F32)
        third = value - first - second
        rest = jnp.zeros((PACK - ROWS - 18, 128), F32)
        kvo_ref[h, ROWS:PACK, :] = jnp.concatenate(
            [first, second, third, rest], axis=0
        ).astype(BF16)


def pack(q, k, v, g):
    return pl.pallas_call(
        pack_kernel,
        out_shape=(
            jax.ShapeDtypeStruct((NSH, HALF, 128), BF16),
            jax.ShapeDtypeStruct((4, PACK, 128), BF16),
        ),
        in_specs=[vmem()] * 4,
        out_specs=(vmem(), vmem()),
        compiler_params=params(60),
        cost_estimate=pl.CostEstimate(flops=10**6, bytes_accessed=2500000, transcendentals=0),
    )(q, k, v, g)


def unit_table(steps):
    tables, counts = [], []
    for y in range(4):
        units = []
        for t in range(TILES):
            low = (TILE * t) // SUB
            for i, d in enumerate(steps):
                for z in range(4):
                    s = z * 4 + (y + d) % 4
                    if s <= low + 1:
                        units.append((t, i * 4 + z, s, int(s >= low)))
        plain = [u for u in units if not u[3]]
        held = [u for u in units if u[3]]
        if len(plain) % 2:
            held.insert(0, plain.pop())
        if len(held) % 2:
            held.append((0, 0, NSH - 1, 1))
        units = plain + held
        counts.append((len(plain) // 2, len(units) // 2))
        tables.append([(0, 0, 0, 0)] + units + [units[-1]])
    width = max(len(u) for u in tables) + 1
    out = np.zeros((4, 4, width), np.int32)
    for y in range(4):
        out[y, :, : len(tables[y])] = np.array(tables[y], np.int32).T
        out[y, 0:2, -1] = counts[y]
    return out


def attend_kernel(chunks, first, final, *refs):
    refs = list(refs)
    tab, y_ref = refs[:2]
    kv_refs = refs[2 : 2 + chunks]
    at = 2 + chunks
    if first:
        q_ref, qt, top, acc = refs[at : at + 4]
        at += 4
    else:
        qt, top_in, acc_in = refs[at : at + 3]
        at += 3
        if final:
            o_ref = refs[at]
            at += 1
        else:
            top, acc = refs[at : at + 2]
            at += 2
    kaug, vt, qpos, s_a, s_b, p_a, p_b, al_a, al_b, mx_a, mx_b = refs[at : at + 11]
    at += 11
    if first:
        qrow = refs[at]
    if final:
        top, acc, oscr = refs[at : at + 3]
    y = y_ref[0]
    lane = lax.broadcasted_iota(jnp.int32, (1, 128), 1)
    for i in range(chunks):
        kv_ref = kv_refs[i]

        def per_shard(s, carry):
            gates = kv_ref[s, ROWS:PACK, :].astype(F32)
            square = jnp.concatenate(
                [jnp.zeros((HD, 128), F32), gates, jnp.zeros((32, 128), F32)], axis=0
            )
            turned = square.T
            to = i * 4 + s
            for c in range(6):
                part = kv_ref[s, c * 128 : (c + 1) * 128, :]
                mine = (lane == HD + c) | (lane == HD + 6 + c) | (lane == HD + 12 + c)
                biased = jnp.where(mine, turned, 0.0).astype(BF16)
                kaug[to, c * 128 : (c + 1) * 128, :] = jnp.where(lane < HD, part, biased)
                vt[to, :, c * 128 : (c + 1) * 128] = part.T
            vt[to, 48:64, :] = jnp.ones((16, ROWS), BF16)
            return carry

        lax.fori_loop(0, 4, per_shard, 0)

    lane_h = lax.broadcasted_iota(jnp.int32, (HALF, 128), 1)
    lane_t = lax.broadcasted_iota(jnp.int32, (8, TILE), 1)
    if first:

        def per_query(s, carry):
            both = q_ref[s].astype(F32) * (HD**-0.5)
            ones = jnp.where(lane_h < HD + 18, 1.0, 0.0)
            qrow[s, 0:HALF, :] = jnp.where(lane_h < HD, both, ones)
            qrow[s, HALF:SUB, :] = jnp.where(lane_h < HD, pltpu.roll(both, HD, 1), ones)
            return carry

        lax.fori_loop(0, NSH, per_query, 0)
    for t in range(TILES):
        low = (TILE * t) // SUB
        edge = (low + 1) * SUB - TILE * t
        qpos[t] = y * SUB + jnp.where(
            lane_t < edge,
            low * ROWS + (SUB - edge) + lane_t,
            (low + 1) * ROWS + lane_t - edge,
        )
        if first:
            rows = jnp.concatenate(
                [qrow[low, SUB - edge : SUB, :], qrow[low + 1, 0 : TILE - edge, :]], axis=0
            )
            qt[t] = rows.T.astype(BF16)
    if first:
        acc[...] = jnp.zeros(acc.shape, F32)
        top[...] = jnp.full(top.shape, -1e30, F32)
    else:
        acc[...] = acc_in[...]
        top[...] = top_in[...]
    al_b[...] = jnp.ones(al_b.shape, F32)
    p_b[...] = jnp.zeros(p_b.shape, BF16)

    def scores(u, out, most, masked):
        rows = ROWS // SPLIT
        high = None
        for i in range(SPLIT):
            part = slice(i * rows, (i + 1) * rows)
            s = jnp.dot(
                kaug[tab[y, 1, u], part, :], qt[tab[y, 0, u]], preferred_element_type=F32
            )
            if masked:
                pos = tab[y, 2, u] * ROWS + i * rows
                pos = pos + lax.broadcasted_iota(jnp.int32, (rows, TILE), 0)
                s = jnp.where(pos <= qpos[tab[y, 0, u], 0:1, :], s, -1e30)
            out[part, :] = s
            here = jnp.max(s.reshape(rows // 8, 8, TILE), axis=0)
            high = here if high is None else jnp.maximum(high, here)
        most[...] = high

    def gather(u, p_before, al_before):
        t = tab[y, 0, u]
        pv = jnp.dot(vt[tab[y, 1, u], 48:128, :], p_before[...], preferred_element_type=F32)
        acc[t] = acc[t] * al_before[0:1, :] + pv

    def unit(u, now, later, before, masked):
        s_now, p_now, al_now, mx_now = now
        s_next, _, _, mx_next = later
        _, p_before, al_before, _ = before
        t = tab[y, 0, u]
        old = top[t, 0:1, :]
        high = jnp.maximum(old, jnp.max(mx_now[...], axis=0, keepdims=True))
        top[t, 0:1, :] = high
        al_now[0:1, :] = jnp.exp(old - high)
        scores(u + 1, s_next, mx_next, masked)
        for k in range(2):
            part = slice(384 * k, 384 * (k + 1))
            p_now[part, :] = jnp.exp(s_now[part, :] - high).astype(BF16)
        gather(u - 1, p_before, al_before)

    one, two = (s_a, p_a, al_a, mx_a), (s_b, p_b, al_b, mx_b)
    last_at = tab.shape[2] - 1
    plain, pairs = tab[y, 0, last_at], tab[y, 1, last_at]
    for masked, low, high in ((False, 0, plain), (True, plain, pairs)):

        def pair(i, carry):
            unit(2 * i + 1, one, two, two, masked)
            unit(2 * i + 2, two, one, one, masked)
            return carry

        scores(2 * low + 1, s_a, mx_a, masked)
        lax.fori_loop(low, high, pair, 0)
    gather(2 * pairs, p_b, al_b)

    if final:

        def finish(t, carry):
            good = acc[t, 16:80, :] / acc[t, 0:1, :]
            full = jnp.concatenate([good, jnp.zeros((HD, TILE), F32)], axis=0)
            oscr[pl.ds(pl.multiple_of(t * TILE, TILE), TILE), :] = full.T
            return carry

        lax.fori_loop(0, TILES, finish, 0)

        def out(s, carry):
            row = pl.multiple_of(s * SUB, SUB)
            one = oscr[pl.ds(row, HALF), :]
            two = oscr[pl.ds(row + HALF, HALF), :]
            o_ref[s] = jnp.where(lane_h < HD, one, pltpu.roll(two, HD, 1)).astype(BF16)
            return carry

        lax.fori_loop(0, NSH, out, 0)


def attend(y, steps, kvs, q=None, state=None, final=False):
    chunks, first = len(kvs), q is not None
    state_shapes = (
        jax.ShapeDtypeStruct((TILES, 8, TILE), F32),
        jax.ShapeDtypeStruct((TILES, 80, TILE), F32),
    )
    scratch = [
        pltpu.VMEM((4 * chunks, ROWS, 128), BF16),
        pltpu.VMEM((4 * chunks, 128, ROWS), BF16),
        pltpu.VMEM((TILES, 8, TILE), jnp.int32),
        pltpu.VMEM((ROWS, TILE), F32),
        pltpu.VMEM((ROWS, TILE), F32),
        pltpu.VMEM((ROWS, TILE), BF16),
        pltpu.VMEM((ROWS, TILE), BF16),
    ] + [pltpu.VMEM((8, TILE), F32)] * 4
    if first:
        outs = (jax.ShapeDtypeStruct((TILES, 128, TILE), BF16),) + state_shapes
        scratch += [pltpu.VMEM((NSH, SUB, 128), F32)]
        rest = [q]
    elif final:
        outs = jax.ShapeDtypeStruct((NSH, HALF, 128), BF16)
        scratch += [pltpu.VMEM(s.shape, F32) for s in state_shapes]
        scratch += [pltpu.VMEM((SUB * NSH, 128), F32)]
        rest = list(state)
    else:
        outs = state_shapes
        rest = list(state)
    table = unit_table(steps)
    share = 2 * int(table[:, 1, -1].mean())
    return pl.pallas_call(
        functools.partial(attend_kernel, chunks, first, final),
        out_shape=outs,
        in_specs=[smem(), smem()] + [vmem()] * (chunks + len(rest)),
        out_specs=jax.tree.map(lambda _: vmem(), outs),
        scratch_shapes=scratch,
        compiler_params=params(60),
        cost_estimate=pl.CostEstimate(
            flops=share * 4 * 10**8, bytes_accessed=3 * 10**6, transcendentals=share * 200000
        ),
    )(jnp.asarray(table), y, *kvs, *rest)


def spread_kernel(o_ref, a_ref):
    for z in range(4):
        for y in range(4):
            for half in range(2):
                a_ref[2 * y + half, :, z * HD : (z + 1) * HD] = o_ref[
                    4 * z + y, :, half * HD : (half + 1) * HD
                ]


def spread(o):
    return pl.pallas_call(
        spread_kernel,
        out_shape=jax.ShapeDtypeStruct((8, HALF, 256), BF16),
        in_specs=[vmem()],
        out_specs=vmem(),
        compiler_params=params(60),
        cost_estimate=pl.CostEstimate(flops=10**5, bytes_accessed=800000, transcendentals=0),
    )(o)


def norm_rows(matrix, gain, shift):
    centred = matrix - jnp.mean(matrix, axis=-1, keepdims=True)
    spread_ = jnp.mean(centred * centred, axis=-1, keepdims=True)
    return centred * lax.rsqrt(spread_ + EPSILON) * gain + shift


def mix_kernel(place, a_ref, stream_ref, gain_ref, bias_ref, same_ref, other_ref, n_ref, total):
    c, x = place[0], pl.program_id(0)
    term = jnp.dot(a_ref[2 * x + c], same_ref[0], preferred_element_type=F32)
    term = term + jnp.dot(a_ref[2 * x + 1 - c], other_ref[0], preferred_element_type=F32)

    @pl.when(x == 0)
    def _():
        total[...] = term

    @pl.when(x > 0)
    def _():
        total[...] += term

    @pl.when(x == 3)
    def _():
        mixed = total[...].astype(BF16).astype(F32)
        matrix = ALPHA * stream_ref[...].astype(F32) + mixed
        n_ref[...] = norm_rows(matrix, gain_ref[...], bias_ref[...]).astype(BF16)


def whole(shape):
    return pl.BlockSpec(shape, lambda i, place: (0,) * len(shape))


def along(shape):
    return pl.BlockSpec((1, *shape), lambda i, place: (i,) + (0,) * len(shape))


def mix(place, att, stream, gain, bias, same, other):
    return pl.pallas_call(
        mix_kernel,
        out_shape=jax.ShapeDtypeStruct((HALF, 2048), BF16),
        grid_spec=pltpu.PrefetchScalarGridSpec(
            num_scalar_prefetch=1,
            grid=(4,),
            in_specs=[
                whole((8, HALF, 256)),
                pl.BlockSpec((HALF, 2048), lambda i, place: (place[1], 0)),
                whole((1, 2048)),
                whole((1, 2048)),
                along((256, 2048)),
                along((256, 2048)),
            ],
            out_specs=whole((HALF, 2048)),
            scratch_shapes=[pltpu.VMEM((HALF, 2048), F32)],
        ),
        compiler_params=params(60),
        cost_estimate=pl.CostEstimate(
            flops=2 * HALF * 2048 * 2048, bytes_accessed=9 * 10**6, transcendentals=0
        ),
    )(place, att, stream, gain, bias, same, other)


BLOCKS = 3


def ffn_kernel(count, *refs):
    x_refs = refs[: 2 * count]
    w_ref, same_ref, other_ref = refs[2 * count :]
    x = jnp.concatenate([r[...] for r in x_refs], axis=0)

    def rows(at, width):
        return jnp.concatenate([w_ref[s, at : at + width, :] for s in range(NSH)], axis=1)

    total = None
    for j in range(BLOCKS):
        width = min(256, 704 - 256 * j)
        across = (((1,), (1,)), ((), ()))
        gate = lax.dot_general(x, rows(256 * j, width), across, preferred_element_type=F32)
        up = lax.dot_general(x, rows(704 + 256 * j, width), across, preferred_element_type=F32)
        hidden = (gate / (1.0 + jnp.exp(-gate)) * up).astype(BF16)
        term = jnp.dot(hidden, rows(1408 + 256 * j, width), preferred_element_type=F32)
        total = term if total is None else total + term
    out = total.astype(BF16)
    for i in range(count):
        same_ref[i] = out[i * HALF : (i + 1) * HALF]
        other_ref[i] = out[(count + i) * HALF : (count + i + 1) * HALF]


def ffn(pieces, w):
    count = len(pieces) // 2
    shape = jax.ShapeDtypeStruct((count, HALF, 2048), BF16)
    rows = 2 * count * HALF
    return pl.pallas_call(
        functools.partial(ffn_kernel, count),
        out_shape=(shape, shape),
        in_specs=[vmem()] * (2 * count + 1),
        out_specs=(vmem(), vmem()),
        compiler_params=params(30),
        cost_estimate=pl.CostEstimate(
            flops=6 * rows * 2048 * 704, bytes_accessed=10**7, transcendentals=rows * 704
        ),
    )(*pieces, w)


def join_kernel(split, *refs):
    same_ref, other_ref = refs[:2]
    outs = refs[2:]
    for i in range(same_ref.shape[0]):
        both = (same_ref[i].astype(F32) + other_ref[i].astype(F32)).astype(BF16)
        for k in range(split):
            rows = HALF // split
            outs[i * split + k][...] = both[k * rows : (k + 1) * rows]


def join(same, other, split=1):
    count = same.shape[0] * split
    shape = jax.ShapeDtypeStruct((HALF // split, 2048), BF16)
    return pl.pallas_call(
        functools.partial(join_kernel, split),
        out_shape=(shape,) * count,
        in_specs=[vmem()] * 2,
        out_specs=(vmem(),) * count,
        compiler_params=params(8),
        cost_estimate=pl.CostEstimate(flops=10**6, bytes_accessed=10**6, transcendentals=0),
    )(same, other)


def last_kernel(n_ref, gain_ref, bias_ref, *refs):
    o_ref = refs[-1]
    total = refs[0][...].astype(F32)
    for r in refs[1:-1]:
        total = total + r[...].astype(F32)
    lowered = total.astype(BF16).astype(F32)
    matrix = ALPHA * n_ref[...].astype(F32) + lowered
    o_ref[...] = norm_rows(matrix, gain_ref[...], bias_ref[...]).astype(BF16)


def last(parts, normed, gain, bias):
    return pl.pallas_call(
        last_kernel,
        out_shape=jax.ShapeDtypeStruct((HALF, 2048), BF16),
        in_specs=[vmem()] * (3 + len(parts)),
        out_specs=vmem(),
        compiler_params=params(16),
        cost_estimate=pl.CostEstimate(
            flops=4 * 10**6, bytes_accessed=4 * 10**6, transcendentals=0
        ),
    )(normed, gain, bias, *parts)


def body(
    queries, key_rows, value_rows, log_forget, stream_in, out_weight, mix_gain, mix_bias,
    gate_weight, up_weight, down_weight, ffn_gain, ffn_bias,
):
    yi = lax.axis_index("y").astype(jnp.int32)[None]
    xi = lax.axis_index("x")
    ci = lax.axis_index("c")

    def turn(value, axis, d):
        return lax.ppermute(value, axis, [(i, (i + d) % 4) for i in range(4)])

    def swap(value):
        return lax.ppermute(value, "c", [(0, 1), (1, 0)])

    place = jnp.stack([ci, 2 * xi + ci, xi]).astype(jnp.int32)
    w_same = lax.all_gather(out_weight, "x", axis=0, tiled=False)
    q_pack, kv_pack = pack(queries, key_rows, value_rows, log_forget.T)
    q_mine = lax.all_to_all(q_pack, ("z", "y"), split_axis=0, concat_axis=0, tiled=True)
    kv_own = lax.all_to_all(kv_pack, "z", split_axis=0, concat_axis=0, tiled=True)
    kv_back, kv_ahead = turn(kv_own, "y", 1), turn(kv_own, "y", 3)
    kv_far = turn(kv_own, "y", 2)
    w_other = swap(w_same)
    shards = jnp.concatenate([gate_weight.T, up_weight.T, down_weight], axis=0)
    ffn_all = lax.all_gather(shards, ("z", "y"), axis=0, tiled=False)

    qt, *state = attend(yi, (0,), [kv_own], q=q_mine)
    state = attend(yi, (3, 1), [kv_back, kv_ahead], state=(qt, *state))
    attended = attend(yi, (2,), [kv_far], state=(qt, *state), final=True)
    by_shard = lax.all_to_all(attended, ("z", "y"), split_axis=0, concat_axis=0, tiled=True)
    by_rows = lax.all_to_all(
        spread(by_shard), ("x", "c"), split_axis=0, concat_axis=0, tiled=True
    )
    normed = mix(place, by_rows, stream_in, mix_gain[None], mix_bias[None], w_same, w_other)
    back, ahead = turn(normed, "x", 1), turn(normed, "x", 3)
    n_swapped = swap(normed)
    own_same, own_other = ffn((normed, n_swapped), ffn_all)
    own_swapped = swap(own_other)
    far = turn(back, "x", 1)
    near = (back, ahead, swap(back), swap(ahead))
    near_same, near_other = ffn(near, ffn_all)
    near_swapped = swap(near_other)
    far_other_rows = swap(far)
    to_back, to_ahead = join(near_same, near_swapped)
    from_ahead, from_back = turn(to_back, "x", 3), turn(to_ahead, "x", 1)
    far_same, far_other = ffn((far, far_other_rows), ffn_all)
    far_swapped = swap(far_other)
    (to_far,) = join(far_same, far_swapped)
    from_far = turn(to_far, "x", 2)
    parts = [own_same[0], own_swapped[0], from_back, from_ahead, from_far]
    return last(parts, normed, ffn_gain[None], ffn_bias[None])


def solution(mesh):
    fine = Mesh(mesh.devices.reshape(4, 4, 4, 2), ("z", "y", "x", "c"))
    sp, tp = ("z", "y"), ("x", "c")
    placed = (
        P(sp, tp), P(sp, tp), P(sp, tp), P(sp, tp), P(sp, None), P(tp, None), P(), P(),
        P(sp, tp), P(sp, tp), P(tp, sp), P(), P(),
    )

    return jax.shard_map(
        body, mesh=fine, in_specs=placed, out_specs=P(("z", "y", "x", "c"), None), check_vma=False
    )
```

```python
import functools
import jax
import jax.numpy as jnp
import numpy as np
from jax import lax
from jax.experimental import pallas as pl
from jax.experimental.pallas import tpu as pltpu
from jax.sharding import Mesh, PartitionSpec as P


ALPHA = 8.0**0.25
EPSILON = 1e-05
F32 = jnp.float32
BF16 = jnp.bfloat16

ROWS = 768
SUB = 192
HALF = 96
HD = 64
NSH = 16
PACK = 800
TILE = 256
SPLIT = 1
TILES = SUB * NSH // TILE


def vmem():
    return pl.BlockSpec(memory_space=pltpu.VMEM)


def smem():
    return pl.BlockSpec(memory_space=pltpu.SMEM)


def params(mb):
    return pltpu.CompilerParams(vmem_limit_bytes=mb * 1024 * 1024)


def pack_kernel(z_ref, q_ref, k_ref, v_ref, g_ref, qo_ref, *refs):
    outs, held = refs[:4], refs[4]
    for h in range(4):
        cols = slice(h * HD, (h + 1) * HD)
        held[h, 0:ROWS, 0:HD] = k_ref[:, cols]
        held[h, 0:ROWS, HD : 2 * HD] = v_ref[:, cols]
        for y in range(4):
            at = y * SUB
            qo_ref[h * 4 + y, :, 0:HD] = q_ref[at : at + HALF, cols]
            qo_ref[h * 4 + y, :, HD : 2 * HD] = q_ref[at + HALF : at + SUB, cols]
        chunks = [-g_ref[h : h + 1, c * 128 : (c + 1) * 128] for c in range(6)]
        value = jnp.concatenate(chunks, axis=0)
        first = value.astype(BF16).astype(F32)
        second = (value - first).astype(BF16).astype(F32)
        third = value - first - second
        rest = jnp.zeros((PACK - ROWS - 18, 128), F32)
        held[h, ROWS:PACK, :] = jnp.concatenate([first, second, third, rest], axis=0).astype(BF16)
    for d in range(4):
        outs[d][...] = held[lax.rem(z_ref[0] + d, 4)]


def pack(z, q, k, v, g):
    packet = jax.ShapeDtypeStruct((PACK, 128), BF16)
    return pl.pallas_call(
        pack_kernel,
        out_shape=(jax.ShapeDtypeStruct((NSH, HALF, 128), BF16),) + (packet,) * 4,
        in_specs=[smem()] + [vmem()] * 4,
        out_specs=(vmem(),) * 5,
        scratch_shapes=[pltpu.VMEM((4, PACK, 128), BF16)],
        compiler_params=params(60),
        cost_estimate=pl.CostEstimate(flops=10**6, bytes_accessed=2500000, transcendentals=0),
    )(z, q, k, v, g)


def assemble_kernel(z_ref, *refs):
    for d in range(4):
        refs[4][lax.rem(z_ref[0] + 4 - d, 4)] = refs[d][...]


def assemble(z, pieces):
    return pl.pallas_call(
        assemble_kernel,
        out_shape=jax.ShapeDtypeStruct((4, PACK, 128), BF16),
        in_specs=[smem()] + [vmem()] * 4,
        out_specs=vmem(),
        compiler_params=params(16),
        cost_estimate=pl.CostEstimate(flops=10**6, bytes_accessed=1700000, transcendentals=0),
    )(z, *pieces)


def unit_table(steps):
    tables, counts = [], []
    for y in range(4):
        units = []
        for t in range(TILES):
            low = (TILE * t) // SUB
            for i, d in enumerate(steps):
                for z in range(4):
                    s = z * 4 + (y + d) % 4
                    if s <= low + 1:
                        units.append((t, i * 4 + z, s, int(s >= low)))
        plain = [u for u in units if not u[3]]
        held = [u for u in units if u[3]]
        if len(plain) % 2:
            held.insert(0, plain.pop())
        if len(held) % 2:
            held.append((0, 0, NSH - 1, 1))
        units = plain + held
        counts.append((len(plain) // 2, len(units) // 2))
        tables.append([(0, 0, 0, 0)] + units + [units[-1]])
    width = max(len(u) for u in tables) + 1
    out = np.zeros((4, 4, width), np.int32)
    for y in range(4):
        out[y, :, : len(tables[y])] = np.array(tables[y], np.int32).T
        out[y, 0:2, -1] = counts[y]
    return out


def attend_kernel(chunks, first, final, *refs):
    refs = list(refs)
    tab, y_ref = refs[:2]
    kv_refs = refs[2 : 2 + chunks]
    at = 2 + chunks
    if first:
        q_ref, qt, top, acc = refs[at : at + 4]
        at += 4
    else:
        qt, top_in, acc_in = refs[at : at + 3]
        at += 3
        if final:
            o_ref = refs[at]
            at += 1
        else:
            top, acc = refs[at : at + 2]
            at += 2
    kaug, vt, qpos, s_a, s_b, p_a, p_b, al_a, al_b, mx_a, mx_b = refs[at : at + 11]
    at += 11
    if first:
        qrow = refs[at]
    if final:
        top, acc, oscr = refs[at : at + 3]
    y = y_ref[0]
    lane = lax.broadcasted_iota(jnp.int32, (1, 128), 1)
    for i in range(chunks):
        kv_ref = kv_refs[i]

        def per_shard(s, carry):
            gates = kv_ref[s, ROWS:PACK, :].astype(F32)
            square = jnp.concatenate(
                [jnp.zeros((HD, 128), F32), gates, jnp.zeros((32, 128), F32)], axis=0
            )
            turned = square.T
            to = i * 4 + s
            for c in range(6):
                part = kv_ref[s, c * 128 : (c + 1) * 128, :]
                mine = (lane == HD + c) | (lane == HD + 6 + c) | (lane == HD + 12 + c)
                biased = jnp.where(mine, turned, 0.0).astype(BF16)
                kaug[to, c * 128 : (c + 1) * 128, :] = jnp.where(lane < HD, part, biased)
                vt[to, :, c * 128 : (c + 1) * 128] = part.T
            vt[to, 48:64, :] = jnp.ones((16, ROWS), BF16)
            return carry

        lax.fori_loop(0, 4, per_shard, 0)

    lane_h = lax.broadcasted_iota(jnp.int32, (HALF, 128), 1)
    lane_t = lax.broadcasted_iota(jnp.int32, (8, TILE), 1)
    if first:

        def per_query(s, carry):
            both = q_ref[s].astype(F32) * (HD**-0.5)
            ones = jnp.where(lane_h < HD + 18, 1.0, 0.0)
            qrow[s, 0:HALF, :] = jnp.where(lane_h < HD, both, ones)
            qrow[s, HALF:SUB, :] = jnp.where(lane_h < HD, pltpu.roll(both, HD, 1), ones)
            return carry

        lax.fori_loop(0, NSH, per_query, 0)
    for t in range(TILES):
        low = (TILE * t) // SUB
        edge = (low + 1) * SUB - TILE * t
        qpos[t] = y * SUB + jnp.where(
            lane_t < edge,
            low * ROWS + (SUB - edge) + lane_t,
            (low + 1) * ROWS + lane_t - edge,
        )
        if first:
            rows = jnp.concatenate(
                [qrow[low, SUB - edge : SUB, :], qrow[low + 1, 0 : TILE - edge, :]], axis=0
            )
            qt[t] = rows.T.astype(BF16)
    if first:
        acc[...] = jnp.zeros(acc.shape, F32)
        top[...] = jnp.full(top.shape, -1e30, F32)
    else:
        acc[...] = acc_in[...]
        top[...] = top_in[...]
    al_b[...] = jnp.ones(al_b.shape, F32)
    p_b[...] = jnp.zeros(p_b.shape, BF16)

    def scores(u, out, most, masked):
        rows = ROWS // SPLIT
        high = None
        for i in range(SPLIT):
            part = slice(i * rows, (i + 1) * rows)
            s = jnp.dot(
                kaug[tab[y, 1, u], part, :], qt[tab[y, 0, u]], preferred_element_type=F32
            )
            if masked:
                pos = tab[y, 2, u] * ROWS + i * rows
                pos = pos + lax.broadcasted_iota(jnp.int32, (rows, TILE), 0)
                s = jnp.where(pos <= qpos[tab[y, 0, u], 0:1, :], s, -1e30)
            out[part, :] = s
            here = jnp.max(s.reshape(rows // 8, 8, TILE), axis=0)
            high = here if high is None else jnp.maximum(high, here)
        most[...] = high

    def gather(u, p_before, al_before):
        t = tab[y, 0, u]
        pv = jnp.dot(vt[tab[y, 1, u], 48:128, :], p_before[...], preferred_element_type=F32)
        acc[t] = acc[t] * al_before[0:1, :] + pv

    def unit(u, now, later, before, masked):
        s_now, p_now, al_now, mx_now = now
        s_next, _, _, mx_next = later
        _, p_before, al_before, _ = before
        t = tab[y, 0, u]
        old = top[t, 0:1, :]
        high = jnp.maximum(old, jnp.max(mx_now[...], axis=0, keepdims=True))
        top[t, 0:1, :] = high
        al_now[0:1, :] = jnp.exp(old - high)
        scores(u + 1, s_next, mx_next, masked)
        for k in range(2):
            part = slice(384 * k, 384 * (k + 1))
            p_now[part, :] = jnp.exp(s_now[part, :] - high).astype(BF16)
        gather(u - 1, p_before, al_before)

    one, two = (s_a, p_a, al_a, mx_a), (s_b, p_b, al_b, mx_b)
    last_at = tab.shape[2] - 1
    plain, pairs = tab[y, 0, last_at], tab[y, 1, last_at]
    for masked, low, high in ((False, 0, plain), (True, plain, pairs)):

        def pair(i, carry):
            unit(2 * i + 1, one, two, two, masked)
            unit(2 * i + 2, two, one, one, masked)
            return carry

        scores(2 * low + 1, s_a, mx_a, masked)
        lax.fori_loop(low, high, pair, 0)
    gather(2 * pairs, p_b, al_b)

    if final:

        def finish(t, carry):
            good = acc[t, 16:80, :] / acc[t, 0:1, :]
            full = jnp.concatenate([good, jnp.zeros((HD, TILE), F32)], axis=0)
            oscr[pl.ds(pl.multiple_of(t * TILE, TILE), TILE), :] = full.T
            return carry

        lax.fori_loop(0, TILES, finish, 0)

        def out(s, carry):
            row = pl.multiple_of(s * SUB, SUB)
            one = oscr[pl.ds(row, HALF), :]
            two = oscr[pl.ds(row + HALF, HALF), :]
            o_ref[s] = jnp.where(lane_h < HD, one, pltpu.roll(two, HD, 1)).astype(BF16)
            return carry

        lax.fori_loop(0, NSH, out, 0)


def attend(y, steps, kvs, q=None, state=None, final=False):
    chunks, first = len(kvs), q is not None
    state_shapes = (
        jax.ShapeDtypeStruct((TILES, 8, TILE), F32),
        jax.ShapeDtypeStruct((TILES, 80, TILE), F32),
    )
    scratch = [
        pltpu.VMEM((4 * chunks, ROWS, 128), BF16),
        pltpu.VMEM((4 * chunks, 128, ROWS), BF16),
        pltpu.VMEM((TILES, 8, TILE), jnp.int32),
        pltpu.VMEM((ROWS, TILE), F32),
        pltpu.VMEM((ROWS, TILE), F32),
        pltpu.VMEM((ROWS, TILE), BF16),
        pltpu.VMEM((ROWS, TILE), BF16),
    ] + [pltpu.VMEM((8, TILE), F32)] * 4
    if first:
        outs = (jax.ShapeDtypeStruct((TILES, 128, TILE), BF16),) + state_shapes
        scratch += [pltpu.VMEM((NSH, SUB, 128), F32)]
        rest = [q]
    elif final:
        outs = jax.ShapeDtypeStruct((NSH, HALF, 128), BF16)
        scratch += [pltpu.VMEM(s.shape, F32) for s in state_shapes]
        scratch += [pltpu.VMEM((SUB * NSH, 128), F32)]
        rest = list(state)
    else:
        outs = state_shapes
        rest = list(state)
    table = unit_table(steps)
    share = 2 * int(table[:, 1, -1].mean())
    return pl.pallas_call(
        functools.partial(attend_kernel, chunks, first, final),
        out_shape=outs,
        in_specs=[smem(), smem()] + [vmem()] * (chunks + len(rest)),
        out_specs=jax.tree.map(lambda _: vmem(), outs),
        scratch_shapes=scratch,
        compiler_params=params(60),
        cost_estimate=pl.CostEstimate(
            flops=share * 4 * 10**8, bytes_accessed=3 * 10**6, transcendentals=share * 200000
        ),
    )(jnp.asarray(table), y, *kvs, *rest)


def spread_kernel(o_ref, a_ref):
    for z in range(4):
        for y in range(4):
            for half in range(2):
                a_ref[2 * y + half, :, z * HD : (z + 1) * HD] = o_ref[
                    4 * z + y, :, half * HD : (half + 1) * HD
                ]


def spread(o):
    return pl.pallas_call(
        spread_kernel,
        out_shape=jax.ShapeDtypeStruct((8, HALF, 256), BF16),
        in_specs=[vmem()],
        out_specs=vmem(),
        compiler_params=params(16),
        cost_estimate=pl.CostEstimate(flops=10**5, bytes_accessed=800000, transcendentals=0),
    )(o)


def norm_rows(matrix, gain, shift):
    centred = matrix - jnp.mean(matrix, axis=-1, keepdims=True)
    spread_ = jnp.mean(centred * centred, axis=-1, keepdims=True)
    return centred * lax.rsqrt(spread_ + EPSILON) * gain + shift


def mix_kernel(place, a_ref, stream_ref, gain_ref, bias_ref, same_ref, other_ref, n_ref, total):
    c, x = place[0], pl.program_id(0)
    term = jnp.dot(a_ref[2 * x + c], same_ref[0], preferred_element_type=F32)
    term = term + jnp.dot(a_ref[2 * x + 1 - c], other_ref[0], preferred_element_type=F32)

    @pl.when(x == 0)
    def _():
        total[...] = term

    @pl.when(x > 0)
    def _():
        total[...] += term

    @pl.when(x == 3)
    def _():
        mixed = total[...].astype(BF16).astype(F32)
        matrix = ALPHA * stream_ref[...].astype(F32) + mixed
        n_ref[...] = norm_rows(matrix, gain_ref[...], bias_ref[...]).astype(BF16)


def whole(shape):
    return pl.BlockSpec(shape, lambda i, place: (0,) * len(shape))


def along(shape):
    return pl.BlockSpec((1, *shape), lambda i, place: (i,) + (0,) * len(shape))


def mix(place, att, stream, gain, bias, same, other):
    return pl.pallas_call(
        mix_kernel,
        out_shape=jax.ShapeDtypeStruct((HALF, 2048), BF16),
        grid_spec=pltpu.PrefetchScalarGridSpec(
            num_scalar_prefetch=1,
            grid=(4,),
            in_specs=[
                whole((8, HALF, 256)),
                pl.BlockSpec((HALF, 2048), lambda i, place: (place[1], 0)),
                whole((1, 2048)),
                whole((1, 2048)),
                along((256, 2048)),
                along((256, 2048)),
            ],
            out_specs=whole((HALF, 2048)),
            scratch_shapes=[pltpu.VMEM((HALF, 2048), F32)],
        ),
        compiler_params=params(52),
        cost_estimate=pl.CostEstimate(
            flops=2 * HALF * 2048 * 2048, bytes_accessed=9 * 10**6, transcendentals=0
        ),
    )(place, att, stream, gain, bias, same, other)


BLOCKS = 3


def ffn_kernel(count, *refs):
    x_refs = refs[: 2 * count]
    w_ref, same_ref, other_ref = refs[2 * count :]
    x = jnp.concatenate([r[...] for r in x_refs], axis=0)

    def rows(at, width):
        return jnp.concatenate([w_ref[s, at : at + width, :] for s in range(NSH)], axis=1)

    total = None
    for j in range(BLOCKS):
        width = min(256, 704 - 256 * j)
        across = (((1,), (1,)), ((), ()))
        gate = lax.dot_general(x, rows(256 * j, width), across, preferred_element_type=F32)
        up = lax.dot_general(x, rows(704 + 256 * j, width), across, preferred_element_type=F32)
        hidden = (gate / (1.0 + jnp.exp(-gate)) * up).astype(BF16)
        term = jnp.dot(hidden, rows(1408 + 256 * j, width), preferred_element_type=F32)
        total = term if total is None else total + term
    out = total.astype(BF16)
    for i in range(count):
        same_ref[i] = out[i * HALF : (i + 1) * HALF]
        other_ref[i] = out[(count + i) * HALF : (count + i + 1) * HALF]


def ffn(pieces, w):
    count = len(pieces) // 2
    shape = jax.ShapeDtypeStruct((count, HALF, 2048), BF16)
    rows = 2 * count * HALF
    return pl.pallas_call(
        functools.partial(ffn_kernel, count),
        out_shape=(shape, shape),
        in_specs=[vmem()] * (2 * count + 1),
        out_specs=(vmem(), vmem()),
        compiler_params=params(30),
        cost_estimate=pl.CostEstimate(
            flops=6 * rows * 2048 * 704, bytes_accessed=10**7, transcendentals=rows * 704
        ),
    )(*pieces, w)


def join_kernel(split, *refs):
    same_ref, other_ref = refs[:2]
    outs = refs[2:]
    for i in range(same_ref.shape[0]):
        both = (same_ref[i].astype(F32) + other_ref[i].astype(F32)).astype(BF16)
        for k in range(split):
            rows = HALF // split
            outs[i * split + k][...] = both[k * rows : (k + 1) * rows]


def join(same, other, split=1):
    count = same.shape[0] * split
    shape = jax.ShapeDtypeStruct((HALF // split, 2048), BF16)
    return pl.pallas_call(
        functools.partial(join_kernel, split),
        out_shape=(shape,) * count,
        in_specs=[vmem()] * 2,
        out_specs=(vmem(),) * count,
        compiler_params=params(8),
        cost_estimate=pl.CostEstimate(flops=10**6, bytes_accessed=10**6, transcendentals=0),
    )(same, other)


def last_kernel(n_ref, gain_ref, bias_ref, *refs):
    o_ref = refs[-1]
    total = refs[0][...].astype(F32)
    for r in refs[1:-1]:
        total = total + r[...].astype(F32)
    lowered = total.astype(BF16).astype(F32)
    matrix = ALPHA * n_ref[...].astype(F32) + lowered
    o_ref[...] = norm_rows(matrix, gain_ref[...], bias_ref[...]).astype(BF16)


def last(parts, normed, gain, bias):
    return pl.pallas_call(
        last_kernel,
        out_shape=jax.ShapeDtypeStruct((HALF, 2048), BF16),
        in_specs=[vmem()] * (3 + len(parts)),
        out_specs=vmem(),
        compiler_params=params(16),
        cost_estimate=pl.CostEstimate(
            flops=4 * 10**6, bytes_accessed=4 * 10**6, transcendentals=0
        ),
    )(normed, gain, bias, *parts)


def body(
    queries, key_rows, value_rows, log_forget, stream_in, out_weight, mix_gain, mix_bias,
    gate_weight, up_weight, down_weight, ffn_gain, ffn_bias,
):
    yi = lax.axis_index("y").astype(jnp.int32)[None]
    xi = lax.axis_index("x")
    ci = lax.axis_index("c")

    def turn(value, axis, d):
        return lax.ppermute(value, axis, [(i, (i + d) % 4) for i in range(4)])

    def swap(value):
        return lax.ppermute(value, "c", [(0, 1), (1, 0)])

    place = jnp.stack([ci, 2 * xi + ci, xi]).astype(jnp.int32)
    w_same = lax.all_gather(out_weight, "x", axis=0, tiled=False)
    zi = lax.axis_index("z").astype(jnp.int32)[None]
    q_pack, *packets = pack(zi, queries, key_rows, value_rows, log_forget.T)
    q_mine = lax.all_to_all(q_pack, ("z", "y"), split_axis=0, concat_axis=0, tiled=True)
    pieces = [packets[0]] + [turn(packets[d], "z", d) for d in (1, 2, 3)]
    kv_own = assemble(zi, pieces)
    kv_back, kv_ahead = turn(kv_own, "y", 1), turn(kv_own, "y", 3)
    kv_far = turn(kv_own, "y", 2)
    w_other = swap(w_same)
    shards = jnp.concatenate([gate_weight.T, up_weight.T, down_weight], axis=0)
    ffn_all = lax.all_gather(shards, ("z", "y"), axis=0, tiled=False)

    qt, *state = attend(yi, (0,), [kv_own], q=q_mine)
    state = attend(yi, (3, 1), [kv_back, kv_ahead], state=(qt, *state))
    attended = attend(yi, (2,), [kv_far], state=(qt, *state), final=True)
    by_shard = lax.all_to_all(attended, ("z", "y"), split_axis=0, concat_axis=0, tiled=True)
    by_rows = lax.all_to_all(
        spread(by_shard), ("x", "c"), split_axis=0, concat_axis=0, tiled=True
    )
    normed = mix(place, by_rows, stream_in, mix_gain[None], mix_bias[None], w_same, w_other)
    back, ahead = turn(normed, "x", 1), turn(normed, "x", 3)
    n_swapped = swap(normed)
    own_same, own_other = ffn((normed, n_swapped), ffn_all)
    own_swapped = swap(own_other)
    far = turn(back, "x", 1)
    near = (back, ahead, swap(back), swap(ahead))
    near_same, near_other = ffn(near, ffn_all)
    near_swapped = swap(near_other)
    far_other_rows = swap(far)
    to_back, to_ahead = join(near_same, near_swapped)
    from_ahead, from_back = turn(to_back, "x", 3), turn(to_ahead, "x", 1)
    far_same, far_other = ffn((far, far_other_rows), ffn_all)
    far_swapped = swap(far_other)
    (to_far,) = join(far_same, far_swapped)
    from_far = turn(to_far, "x", 2)
    parts = [own_same[0], own_swapped[0], from_back, from_ahead, from_far]
    return last(parts, normed, ffn_gain[None], ffn_bias[None])


def solution(mesh):
    fine = Mesh(mesh.devices.reshape(4, 4, 4, 2), ("z", "y", "x", "c"))
    sp, tp = ("z", "y"), ("x", "c")
    placed = (
        P(sp, tp), P(sp, tp), P(sp, tp), P(sp, tp), P(sp, None), P(tp, None), P(), P(),
        P(sp, tp), P(sp, tp), P(tp, sp), P(), P(),
    )

    return jax.shard_map(
        body, mesh=fine, in_specs=placed, out_specs=P(("z", "y", "x", "c"), None), check_vma=False
    )
```
